512 devices in a mesh: sp: 64 (over z, y), tp: 8 (over x, core).
Axes of the slice: x: 4, y: 8, z: 8, core: 2. Of those that a mesh axis runs over, the one named last changes fastest.
Arguments:
- hidden_in: bfloat16 [32768, 2048], P('sp'), may hold values from -64 to 64
- pre_gain: float32 [2048], replicated, may hold values from 0.1 to 1.9
- query_proj: bfloat16 [2048, 2048], P(None, 'tp'), may hold values from -2 to 2
- key_proj: bfloat16 [2048, 2048], P('sp', 'tp'), may hold values from -2 to 2
- value_proj: bfloat16 [2048, 2048], P('sp', 'tp'), may hold values from -0.125 to 0.125
- out_proj: bfloat16 [2048, 2048], P('tp'), may hold values from -0.125 to 0.125
- post_gain: float32 [2048], replicated, may hold values from 0.1 to 1.9
Outputs:
- layer_out: bfloat16 [32768, 2048], P(('sp', 'tp'))
- log_weight: float32 [32, 32768], P('tp', 'sp')
The draws below stay inside these ranges and needn't reach their ends.
All inputs are finite; a program needn't handle non-finite values.
Results may differ from the reference program's by a relative error of at most 0.018.
The reference program's roundings to bfloat16 on the way count: a program that leaves them out, or rounds other values in their place, can miss the bound.
Values may be sent and summed in bfloat16 or wider, within the bound.
No kernel may reach another device: no remote copies, remote signals or barrier semaphores. Data moves between devices by JAX's collectives and lax.ppermute only.
A program may use at most 64 MiB of HBM per device.

```python
import jax
import jax.numpy as jnp
from jax import lax

D = 2048
HEADS = 32
HEAD_DIM = 64
SPAN = 128
TOKENS = 32768
N_TP = 8


def draw_hidden_in(key, part):
    noise_part = jax.random.normal(jax.random.fold_in(key, 3), (TOKENS, D), jnp.float32)
    return jnp.clip(noise_part, -64.0, 64.0).astype(jnp.bfloat16)


def shared_pair(key):
    fan_scale = D ** (-0.5)
    query_part = jax.random.normal(jax.random.fold_in(key, 22), (D, HEADS * HEAD_DIM), jnp.float32) * fan_scale
    key_part = jax.random.normal(jax.random.fold_in(key, 23), (D, HEADS * HEAD_DIM), jnp.float32) * fan_scale
    return (jnp.clip(query_part, -2.0, 2.0), jnp.clip(key_part, -2.0, 2.0))


def draw_query_proj(key, part):
    return shared_pair(key)[0].astype(jnp.bfloat16)


def draw_key_proj(key, part):
    return shared_pair(key)[1].astype(jnp.bfloat16)


def steps_of(key, dims, split, least, high):
    factor_of = 1.0
    for dim, parts in split:
        steps = jax.random.uniform(jax.random.fold_in(jax.random.fold_in(key, 6), dim), (parts,), jnp.float32, least / len(split), high / len(split))
        factor_of = factor_of * jnp.repeat(jnp.exp(steps), dims[dim] // parts).reshape((-1,) + (1,) * (len(dims) - 1 - dim))
    return factor_of


def noise(key, shape, deviation, most, shards=(), held_as=jnp.bfloat16):
    values = jax.random.normal(key, shape, jnp.float32) * deviation
    if len(shards) > 0:
        values = steps_of(key, shape, shards, -0.22, 0.18) * values
    return jnp.clip(values, min=-most, max=most).astype(held_as)


def setup_inputs(seed: int = 0) -> dict:
    splits = jax.random.split(jax.random.key(seed), 8)
    return {
        "hidden_in": draw_hidden_in(jax.random.fold_in(splits[7], 71), 0),
        "pre_gain": jnp.clip(1.0 + 0.18 * jax.random.normal(splits[1], (D,), jnp.float32), 0.1, 1.9),
        "query_proj": draw_query_proj(jax.random.fold_in(splits[7], 71), 0),
        "key_proj": draw_key_proj(jax.random.fold_in(splits[7], 71), 0),
        "value_proj": noise(splits[4], (D, HEADS * HEAD_DIM), D ** -0.5, 0.125, ((0, 64), (1, 8))),
        "out_proj": noise(splits[5], (HEADS * HEAD_DIM, D), (HEADS * HEAD_DIM) ** -0.5, 0.125, ((0, 8),)),
        "post_gain": jnp.clip(1.0 + 0.18 * jax.random.normal(splits[6], (D,), jnp.float32), 0.1, 1.9),
    }


EPS = 1e-06
ROPE_BASE = 10000.0
DILATIONS = (1, 4, 16)

def rotate(vectors, positions):
    half_dim = vectors.shape[-1] // 2
    frequency = ROPE_BASE ** (-(jnp.arange(half_dim, dtype=jnp.float32) * 2.0 / vectors.shape[-1]))
    angles = positions[:, None] * frequency[None, :]
    cos_part = jnp.cos(angles)[:, None, :]
    sin_part = jnp.sin(angles)[:, None, :]
    front_half = vectors[..., :half_dim]
    back_half = vectors[..., half_dim:]
    return jnp.concatenate([front_half * cos_part - back_half * sin_part, back_half * cos_part + front_half * sin_part], axis=-1)

def rms_scale(matrix, gain):
    return matrix * lax.rsqrt(lax.optimization_barrier(jnp.mean(matrix * matrix, axis=-1, keepdims=True)) + EPS) * gain

def residue_attention(queries, key_rows, values, dilation):
    seq_len, head_count, head_depth = queries.shape
    blocks = seq_len // (dilation * SPAN)
    block_shape = (blocks, SPAN, dilation, head_count, head_depth)
    query_blocks = queries.reshape(block_shape).astype(jnp.float32)
    key_blocks = key_rows.reshape(block_shape).astype(jnp.float32)
    value_blocks = values.reshape(block_shape).astype(jnp.float32)
    zero_block = jnp.zeros((1,) + block_shape[1:], jnp.float32)
    key_pairs = jnp.concatenate([jnp.concatenate([zero_block, key_blocks[:-1]], axis=0), key_blocks], axis=1)
    value_pairs = jnp.concatenate([jnp.concatenate([zero_block, value_blocks[:-1]], axis=0), value_blocks], axis=1)
    scores = jnp.einsum('bqrhe,bkrhe->brhqk', query_blocks, key_pairs) * head_depth ** (-0.5)
    query_idx = jnp.arange(SPAN, dtype=jnp.int32)[:, None]
    key_idx = jnp.arange(2 * SPAN, dtype=jnp.int32)[None, :]
    distance = query_idx + SPAN - key_idx
    in_band = (distance >= 0) & (distance <= SPAN)
    key_pos = (jnp.arange(blocks, dtype=jnp.int32)[:, None, None, None, None] * SPAN + jnp.arange(2 * SPAN, dtype=jnp.int32)[None, None, None, None, :] - SPAN) * dilation + jnp.arange(dilation, dtype=jnp.int32)[None, :, None, None, None]
    valid = in_band[None, None, None] & (key_pos >= 0)
    scores = jnp.where(valid, scores, -jnp.inf)
    row_max = lax.optimization_barrier(jnp.max(scores, axis=-1, keepdims=True))
    exp_scores = jnp.exp(scores - row_max)
    denominator = lax.optimization_barrier(jnp.sum(exp_scores, axis=-1, keepdims=True))
    levels = (row_max + jnp.log(denominator))[..., 0]
    shares = lax.optimization_barrier((exp_scores / denominator).astype(jnp.bfloat16))
    outcome = jnp.einsum('brhqk,bkrhe->bqrhe', shares.astype(jnp.float32), value_pairs)
    outcome = outcome.reshape(seq_len, head_count, head_depth)
    levels = levels.transpose(2, 0, 3, 1).reshape(head_count, seq_len)
    return (outcome, levels)

def blend(group_outs, group_levels):
    levels = jnp.stack(group_levels)
    row_max = lax.optimization_barrier(jnp.max(levels, axis=0))
    log_weight = row_max + jnp.log(lax.optimization_barrier(jnp.sum(jnp.exp(levels - row_max[None]), axis=0)))
    shares = jnp.exp(levels - log_weight[None])
    blended = lax.optimization_barrier(jnp.sum(shares.transpose(0, 2, 1)[..., None] * jnp.stack(group_outs), axis=0))
    return (blended, log_weight)

def reference(hidden_in, pre_gain, query_proj, key_proj, value_proj, out_proj, post_gain):
    normed = rms_scale(hidden_in.astype(jnp.float32), pre_gain).astype(jnp.bfloat16)
    positions = jnp.arange(TOKENS, dtype=jnp.int32).astype(jnp.float32)
    group_width = HEADS // N_TP * HEAD_DIM

    def split_cols(matrix):
        return matrix.reshape(D, N_TP, group_width).transpose(1, 0, 2)

    def one_group(summed, weights):
        w_query, w_key, w_value, w_out = weights
        queries = rotate(jnp.dot(normed, w_query, preferred_element_type=jnp.float32).reshape(TOKENS, -1, HEAD_DIM), positions).astype(jnp.bfloat16)
        key_rows = rotate(jnp.dot(normed, w_key, preferred_element_type=jnp.float32).reshape(TOKENS, -1, HEAD_DIM), positions).astype(jnp.bfloat16)
        values = jnp.dot(normed, w_value, preferred_element_type=jnp.float32).astype(jnp.bfloat16).reshape(TOKENS, -1, HEAD_DIM)
        group_outs = []
        group_levels = []
        for dilation in DILATIONS:
            outcome, levels = residue_attention(queries, key_rows, values, dilation)
            group_outs.append(outcome)
            group_levels.append(levels)
        blended, log_weight = blend(group_outs, group_levels)
        attended = blended.astype(jnp.bfloat16).reshape(TOKENS, group_width)
        partial_value = lax.optimization_barrier(jnp.dot(attended, w_out, preferred_element_type=jnp.float32).astype(jnp.bfloat16))
        return (summed + partial_value.astype(jnp.float32), log_weight)
    summed, log_weight = lax.scan(one_group, jnp.zeros((TOKENS, D), jnp.float32), (split_cols(query_proj), split_cols(key_proj), split_cols(value_proj), out_proj.reshape(N_TP, group_width, D)))
    layer_out = rms_scale(summed, post_gain).astype(jnp.bfloat16)
    return (layer_out, log_weight.reshape(HEADS, TOKENS))
```

```python
import jax
import jax.numpy as jnp
import numpy as np
from jax import lax
from jax.experimental import pallas as pl
from jax.experimental.pallas import tpu as pltpu
from jax.sharding import Mesh
from jax.sharding import PartitionSpec as P

HEAD_DIM = 64
SPAN = 128
EPS = 1e-06
ROPE_BASE = 10000.0
LOW = -1e30
SP = ("zh", "zl", "y")
Z = ("zh", "zl")
TP = ("x", "c")
F32 = jnp.float32
BF16 = jnp.bfloat16


def ring(count, steps):
    return [(i, (i + steps) % count) for i in range(count)]


def natural(i):
    return (i & 31) * 16 + ((i >> 5) & 3) * 4 + (i >> 7)


def to_residue(rows):
    i = lax.broadcasted_iota(jnp.int32, (rows, rows), 0)
    n = lax.broadcasted_iota(jnp.int32, (rows, rows), 1)
    return (natural(i) == n).astype(BF16)


def to_natural(rows):
    i = lax.broadcasted_iota(jnp.int32, (rows, rows), 1)
    n = lax.broadcasted_iota(jnp.int32, (rows, rows), 0)
    return (natural(i) == n).astype(BF16)


def rotated(x, cos, sin):
    width = x.shape[1]
    lane = lax.broadcasted_iota(jnp.int32, x.shape, 1)
    other = jnp.where((lane & 63) < 32, pltpu.roll(x, width - 32, 1), pltpu.roll(x, 32, 1))
    return x * cos + other * sin


def permuted(perm, x):
    return jnp.dot(perm, x, preferred_element_type=F32).astype(BF16)


def query_kernel(hidden_ref, gain_ref, weight_ref, cos_ref, sin_ref, normed_ref, query_ref):
    rows = hidden_ref.shape[0]
    gain = gain_ref[...]

    def step(i, carry):
        part = pl.ds(pl.multiple_of(i * 64, 64), 64)
        x = hidden_ref[part, :].astype(F32)
        scale = lax.rsqrt(jnp.mean(x * x, axis=1, keepdims=True) + EPS)
        normed_ref[part, :] = (x * scale * gain).astype(BF16)
        return carry

    lax.fori_loop(0, rows // 64, step, 0)
    query = jnp.dot(normed_ref[...], weight_ref[...], preferred_element_type=F32)
    query = rotated(query, cos_ref[...], sin_ref[...]).astype(BF16) * 0.125
    query_ref[...] = permuted(to_residue(rows), query)


def key_value_kernel(place_ref, normed_ref, mine_ref, below_ref, above_ref, cos_ref, sin_ref, key_ref, value_ref, weight_ref):
    rows = normed_ref.shape[0]
    width = key_ref.shape[1]
    low = place_ref[0]
    slabs = []
    for k in range(4):
        slabs.append((2 * k + low, mine_ref, k))
    for k in range(2):
        slabs.append((2 * k + 1 - low, below_ref, k))
        slabs.append((2 * (k + 2) + 1 - low, above_ref, k))
    for place, ref, k in slabs:
        weight_ref[pl.ds(pl.multiple_of(place * 256, 256), 256), :] = ref[k]
    normed = normed_ref[...]
    perm = to_residue(rows)
    key = jnp.dot(normed, weight_ref[:, :width], preferred_element_type=F32)
    key = rotated(key, cos_ref[...], sin_ref[...]).astype(BF16)
    key_ref[...] = permuted(perm, key)
    value = jnp.dot(normed, weight_ref[:, width:], preferred_element_type=F32).astype(BF16)
    value_ref[...] = permuted(perm, value)


def near_kernel(q_ref, k0_ref, v0_ref, k1_ref, v1_ref, bias_ref, count_ref, max_ref, sum_ref, acc_ref):
    q = q_ref[...]
    lane = lax.broadcasted_iota(jnp.int32, q.shape, 1) >> 6
    keys = k0_ref.shape[0]
    nt = (((1,), (1,)), ((), ()))
    top = jnp.zeros(q.shape, F32)
    total = jnp.zeros(q.shape, F32)
    acc = jnp.zeros(q.shape, F32)
    for head in range(q.shape[1] // HEAD_DIM):
        mine = lane == head
        qh = jnp.where(mine, q, jnp.zeros_like(q))
        s0 = lax.dot_general(qh, k0_ref[...], nt, preferred_element_type=F32) + bias_ref[0, :, :keys]
        s1 = lax.dot_general(qh, k1_ref[...], nt, preferred_element_type=F32) + bias_ref[0, :, keys:]
        m = jnp.maximum(jnp.max(s0, axis=1, keepdims=True), jnp.max(s1, axis=1, keepdims=True))
        p0 = jnp.exp(s0 - m) * count_ref[0, :, :keys]
        p1 = jnp.exp(s1 - m) * count_ref[0, :, keys:]
        l = jnp.sum(p0, axis=1, keepdims=True) + jnp.sum(p1, axis=1, keepdims=True)
        pv = jnp.dot(p0.astype(BF16), v0_ref[...], preferred_element_type=F32)
        pv = pv + jnp.dot(p1.astype(BF16), v1_ref[...], preferred_element_type=F32)
        top = jnp.where(mine, m, top)
        total = jnp.where(mine, l, total)
        acc = jnp.where(mine, pv, acc)
    max_ref[...] = top
    sum_ref[...] = total
    acc_ref[...] = acc


def far_kernel(place_ref, q_ref, max_ref, sum_ref, acc_ref, k2, v2, k3, v3, k4, v4, out_ref, log_ref, att_ref, lw_ref):
    rows, width = q_ref.shape
    block = place_ref[0]
    nt = (((1,), (1,)), ((), ()))
    qi = lax.broadcasted_iota(jnp.int32, (128, 128), 0)
    ki = lax.broadcasted_iota(jnp.int32, (128, 128), 1)
    same = (qi >> 5) == (ki >> 5)
    biases = []
    for back in (2, 3, 4):
        ok = same & (block >= back)
        if back == 4:
            ok = ok & ((ki & 31) >= (qi & 31))
        biases.append(jnp.where(ok, 0.0, LOW).astype(F32))
    lane = lax.broadcasted_iota(jnp.int32, (128, width), 1) >> 6

    def one(cls, carry):
        part = pl.ds(pl.multiple_of(cls * 128, 128), 128)
        q = q_ref[part, :]
        top, total, acc = max_ref[part, :], sum_ref[part, :], acc_ref[part, :]
        att = jnp.zeros((128, width), F32)
        lw = jnp.zeros((128, width), F32)
        for head in range(width // HEAD_DIM):
            mine = lane == head
            qh = jnp.where(mine, q, jnp.zeros_like(q))
            old = max_ref[part, :][:, head * HEAD_DIM : head * HEAD_DIM + 1]
            scores = []
            m = old
            for k, bias in zip((k2, k3, k4), biases):
                s = lax.dot_general(qh, k[part, :], nt, preferred_element_type=F32) + bias
                m = jnp.maximum(m, jnp.max(s, axis=1, keepdims=True))
                scores.append(s)
            l = jnp.zeros((128, 1), F32)
            pv = jnp.zeros((128, width), F32)
            for s, v in zip(scores, (v2, v3, v4)):
                p = jnp.exp(s - m)
                l = l + jnp.sum(p, axis=1, keepdims=True)
                pv = pv + jnp.dot(p.astype(BF16), v[part, :], preferred_element_type=F32)
            alpha = jnp.exp(top - m)
            whole = total * alpha + l
            att = jnp.where(mine, (acc * alpha + pv) / whole, att)
            lw = jnp.where(mine, m + jnp.log(whole), lw)
        att_ref[part, :] = att.astype(BF16)
        lw_ref[part, :] = lw
        return carry

    lax.fori_loop(0, rows // 128, one, 0)
    perm = to_natural(rows)
    out_ref[...] = permuted(perm, att_ref[...])
    rest = lw_ref[...]
    ordered = jnp.zeros((rows, width), F32)
    for k in range(3):
        piece = rest.astype(BF16)
        rest = rest - piece.astype(F32)
        ordered = ordered + jnp.dot(perm, piece, preferred_element_type=F32)
    flipped = ordered.T
    for head in range(width // HEAD_DIM):
        log_ref[head : head + 1, :] = flipped[head * HEAD_DIM : head * HEAD_DIM + 1, :]


def vmem(count):
    return [pl.BlockSpec(memory_space=pltpu.VMEM)] * count


SMEM = pl.BlockSpec(memory_space=pltpu.SMEM)


def cost(flops, data):
    return pl.CostEstimate(flops=flops, bytes_accessed=data, transcendentals=0)


def tables(offset, rows, width):
    half = HEAD_DIM // 2
    frequency = ROPE_BASE ** (-(jnp.arange(half, dtype=F32) * 2.0 / HEAD_DIM))
    positions = (offset + jnp.arange(rows, dtype=jnp.int32)).astype(F32)
    angles = positions[:, None] * frequency[None, :]
    cos, sin = jnp.cos(angles), jnp.sin(angles)
    heads = width // HEAD_DIM
    return jnp.tile(jnp.concatenate([cos, cos], 1), (1, heads)), jnp.tile(jnp.concatenate([-sin, sin], 1), (1, heads))


def near_masks(rows, block):
    i = jnp.arange(rows, dtype=jnp.int32)
    q = natural(i).reshape(rows // 128, 128, 1)
    k = natural(i)
    k = jnp.concatenate([k, k - rows]).reshape(1, 1, 2 * rows)
    o = q - k
    back = (o >= 0) & ((k >= 0) | (block >= 1))
    count = (o <= SPAN).astype(F32)
    count = count + (((o & 3) == 0) & (o <= 4 * SPAN)).astype(F32)
    count = count + (((o & 15) == 0) & (o <= 16 * SPAN)).astype(F32)
    count = jnp.where(back, count, 0.0)
    return jnp.where(count > 0, 0.0, LOW).astype(F32), count


def body(hidden_in, pre_gain, query_proj, key_proj, value_proj, out_proj, post_gain):
    rows, depth = hidden_in.shape
    width = query_proj.shape[1]
    shape = jax.ShapeDtypeStruct
    block = lax.axis_index(SP)
    low = lax.axis_index("zl")
    core = lax.axis_index("c")

    shard = jnp.concatenate([key_proj, value_proj], axis=1)
    copies = jnp.broadcast_to(shard[None], (32,) + shard.shape)
    mine = lax.all_to_all(copies, ("zh", "y"), split_axis=0, concat_axis=0, tiled=True)
    mine = mine.reshape(4, 256, 2 * width)
    below = lax.ppermute(mine[:2], Z, ring(8, 1))
    above = lax.ppermute(mine[2:], Z, ring(8, -1))

    cos, sin = tables(block * rows, rows, width)
    normed, query = pl.pallas_call(
        query_kernel,
        out_shape=(shape((rows, depth), BF16), shape((rows, width), BF16)),
        in_specs=vmem(5),
        out_specs=tuple(vmem(2)),
        cost_estimate=cost(2 * rows * depth * width, 4 * rows * depth),
        name="query",
    )(hidden_in, pre_gain[None], query_proj, cos, sin)

    key, value = pl.pallas_call(
        key_value_kernel,
        out_shape=(shape((rows, width), BF16),) * 2,
        in_specs=[SMEM] + vmem(6),
        out_specs=tuple(vmem(2)),
        scratch_shapes=[pltpu.VMEM((depth, 2 * width), BF16)],
        cost_estimate=cost(4 * rows * depth * width, 4 * rows * depth),
        name="key_value",
    )(low[None].astype(jnp.int32), normed, mine, below, above, cos, sin)

    forward = [(i, i + 1) for i in range(63)]
    keys, values = [key], [value]
    for back in range(4):
        keys.append(lax.ppermute(keys[-1], SP, forward))
        values.append(lax.ppermute(values[-1], SP, forward))

    bias, count = near_masks(rows, block)
    whole = pl.BlockSpec((rows, width), lambda c: (0, 0))
    piece = pl.BlockSpec((128, width), lambda c: (c, 0))
    mask = pl.BlockSpec((1, 128, 2 * rows), lambda c: (c, 0, 0))
    state = pl.pallas_call(
        near_kernel,
        grid=(rows // 128,),
        out_shape=(shape((rows, width), F32),) * 3,
        in_specs=[piece, whole, whole, whole, whole, mask, mask],
        out_specs=(piece,) * 3,
        cost_estimate=cost(8 * rows * 2 * rows * width, 4 * rows * depth),
        name="near",
    )(query, keys[0], values[0], keys[1], values[1], bias, count)

    attended, log_weight = pl.pallas_call(
        far_kernel,
        out_shape=(shape((rows, width), BF16), shape((width // HEAD_DIM, rows), F32)),
        in_specs=[SMEM] + vmem(10),
        out_specs=tuple(vmem(2)),
        scratch_shapes=[pltpu.VMEM((rows, width), BF16), pltpu.VMEM((rows, width), F32)],
        cost_estimate=cost(8 * rows * 384 * width, 4 * rows * depth),
        name="far",
    )(block[None].astype(jnp.int32), query, *state, keys[2], values[2], keys[3], values[3], keys[4], values[4])

    partial = jnp.dot(attended, out_proj, preferred_element_type=F32).astype(BF16)
    partial = partial.reshape(4, 2, rows // 8, depth)
    kept = lax.dynamic_index_in_dim(partial, core, 1, keepdims=False)
    given = lax.dynamic_index_in_dim(partial, 1 - core, 1, keepdims=False)
    taken = lax.ppermute(given, "c", [(0, 1), (1, 0)])
    pair = (kept.astype(F32) + taken.astype(F32)).astype(BF16)
    arrived = lax.all_to_all(pair, "x", split_axis=0, concat_axis=0, tiled=True)
    summed = arrived.astype(F32).sum(axis=0)
    scale = lax.rsqrt(jnp.mean(summed * summed, axis=-1, keepdims=True) + EPS)
    return (summed * scale * post_gain).astype(BF16), log_weight


def solution(mesh):
    fine = Mesh(np.asarray(mesh.devices).reshape(4, 2, 8, 4, 2), ("zh", "zl", "y", "x", "c"))
    placed = (P(SP, None), P(), P(None, TP), P(SP, TP), P(SP, TP), P(TP, None), P())
    return jax.shard_map(
        body,
        mesh=fine,
        in_specs=placed,
        out_specs=(P(SP + TP, None), P(TP, SP)),
        check_vma=False,
    )
```

```python
import functools

import jax
import jax.numpy as jnp
import numpy as np
from jax import lax
from jax.experimental import pallas as pl
from jax.experimental.pallas import tpu as pltpu
from jax.sharding import Mesh
from jax.sharding import PartitionSpec as P

HEAD_DIM = 64
SPAN = 128
EPS = 1e-06
ROPE_BASE = 10000.0
LOW = -1e30
SP = ("zh", "zl", "y")
Z = ("zh", "zl")
TP = ("x", "c")
F32 = jnp.float32
BF16 = jnp.bfloat16


def ring(count, steps):
    return [(i, (i + steps) % count) for i in range(count)]


def natural(i):
    return (i & 31) * 16 + ((i >> 5) & 3) * 4 + (i >> 7)


def to_residue(rows):
    i = lax.broadcasted_iota(jnp.int32, (rows, rows), 0)
    n = lax.broadcasted_iota(jnp.int32, (rows, rows), 1)
    return (natural(i) == n).astype(BF16)


def to_natural(rows):
    i = lax.broadcasted_iota(jnp.int32, (rows, rows), 1)
    n = lax.broadcasted_iota(jnp.int32, (rows, rows), 0)
    return (natural(i) == n).astype(BF16)


def rotated(x, cos, sin):
    width = x.shape[1]
    lane = lax.broadcasted_iota(jnp.int32, x.shape, 1)
    other = jnp.where((lane & 63) < 32, pltpu.roll(x, width - 32, 1), pltpu.roll(x, 32, 1))
    return x * cos + other * sin


def permuted(perm, x):
    return jnp.dot(perm, x, preferred_element_type=F32).astype(BF16)


def query_kernel(hidden_ref, gain_ref, weight_ref, cos_ref, sin_ref, normed_ref, query_ref):
    rows = hidden_ref.shape[0]
    gain = gain_ref[...]

    def step(i, carry):
        part = pl.ds(pl.multiple_of(i * 64, 64), 64)
        x = hidden_ref[part, :].astype(F32)
        scale = lax.rsqrt(jnp.mean(x * x, axis=1, keepdims=True) + EPS)
        normed_ref[part, :] = (x * scale * gain).astype(BF16)
        return carry

    lax.fori_loop(0, rows // 64, step, 0)
    query = jnp.dot(normed_ref[...], weight_ref[...], preferred_element_type=F32)
    query = rotated(query, cos_ref[...], sin_ref[...]).astype(BF16) * 0.125
    query_ref[...] = permuted(to_residue(rows), query)


def key_value_kernel(place_ref, normed_ref, mine_ref, below_ref, above_ref, cos_ref, sin_ref, key_ref, value_ref, weight_ref):
    rows = normed_ref.shape[0]
    width = key_ref.shape[1]
    low = place_ref[0]
    slabs = []
    for k in range(4):
        slabs.append((2 * k + low, mine_ref, k))
    for k in range(2):
        slabs.append((2 * k + 1 - low, below_ref, k))
        slabs.append((2 * (k + 2) + 1 - low, above_ref, k))
    for place, ref, k in slabs:
        weight_ref[pl.ds(pl.multiple_of(place * 256, 256), 256), :] = ref[k]
    normed = normed_ref[...]
    perm = to_residue(rows)
    key = jnp.dot(normed, weight_ref[:, :width], preferred_element_type=F32)
    key = rotated(key, cos_ref[...], sin_ref[...]).astype(BF16)
    key_ref[...] = permuted(perm, key)
    value = jnp.dot(normed, weight_ref[:, width:], preferred_element_type=F32).astype(BF16)
    value_ref[...] = permuted(perm, value)


NT = (((1,), (1,)), ((), ()))


def stack_heads(q):
    lane = lax.broadcasted_iota(jnp.int32, q.shape, 1) >> 6
    return jnp.concatenate([jnp.where(lane == h, q, jnp.zeros_like(q)) for h in range(q.shape[1] // HEAD_DIM)], axis=0)


def own_heads(stacked):
    rows, width = stacked.shape[0] // 4, stacked.shape[1]
    lane = lax.broadcasted_iota(jnp.int32, (rows, width), 1) >> 6
    out = stacked[:rows]
    for h in range(1, width // HEAD_DIM):
        out = jnp.where(lane == h, stacked[h * rows : (h + 1) * rows], out)
    return out


def near_kernel(place_ref, q_ref, k0_ref, v0_ref, k1_ref, v1_ref, max_ref, sum_ref, acc_ref, s_ref, p_ref, bias_ref, count_ref, stat_ref):
    cls = pl.program_id(0)
    keys, width = k0_ref.shape
    heads = width // HEAD_DIM
    i = lax.broadcasted_iota(jnp.int32, (128, 1), 0)
    qn = (i & 31) * 16 + (i >> 5) * 4 + cls
    kn = natural(lax.broadcasted_iota(jnp.int32, (1, keys), 1))
    seen = (place_ref[0] >= 1).astype(F32)
    for part in range(2):
        o = qn - kn + part * keys
        count = (o <= SPAN).astype(F32)
        count = count + (((o & 3) == 0) & (o <= 4 * SPAN)).astype(F32)
        count = count + ((o & 15) == 0).astype(F32)
        if part == 0:
            count = jnp.where(o >= 0, count, 0.0)
        else:
            count = count * seen
        count_ref[:, part * keys : (part + 1) * keys] = count
        bias_ref[:, part * keys : (part + 1) * keys] = jnp.where(count > 0, 0.0, LOW).astype(F32)
    q4 = stack_heads(q_ref[...])
    s_ref[:, :keys] = lax.dot_general(q4, k0_ref[...], NT, preferred_element_type=F32)
    s_ref[:, keys:] = lax.dot_general(q4, k1_ref[...], NT, preferred_element_type=F32)
    step = 32
    for r in range(0, heads * 128, step):
        mask = slice(r % 128, r % 128 + step)
        s = s_ref[r : r + step, :] + bias_ref[mask, :]
        m = jnp.max(s, axis=1, keepdims=True)
        p = jnp.exp(s - m) * count_ref[mask, :]
        stat_ref[0, r : r + step, :] = jnp.broadcast_to(m, (step, width))
        stat_ref[1, r : r + step, :] = jnp.broadcast_to(jnp.sum(p, axis=1, keepdims=True), (step, width))
        p_ref[r : r + step, :] = p.astype(BF16)
    pv = jnp.dot(p_ref[:, :keys], v0_ref[...], preferred_element_type=F32)
    pv = pv + jnp.dot(p_ref[:, keys:], v1_ref[...], preferred_element_type=F32)
    max_ref[...] = own_heads(stat_ref[0])
    sum_ref[...] = own_heads(stat_ref[1])
    acc_ref[...] = own_heads(pv)


def far_masks(block, backs):
    qi = lax.broadcasted_iota(jnp.int32, (128, 128), 0)
    ki = lax.broadcasted_iota(jnp.int32, (128, 128), 1)
    biases = []
    for back in backs:
        ok = ((qi >> 5) == (ki >> 5)) & (block >= back)
        if back == 4:
            ok = ok & ((ki & 31) >= (qi & 31))
        biases.append(jnp.where(ok, 0.0, LOW).astype(F32))
    return biases


def far_kernel(backs, last, place_ref, q_ref, max_ref, sum_ref, acc_ref, *refs):
    count = len(backs)
    width = q_ref.shape[1]
    heads = width // HEAD_DIM
    sources = [(refs[2 * n], refs[2 * n + 1]) for n in range(count)]
    outs = refs[2 * count :]
    s_ref, p_ref, stat_ref = outs[-3:]
    biases = far_masks(place_ref[0], backs)
    q4 = stack_heads(q_ref[...])
    old = [max_ref[:, h * HEAD_DIM : h * HEAD_DIM + 1] for h in range(heads)]
    for n, (k_ref, _) in enumerate(sources):
        s_ref[:, n * 128 : (n + 1) * 128] = lax.dot_general(q4, k_ref[...], NT, preferred_element_type=F32)
    for h in range(heads):
        part = slice(h * 128, (h + 1) * 128)
        scores = [s_ref[part, n * 128 : (n + 1) * 128] + biases[n] for n in range(count)]
        m = old[h]
        for s in scores:
            m = jnp.maximum(m, jnp.max(s, axis=1, keepdims=True))
        l = jnp.zeros((128, 1), F32)
        for n, s in enumerate(scores):
            p = jnp.exp(s - m)
            l = l + jnp.sum(p, axis=1, keepdims=True)
            p_ref[part, n * 128 : (n + 1) * 128] = p.astype(BF16)
        stat_ref[0, part, :] = jnp.broadcast_to(m, (128, width))
        stat_ref[1, part, :] = jnp.broadcast_to(l, (128, width))
    pv = jnp.dot(p_ref[:, :128], sources[0][1][...], preferred_element_type=F32)
    for n in range(1, count):
        pv = pv + jnp.dot(p_ref[:, n * 128 : (n + 1) * 128], sources[n][1][...], preferred_element_type=F32)
    m = own_heads(stat_ref[0])
    alpha = jnp.exp(max_ref[...] - m)
    total = sum_ref[...] * alpha + own_heads(stat_ref[1])
    acc = acc_ref[...] * alpha + own_heads(pv)
    if last:
        out_ref, log_ref, att_ref = outs[:3]
        cls = pl.program_id(0)
        att_ref[pl.ds(pl.multiple_of(cls * 128, 128), 128), :] = (acc / total).astype(BF16)
        log_ref[...] = m + jnp.log(total)

        @pl.when(cls == pl.num_programs(0) - 1)
        def _():
            out_ref[...] = permuted(to_natural(att_ref.shape[0]), att_ref[...])
    else:
        for ref, value in zip(outs[:3], (m, total, acc)):
            ref[...] = value


def log_kernel(lw_ref, log_ref):
    rows, width = lw_ref.shape
    perm = to_natural(rows)
    rest = lw_ref[...]
    ordered = jnp.zeros((rows, width), F32)
    for _ in range(3):
        piece = rest.astype(BF16)
        rest = rest - piece.astype(F32)
        ordered = ordered + jnp.dot(perm, piece, preferred_element_type=F32)
    flipped = ordered.T
    for head in range(width // HEAD_DIM):
        log_ref[head : head + 1, :] = flipped[head * HEAD_DIM : head * HEAD_DIM + 1, :]


def out_kernel(place_ref, att_ref, mine_ref, other_ref, gain_ref, out_ref, sum_ref):
    x, core = place_ref[0], place_ref[1]
    first = True
    for ref, c in ((mine_ref, core), (other_ref, 1 - core)):
        for n, hop in enumerate((0, 3, 1, 2)):
            group = lax.rem(x + hop, 4) * 2 + c
            part = jnp.dot(att_ref[group], ref[n * 256 : (n + 1) * 256, :], preferred_element_type=F32)
            part = part.astype(BF16).astype(F32)
            if first:
                sum_ref[...] = part
            else:
                sum_ref[...] += part
            first = False
    summed = sum_ref[...]
    scale = lax.rsqrt(jnp.mean(summed * summed, axis=1, keepdims=True) + EPS)
    out_ref[...] = (summed * scale * gain_ref[...]).astype(BF16)


def vmem(count):
    return [pl.BlockSpec(memory_space=pltpu.VMEM)] * count


SMEM = pl.BlockSpec(memory_space=pltpu.SMEM)


def room(mebibytes):
    return pltpu.CompilerParams(vmem_limit_bytes=mebibytes * 1024 * 1024)


def cost(flops, data):
    return pl.CostEstimate(flops=flops, bytes_accessed=data, transcendentals=0)


def tables(offset, rows, width):
    half = HEAD_DIM // 2
    frequency = ROPE_BASE ** (-(jnp.arange(half, dtype=F32) * 2.0 / HEAD_DIM))
    positions = (offset + jnp.arange(rows, dtype=jnp.int32)).astype(F32)
    angles = positions[:, None] * frequency[None, :]
    cos, sin = jnp.cos(angles), jnp.sin(angles)
    heads = width // HEAD_DIM
    return jnp.tile(jnp.concatenate([cos, cos], 1), (1, heads)), jnp.tile(jnp.concatenate([-sin, sin], 1), (1, heads))


def attend_near(block, query, keys, values):
    rows, width = query.shape
    shape = jax.ShapeDtypeStruct
    whole = pl.BlockSpec((rows, width), lambda c: (0, 0))
    piece = pl.BlockSpec((128, width), lambda c: (c, 0))
    return pl.pallas_call(
        near_kernel,
        grid=(rows // 128,),
        out_shape=(shape((rows, width), F32),) * 3,
        in_specs=[SMEM, piece, whole, whole, whole, whole],
        out_specs=(piece,) * 3,
        scratch_shapes=[
            pltpu.VMEM((512, 2 * rows), F32),
            pltpu.VMEM((512, 2 * rows), BF16),
            pltpu.VMEM((128, 2 * rows), F32),
            pltpu.VMEM((128, 2 * rows), F32),
            pltpu.VMEM((2, 512, width), F32),
        ],
        cost_estimate=cost(16 * rows * rows * width, 16 * rows * width),
        compiler_params=room(20),
        name="near",
    )(block, query, keys[0], values[0], keys[1], values[1])


def attend_far(block, query, state, keys, values, backs, last):
    rows, width = query.shape
    shape = jax.ShapeDtypeStruct
    whole = pl.BlockSpec((rows, width), lambda c: (0, 0))
    piece = pl.BlockSpec((128, width), lambda c: (c, 0))
    count = len(backs)
    if last:
        outs = (shape((rows, width), BF16), shape((rows, width), F32))
        specs = (whole, piece)
        scratch = [pltpu.VMEM((rows, width), BF16)]
    else:
        outs = (shape((rows, width), F32),) * 3
        specs = (piece,) * 3
        scratch = []
    scratch = scratch + [
        pltpu.VMEM((512, 128 * count), F32),
        pltpu.VMEM((512, 128 * count), BF16),
        pltpu.VMEM((2, 512, width), F32),
    ]
    sources = []
    for k, v in zip(keys, values):
        sources += [k, v]
    return pl.pallas_call(
        functools.partial(far_kernel, backs, last),
        grid=(rows // 128,),
        out_shape=outs,
        in_specs=[SMEM] + [piece] * (4 + 2 * count),
        out_specs=specs,
        scratch_shapes=scratch,
        cost_estimate=cost(8 * rows * 128 * count * width, 16 * rows * width),
        compiler_params=room(16),
        name="last" if last else "far",
    )(block, query, *state, *sources)


def layer(hidden_in, pre_gain, query_proj, key_proj, value_proj, out_proj, post_gain):
    rows, depth = hidden_in.shape
    width = query_proj.shape[1]
    shape = jax.ShapeDtypeStruct
    sp = lax.axis_index(SP)
    block = sp[None].astype(jnp.int32)
    low = lax.axis_index("zl")
    place = jnp.stack([lax.axis_index("x"), lax.axis_index("c")]).astype(jnp.int32)

    shard = jnp.concatenate([key_proj, value_proj], axis=1)
    copies = jnp.broadcast_to(shard[None], (32,) + shard.shape)
    mine = lax.all_to_all(copies, ("zh", "y"), split_axis=0, concat_axis=0, tiled=True)
    mine = mine.reshape(4, 256, 2 * width)
    below = lax.ppermute(mine[:2], Z, ring(8, 1))
    above = lax.ppermute(mine[2:], Z, ring(8, -1))

    before = lax.ppermute(out_proj, "x", ring(4, 1))
    after = lax.ppermute(out_proj, "x", ring(4, -1))
    upper = lax.ppermute(before[:128], "x", ring(4, 1))
    lower = lax.ppermute(after[128:], "x", ring(4, -1))
    outs = jnp.concatenate([out_proj, before, after, upper, lower], axis=0)
    others = lax.ppermute(outs, "c", [(0, 1), (1, 0)])

    cos, sin = tables(sp * rows, rows, width)
    normed, query = pl.pallas_call(
        query_kernel,
        out_shape=(shape((rows, depth), BF16), shape((rows, width), BF16)),
        in_specs=vmem(5),
        out_specs=tuple(vmem(2)),
        cost_estimate=cost(2 * rows * depth * width, 4 * rows * depth),
        compiler_params=room(16),
    name="query",
    )(hidden_in, pre_gain[None], query_proj, cos, sin)

    key, value = pl.pallas_call(
        key_value_kernel,
        out_shape=(shape((rows, width), BF16),) * 2,
        in_specs=[SMEM] + vmem(6),
        out_specs=tuple(vmem(2)),
        scratch_shapes=[pltpu.VMEM((depth, 2 * width), BF16)],
        cost_estimate=cost(4 * rows * depth * width, 4 * rows * depth),
        compiler_params=room(20),
        name="key_value",
    )(low[None].astype(jnp.int32), normed, mine, below, above, cos, sin)

    forward = [(i, i + 1) for i in range(63)]
    keys, values = [key], [value]
    for _ in range(1, 5):
        keys.append(lax.ppermute(keys[-1], SP, forward))
        values.append(lax.ppermute(values[-1], SP, forward))

    state = attend_near(block, query, keys, values)
    state = attend_far(block, query, state, keys[2:4], values[2:4], (2, 3), False)
    attended, logs = attend_far(block, query, state, keys[4:], values[4:], (4,), True)

    arrived = lax.all_to_all(attended.reshape(8, rows // 8, width), TP, split_axis=0, concat_axis=0, tiled=True)
    log_weight = pl.pallas_call(
        log_kernel,
        out_shape=shape((width // HEAD_DIM, rows), F32),
        in_specs=vmem(1),
        out_specs=vmem(1)[0],
        cost_estimate=cost(6 * rows * rows * width, 4 * rows * width),
        compiler_params=room(12),
    name="log_order",
    )(logs)
    layer_out = pl.pallas_call(
        out_kernel,
        out_shape=shape((rows // 8, depth), BF16),
        in_specs=[SMEM] + vmem(4),
        out_specs=vmem(1)[0],
        scratch_shapes=[pltpu.VMEM((rows // 8, depth), F32)],
        cost_estimate=cost(2 * rows // 8 * depth * depth, 2 * depth * depth),
        compiler_params=room(24),
        name="out",
    )(place, arrived, outs, others, post_gain[None])
    return layer_out, log_weight


def solution(mesh):
    fine = Mesh(np.asarray(mesh.devices).reshape(4, 2, 8, 4, 2), ("zh", "zl", "y", "x", "c"))
    placed = (P(SP, None), P(), P(None, TP), P(SP, TP), P(SP, TP), P(TP, None), P())
    return jax.shard_map(
        layer,
        mesh=fine,
        in_specs=placed,
        out_specs=(P(SP + TP, None), P(TP, SP)),
        check_vma=False,
    )
```

```python
import jax
import jax.numpy as jnp
import numpy as np
from jax import lax
from jax.experimental import pallas as pl
from jax.experimental.pallas import tpu as pltpu
from jax.sharding import Mesh
from jax.sharding import PartitionSpec as P

HEAD_DIM = 64
SPAN = 128
EPS = 1e-06
ROPE_BASE = 10000.0
LOW = -1e30
SP = ("zh", "zl", "y")
Z = ("zh", "zl")
TP = ("x", "c")
F32 = jnp.float32
BF16 = jnp.bfloat16
NT = (((1,), (1,)), ((), ()))
HOPS = (0, 3, 1, 2)


def ring(count, steps):
    return [(i, (i + steps) % count) for i in range(count)]


def natural(i):
    return (i & 31) * 16 + ((i >> 5) & 3) * 4 + (i >> 7)


def to_residue(rows, columns=None):
    i = lax.broadcasted_iota(jnp.int32, (rows, rows), 0)
    if columns is None:
        columns = lax.broadcasted_iota(jnp.int32, (rows, rows), 1)
    return (natural(i) == columns).astype(BF16)


def to_natural(rows):
    i = lax.broadcasted_iota(jnp.int32, (rows, rows), 1)
    n = lax.broadcasted_iota(jnp.int32, (rows, rows), 0)
    return (natural(i) == n).astype(BF16)


def rotated(x, cos, sin):
    width = x.shape[1]
    lane = lax.broadcasted_iota(jnp.int32, x.shape, 1)
    other = jnp.where((lane & 63) < 32, pltpu.roll(x, width - 32, 1), pltpu.roll(x, 32, 1))
    return x * cos + other * sin


def permuted(perm, x):
    return jnp.dot(perm, x, preferred_element_type=F32).astype(BF16)


def normed_rows(x, gain):
    x = x.astype(F32)
    scale = lax.rsqrt(jnp.mean(x * x, axis=1, keepdims=True) + EPS)
    return (x * scale * gain).astype(BF16)


def spread(turn_ref, part):
    cos, sin = turn_ref[0, :, part], turn_ref[1, :, part]
    cos = jnp.concatenate([cos] * 4, axis=0).T
    sin = jnp.concatenate([-sin, sin] * 2, axis=0).T
    return jnp.concatenate([cos, cos], axis=1), jnp.concatenate([sin, sin], axis=1)


def slice_kernel(place_ref, hidden_ref, gain_ref, out_ref):
    out_ref[...] = normed_rows(hidden_ref[...], gain_ref[...])


def query_kernel(hidden_ref, gain_ref, weight_ref, turn_ref, normed_ref, query_ref):
    rows = hidden_ref.shape[0]
    gain = gain_ref[...]

    def step(i, carry):
        part = pl.ds(pl.multiple_of(i * 64, 64), 64)
        normed_ref[part, :] = normed_rows(hidden_ref[part, :], gain)
        return carry

    lax.fori_loop(0, rows // 64, step, 0)
    query = jnp.dot(normed_ref[...], weight_ref[...], preferred_element_type=F32)
    cos, sin = spread(turn_ref, slice(2 * rows, 3 * rows))
    query = rotated(query, cos, sin).astype(BF16) * 0.125
    query_ref[...] = permuted(to_residue(rows), query)


def key_value_kernel(place_ref, normed_ref, mine_ref, below_ref, above_ref, turn_ref, key_ref, value_ref, weight_ref):
    rows = normed_ref.shape[0]
    width = key_ref.shape[1]
    low = place_ref[1]
    slabs = []
    for k in range(4):
        slabs.append((2 * k + low, mine_ref, k))
    for k in range(2):
        slabs.append((2 * k + 1 - low, below_ref, k))
        slabs.append((2 * (k + 2) + 1 - low, above_ref, k))
    for place, ref, k in slabs:
        weight_ref[pl.ds(pl.multiple_of(place * 256, 256), 256), :] = ref[k]
    normed = normed_ref[...]
    perm = to_residue(rows)
    cos, sin = spread(turn_ref, slice(2 * rows, 3 * rows))
    key = jnp.dot(normed, weight_ref[:, :width], preferred_element_type=F32)
    key = rotated(key, cos, sin).astype(BF16)
    key_ref[...] = permuted(perm, key)
    value = jnp.dot(normed, weight_ref[:, width:], preferred_element_type=F32).astype(BF16)
    value_ref[...] = permuted(perm, value)


def far_key_value_kernel(place_ref, mine_ref, other_ref, weight_ref, turn_ref, k4_ref, v4_ref, k3_ref, v3_ref, cos_ref, sin_ref, key_ref, value_ref):
    rows, width = k4_ref.shape
    x, core = place_ref[2], place_ref[3]
    piece = rows // 8
    for n in range(2):
        part = slice(n * rows, (n + 1) * rows)
        cos_ref[part, :], sin_ref[part, :] = spread(turn_ref, part)
    lanes = lax.broadcasted_iota(jnp.int32, (1, rows), 1)
    column = lanes & (piece - 1)
    for half, (ref, c) in enumerate(((mine_ref, core), (other_ref, 1 - core))):
        both = jnp.dot(ref[...], weight_ref[...], preferred_element_type=F32)
        for n, hop in enumerate(HOPS):
            at = (lax.rem(x + hop, 4) * 2 + c) * piece
            lies = (half * 4 + n) * piece
            column = column + jnp.where((lanes >= lies) & (lanes < lies + piece), at, 0)
            for far in range(2):
                source = slice((2 * n + far) * piece, (2 * n + far + 1) * piece)
                table = pl.ds(pl.multiple_of(far * rows + at, piece), piece)
                key = rotated(both[source, :width], cos_ref[table, :], sin_ref[table, :])
                key_ref[far, lies : lies + piece, :] = key.astype(BF16)
                value_ref[far, lies : lies + piece, :] = both[source, width:].astype(BF16)
    perm = to_residue(rows, jnp.broadcast_to(column, (rows, rows)))
    k4_ref[...] = permuted(perm, key_ref[0])
    v4_ref[...] = permuted(perm, value_ref[0])
    k3_ref[...] = permuted(perm, key_ref[1])
    v3_ref[...] = permuted(perm, value_ref[1])


def stack_heads(q):
    lane = lax.broadcasted_iota(jnp.int32, q.shape, 1) >> 6
    return jnp.concatenate([jnp.where(lane == h, q, jnp.zeros_like(q)) for h in range(q.shape[1] // HEAD_DIM)], axis=0)


def own_heads(stacked):
    width = stacked.shape[1]
    heads = width // HEAD_DIM
    rows = stacked.shape[0] // heads
    lane = lax.broadcasted_iota(jnp.int32, (rows, width), 1) >> 6
    out = stacked[:rows]
    for h in range(1, heads):
        out = jnp.where(lane == h, stacked[h * rows : (h + 1) * rows], out)
    return out


def far_bias(block, back):
    qi = lax.broadcasted_iota(jnp.int32, (128, 128), 0)
    ki = lax.broadcasted_iota(jnp.int32, (128, 128), 1)
    ok = ((qi >> 5) == (ki >> 5)) & (block >= back)
    if back == 4:
        ok = ok & ((ki & 31) >= (qi & 31))
    return jnp.where(ok, 0.0, LOW).astype(F32)


def near_kernel(place_ref, q_ref, k0_ref, v0_ref, k1_ref, v1_ref, k3_ref, v3_ref, k4_ref, v4_ref, max_ref, sum_ref, acc_ref, s_ref, p_ref, bias_ref, count_ref, stat_ref, tail_ref):
    cls = pl.program_id(0)
    block = place_ref[0]
    keys, width = k0_ref.shape
    heads = width // HEAD_DIM
    mine = pl.ds(pl.multiple_of(cls * 128, 128), 128)

    @pl.when(cls == 0)
    def _():
        j = lax.broadcasted_iota(jnp.int32, (128, keys), 0)
        i = lax.broadcasted_iota(jnp.int32, (128, keys), 1)
        pick = (i == (j >> 3) * 32 + 24 + (j & 7)).astype(BF16)
        tail_ref[0] = permuted(pick, k1_ref[...])
        tail_ref[1] = permuted(pick, v1_ref[...])
        bias_ref[:, keys + 256 : keys + 384] = far_bias(block, 3)
        bias_ref[:, keys + 384 : keys + 512] = far_bias(block, 4)

    i = lax.broadcasted_iota(jnp.int32, (128, 1), 0)
    qn = (i & 31) * 16 + (i >> 5) * 4 + cls
    seen = block >= 1
    for lies, size in ((0, keys), (keys, 128)):
        k = lax.broadcasted_iota(jnp.int32, (1, size), 1)
        if lies == 0:
            o = qn - natural(k)
        else:
            o = qn - ((k & 31) * 16 + (k >> 5) * 4 + cls) + keys
        count = (o <= SPAN).astype(F32)
        count = count + (((o & 3) == 0) & (o <= 4 * SPAN)).astype(F32)
        count = count + ((o & 15) == 0).astype(F32)
        if lies == 0:
            count = jnp.where(o >= 0, count, 0.0)
        else:
            count = jnp.where(seen, count, 0.0)
        count_ref[:, lies : lies + size] = count
        bias_ref[:, lies : lies + size] = jnp.where(count > 0, 0.0, LOW).astype(F32)
    k = lax.broadcasted_iota(jnp.int32, (1, 128), 1)
    o = qn - ((24 + (k & 7)) * 16 + ((k >> 3) & 3) * 4 + (k >> 5)) + keys
    ok = (o <= SPAN) & ((k >> 5) != cls) & seen
    bias_ref[:, keys + 128 : keys + 256] = jnp.where(ok, 0.0, LOW).astype(F32)

    q4 = stack_heads(q_ref[...])
    s_ref[:, :keys] = lax.dot_general(q4, k0_ref[...], NT, preferred_element_type=F32)
    rest = jnp.concatenate([k1_ref[mine, :], tail_ref[0], k3_ref[mine, :], k4_ref[mine, :]], axis=0)
    s_ref[:, keys:] = lax.dot_general(q4, rest, NT, preferred_element_type=F32)
    step = 32
    for r in range(0, heads * 128, step):
        mask = slice(r % 128, r % 128 + step)
        s = s_ref[r : r + step, :] + bias_ref[mask, :]
        m = jnp.max(s, axis=1, keepdims=True)
        p = jnp.exp(s - m)
        p = jnp.concatenate([p[:, : keys + 128] * count_ref[mask, :], p[:, keys + 128 :]], axis=1)
        stat_ref[0, r : r + step, :] = jnp.broadcast_to(m, (step, width))
        stat_ref[1, r : r + step, :] = jnp.broadcast_to(jnp.sum(p, axis=1, keepdims=True), (step, width))
        p_ref[r : r + step, :] = p.astype(BF16)
    pv = jnp.dot(p_ref[:, :keys], v0_ref[...], preferred_element_type=F32)
    rest = jnp.concatenate([v1_ref[mine, :], tail_ref[1], v3_ref[mine, :], v4_ref[mine, :]], axis=0)
    pv = pv + jnp.dot(p_ref[:, keys:], rest, preferred_element_type=F32)
    max_ref[...] = own_heads(stat_ref[0])
    sum_ref[...] = own_heads(stat_ref[1])
    acc_ref[...] = own_heads(pv)


def last_kernel(place_ref, q_ref, max_ref, sum_ref, acc_ref, k_ref, v_ref, out_ref, log_ref, att_ref, s_ref, p_ref, stat_ref):
    width = q_ref.shape[1]
    heads = width // HEAD_DIM
    bias = far_bias(place_ref[0], 2)
    s_ref[...] = lax.dot_general(stack_heads(q_ref[...]), k_ref[...], NT, preferred_element_type=F32)
    for h in range(heads):
        part = slice(h * 128, (h + 1) * 128)
        s = s_ref[part, :] + bias
        m = jnp.maximum(jnp.max(s, axis=1, keepdims=True), max_ref[:, h * HEAD_DIM : h * HEAD_DIM + 1])
        p = jnp.exp(s - m)
        p_ref[part, :] = p.astype(BF16)
        stat_ref[0, part, :] = jnp.broadcast_to(m, (128, width))
        stat_ref[1, part, :] = jnp.broadcast_to(jnp.sum(p, axis=1, keepdims=True), (128, width))
    pv = jnp.dot(p_ref[...], v_ref[...], preferred_element_type=F32)
    m = own_heads(stat_ref[0])
    alpha = jnp.exp(max_ref[...] - m)
    total = sum_ref[...] * alpha + own_heads(stat_ref[1])
    acc = acc_ref[...] * alpha + own_heads(pv)
    cls = pl.program_id(0)
    att_ref[pl.ds(pl.multiple_of(cls * 128, 128), 128), :] = (acc / total).astype(BF16)
    log_ref[...] = m + jnp.log(total)

    @pl.when(cls == pl.num_programs(0) - 1)
    def _():
        out_ref[...] = permuted(to_natural(att_ref.shape[0]), att_ref[...])


def log_kernel(lw_ref, log_ref):
    rows, width = lw_ref.shape
    perm = to_natural(rows)
    rest = lw_ref[...]
    ordered = jnp.zeros((rows, width), F32)
    for _ in range(3):
        piece = rest.astype(BF16)
        rest = rest - piece.astype(F32)
        ordered = ordered + jnp.dot(perm, piece, preferred_element_type=F32)
    flipped = ordered.T
    for head in range(width // HEAD_DIM):
        log_ref[head : head + 1, :] = flipped[head * HEAD_DIM : head * HEAD_DIM + 1, :]


def out_kernel(place_ref, att_ref, own_ref, before_ref, after_ref, upper_ref, lower_ref, keep_ref, give_ref, sum_ref):
    x, core = place_ref[2], place_ref[3]
    half = own_ref.shape[0] // 2
    rows = keep_ref.shape[0]
    for n, ref in enumerate((own_ref, before_ref, after_ref, None)):
        att = att_ref[lax.rem(x + HOPS[n], 4)]
        if ref is None:
            part = jnp.dot(att[:, :half], upper_ref[...], preferred_element_type=F32)
            part = part + jnp.dot(att[:, half:], lower_ref[...], preferred_element_type=F32)
        else:
            part = jnp.dot(att, ref[...], preferred_element_type=F32)
        part = part.astype(BF16).astype(F32)
        if n == 0:
            sum_ref[...] = part
        else:
            sum_ref[...] += part
    keep_ref[...] = sum_ref[pl.ds(pl.multiple_of(core * rows, rows), rows), :]
    give_ref[...] = sum_ref[pl.ds(pl.multiple_of((1 - core) * rows, rows), rows), :].astype(BF16)


def end_kernel(keep_ref, taken_ref, gain_ref, out_ref):
    summed = keep_ref[...] + taken_ref[...].astype(F32)
    scale = lax.rsqrt(jnp.mean(summed * summed, axis=1, keepdims=True) + EPS)
    out_ref[...] = (summed * scale * gain_ref[...]).astype(BF16)


SMEM = pl.BlockSpec(memory_space=pltpu.SMEM)
VMEM = pl.BlockSpec(memory_space=pltpu.VMEM)


def kernel_call(body, outs, args, flops, limit, scratch=(), **more):
    if "grid_spec" not in more:
        more["scratch_shapes"] = [pltpu.VMEM(s, t) for s, t in scratch]
    if "in_specs" not in more and "grid_spec" not in more:
        more["in_specs"] = [SMEM if a.dtype == jnp.int32 else VMEM for a in args]
        more["out_specs"] = tuple(VMEM for _ in outs)
    data = sum(a.size * a.dtype.itemsize for a in args)
    return pl.pallas_call(
        body,
        out_shape=tuple(jax.ShapeDtypeStruct(s, t) for s, t in outs),
        compiler_params=pltpu.CompilerParams(vmem_limit_bytes=limit * 1024 * 1024),
        cost_estimate=pl.CostEstimate(flops=flops, bytes_accessed=data, transcendentals=0),
        **more,
    )(*args)


def layer(hidden_in, pre_gain, query_proj, key_proj, value_proj, out_proj, post_gain):
    rows, depth = hidden_in.shape
    width = query_proj.shape[1]
    heads = width // HEAD_DIM
    sp, x, core = lax.axis_index(SP), lax.axis_index("x"), lax.axis_index("c")
    place = jnp.stack([sp, lax.axis_index("zl"), x, core]).astype(jnp.int32)
    member = (x * 2 + core)[None].astype(jnp.int32)
    gain = pre_gain[None]
    row = (rows, width)

    shard = jnp.concatenate([key_proj, value_proj], axis=1)
    copies = jnp.broadcast_to(shard[None], (32,) + shard.shape)
    mine = lax.all_to_all(copies, ("zh", "y"), split_axis=0, concat_axis=0, tiled=True)
    mine = mine.reshape(4, 256, 2 * width)
    below = lax.ppermute(mine[:2], Z, ring(8, 1))
    above = lax.ppermute(mine[2:], Z, ring(8, -1))

    piece = rows // 8
    (eighth,) = kernel_call(
        slice_kernel,
        [((piece, depth), BF16)],
        (member, hidden_in, gain),
        10 * piece * depth,
        12,
        grid_spec=pltpu.PrefetchScalarGridSpec(
            num_scalar_prefetch=1,
            grid=(1,),
            in_specs=[pl.BlockSpec((piece, depth), lambda i, t: (t[0], 0)), pl.BlockSpec((1, depth), lambda i, t: (0, 0))],
            out_specs=[pl.BlockSpec((piece, depth), lambda i, t: (0, 0))],
        ),
    )
    fourth = lax.ppermute(eighth, SP, ring(64, 4))
    third = lax.ppermute(fourth, SP, ring(64, -1))
    both = jnp.concatenate([fourth, third], axis=0)
    left = lax.ppermute(both, "x", ring(4, 1))
    right = lax.ppermute(both, "x", ring(4, -1))
    across4 = lax.ppermute(left[:piece], "x", ring(4, 1))
    across3 = lax.ppermute(right[piece:], "x", ring(4, -1))
    far_rows = jnp.concatenate([both, left, right, across4, across3], axis=0)
    far_others = lax.ppermute(far_rows, "c", ring(2, 1))

    before = lax.ppermute(out_proj, "x", ring(4, 1))
    after = lax.ppermute(out_proj, "x", ring(4, -1))
    upper = lax.ppermute(before[: width // 2], "x", ring(4, 1))
    lower = lax.ppermute(after[width // 2 :], "x", ring(4, -1))

    half = HEAD_DIM // 2
    frequency = ROPE_BASE ** (-(jnp.arange(half, dtype=F32) * 2.0 / HEAD_DIM))
    local = jnp.arange(rows, dtype=jnp.int32)
    positions = jnp.concatenate([(sp - 4) * rows + local, (sp - 3) * rows + local, sp * rows + local]).astype(F32)
    angles = positions[None, :] * frequency[:, None]
    turns = jnp.stack([jnp.cos(angles), jnp.sin(angles)])

    normed, query = kernel_call(
        query_kernel, [((rows, depth), BF16), (row, BF16)], (hidden_in, gain, query_proj, turns), 2 * rows * depth * width, 16
    )
    key, value, weights = kernel_call(
        key_value_kernel,
        [(row, BF16), (row, BF16), ((depth, 2 * width), BF16)],
        (place, normed, mine, below, above, turns),
        4 * rows * depth * width,
        20,
    )

    forward = [(i, i + 1) for i in range(63)]
    key1 = lax.ppermute(key, SP, forward)
    value1 = lax.ppermute(value, SP, forward)
    key2 = lax.ppermute(key1, SP, forward)
    value2 = lax.ppermute(value1, SP, forward)

    key4, value4, key3, value3 = kernel_call(
        far_key_value_kernel,
        [(row, BF16)] * 4,
        (place, far_rows, far_others, weights, turns),
        8 * rows * depth * width,
        24,
        [((2 * rows, width), F32), ((2 * rows, width), F32), ((2,) + row, BF16), ((2,) + row, BF16)],
    )

    whole = pl.BlockSpec(row, lambda c: (0, 0))
    part = pl.BlockSpec((128, width), lambda c: (c, 0))
    state = kernel_call(
        near_kernel,
        [(row, F32)] * 3,
        (place, query, key, value, key1, value1, key3, value3, key4, value4),
        16 * rows * rows * width,
        24,
        [((512, 1024), F32), ((512, 1024), BF16), ((128, 1024), F32), ((128, 640), F32), ((2, 512, width), F32), ((2, 128, width), BF16)],
        grid=(rows // 128,),
        in_specs=[SMEM, part] + [whole] * 8,
        out_specs=(part,) * 3,
    )
    attended, logs = kernel_call(
        last_kernel,
        [(row, BF16), (row, F32)],
        (place, query, *state, key2, value2),
        4 * rows * 512 * width,
        16,
        [(row, BF16), ((512, 128), F32), ((512, 128), BF16), ((2, 512, width), F32)],
        grid=(rows // 128,),
        in_specs=[SMEM] + [part] * 6,
        out_specs=(whole, part),
    )

    arrived = lax.all_to_all(attended.reshape(4, rows // 4, width), "x", split_axis=0, concat_axis=0, tiled=True)
    (log_weight,) = kernel_call(log_kernel, [((heads, rows), F32)], (logs,), 6 * rows * rows * width, 12)
    keep, give = kernel_call(
        out_kernel,
        [((piece, depth), F32), ((piece, depth), BF16)],
        (place, arrived, out_proj, before, after, upper, lower),
        2 * rows // 8 * depth * depth,
        20,
        [((2 * piece, depth), F32)],
    )
    taken = lax.ppermute(give, "c", ring(2, 1))
    (layer_out,) = kernel_call(end_kernel, [((piece, depth), BF16)], (keep, taken, post_gain[None]), 10 * piece * depth, 8)
    return layer_out, log_weight


def solution(mesh):
    fine = Mesh(np.asarray(mesh.devices).reshape(4, 2, 8, 4, 2), ("zh", "zl", "y", "x", "c"))
    placed = (P(SP, None), P(), P(None, TP), P(SP, TP), P(SP, TP), P(TP, None), P())
    return jax.shard_map(
        layer,
        mesh=fine,
        in_specs=placed,
        out_specs=(P(SP + TP, None), P(TP, SP)),
        check_vma=False,
    )
```

```python
import functools

import jax
import jax.numpy as jnp
import numpy as np
from jax import lax
from jax.experimental import pallas as pl
from jax.experimental.pallas import tpu as pltpu
from jax.sharding import Mesh
from jax.sharding import PartitionSpec as P

HEAD_DIM = 64
SPAN = 128
EPS = 1e-06
ROPE_BASE = 10000.0
LOW = -1e30
SP = ("zh", "zl", "y")
Z = ("zh", "zl")
TP = ("x", "c")
F32 = jnp.float32
BF16 = jnp.bfloat16
NT = (((1,), (1,)), ((), ()))
HOPS = (0, 3, 1, 2)


def ring(count, steps):
    return [(i, (i + steps) % count) for i in range(count)]


def natural(i):
    return (i & 31) * 16 + ((i >> 5) & 3) * 4 + (i >> 7)


def to_residue(rows, columns=None):
    i = lax.broadcasted_iota(jnp.int32, (rows, rows), 0)
    if columns is None:
        columns = lax.broadcasted_iota(jnp.int32, (rows, rows), 1)
    return (natural(i) == columns).astype(BF16)


def to_natural(rows):
    i = lax.broadcasted_iota(jnp.int32, (rows, rows), 1)
    n = lax.broadcasted_iota(jnp.int32, (rows, rows), 0)
    return (natural(i) == n).astype(BF16)


def rotated(x, cos, sin):
    width = x.shape[1]
    lane = lax.broadcasted_iota(jnp.int32, x.shape, 1)
    other = jnp.where((lane & 63) < 32, pltpu.roll(x, width - 32, 1), pltpu.roll(x, 32, 1))
    return x * cos + other * sin


def permuted(perm, x):
    return jnp.dot(perm, x, preferred_element_type=F32).astype(BF16)


def normed_rows(x, gain):
    x = x.astype(F32)
    scale = lax.rsqrt(jnp.mean(x * x, axis=1, keepdims=True) + EPS)
    return (x * scale * gain).astype(BF16)


def spread(turn_ref, part):
    cos, sin = turn_ref[0, :, part], turn_ref[1, :, part]
    cos = jnp.concatenate([cos] * 4, axis=0).T
    sin = jnp.concatenate([-sin, sin] * 2, axis=0).T
    return jnp.concatenate([cos, cos], axis=1), jnp.concatenate([sin, sin], axis=1)


def slice_kernel(place_ref, hidden_ref, gain_ref, out_ref):
    out_ref[...] = normed_rows(hidden_ref[...], gain_ref[...])


def query_kernel(hidden_ref, gain_ref, weight_ref, turn_ref, normed_ref, query_ref):
    rows = hidden_ref.shape[0]
    gain = gain_ref[...]

    def step(i, carry):
        part = pl.ds(pl.multiple_of(i * 64, 64), 64)
        normed_ref[part, :] = normed_rows(hidden_ref[part, :], gain)
        return carry

    lax.fori_loop(0, rows // 64, step, 0)
    query = jnp.dot(normed_ref[...], weight_ref[...], preferred_element_type=F32)
    cos, sin = spread(turn_ref, slice(rows, 2 * rows))
    query = rotated(query, cos, sin).astype(BF16) * 0.125
    query_ref[...] = permuted(to_residue(rows), query)


def project(normed, weight_ref, cos, sin, key_ref, value_ref):
    rows, width = key_ref.shape
    perm = to_residue(rows)
    key = jnp.dot(normed, weight_ref[:, :width], preferred_element_type=F32)
    key_ref[...] = permuted(perm, rotated(key, cos, sin).astype(BF16))
    value = jnp.dot(normed, weight_ref[:, width:], preferred_element_type=F32).astype(BF16)
    value_ref[...] = permuted(perm, value)


def key_value_kernel(place_ref, normed_ref, mine_ref, below_ref, above_ref, turn_ref, key_ref, value_ref, weight_ref):
    rows = normed_ref.shape[0]
    low = place_ref[1]
    slabs = []
    for k in range(4):
        slabs.append((2 * k + low, mine_ref, k))
    for k in range(2):
        slabs.append((2 * k + 1 - low, below_ref, k))
        slabs.append((2 * (k + 2) + 1 - low, above_ref, k))
    for place, ref, k in slabs:
        weight_ref[pl.ds(pl.multiple_of(place * 256, 256), 256), :] = ref[k]
    project(normed_ref[...], weight_ref, *spread(turn_ref, slice(rows, 2 * rows)), key_ref, value_ref)


def far_key_value_kernel(normed_ref, weight_ref, turn_ref, key_ref, value_ref):
    project(normed_ref[...], weight_ref, *spread(turn_ref, slice(0, normed_ref.shape[0])), key_ref, value_ref)


def stack_heads(q):
    lane = lax.broadcasted_iota(jnp.int32, q.shape, 1) >> 6
    return jnp.concatenate([jnp.where(lane == h, q, jnp.zeros_like(q)) for h in range(q.shape[1] // HEAD_DIM)], axis=0)


def own_heads(stacked):
    width = stacked.shape[1]
    heads = width // HEAD_DIM
    rows = stacked.shape[0] // heads
    lane = lax.broadcasted_iota(jnp.int32, (rows, width), 1) >> 6
    out = stacked[:rows]
    for h in range(1, heads):
        out = jnp.where(lane == h, stacked[h * rows : (h + 1) * rows], out)
    return out


def far_bias(block, back):
    qi = lax.broadcasted_iota(jnp.int32, (128, 128), 0)
    ki = lax.broadcasted_iota(jnp.int32, (128, 128), 1)
    ok = ((qi >> 5) == (ki >> 5)) & (block >= back)
    if back == 4:
        ok = ok & ((ki & 31) >= (qi & 31))
    return jnp.where(ok, 0.0, LOW).astype(F32)


def near_kernel(place_ref, q_ref, k0_ref, v0_ref, k1_ref, v1_ref, max_ref, sum_ref, acc_ref, s_ref, p_ref, bias_ref, count_ref, stat_ref, tail_ref):
    cls = pl.program_id(0)
    block = place_ref[0]
    keys, width = k0_ref.shape
    heads = width // HEAD_DIM
    mine = pl.ds(pl.multiple_of(cls * 128, 128), 128)

    @pl.when(cls == 0)
    def _():
        j = lax.broadcasted_iota(jnp.int32, (128, keys), 0)
        i = lax.broadcasted_iota(jnp.int32, (128, keys), 1)
        pick = (i == (j >> 3) * 32 + 24 + (j & 7)).astype(BF16)
        tail_ref[0] = permuted(pick, k1_ref[...])
        tail_ref[1] = permuted(pick, v1_ref[...])

    i = lax.broadcasted_iota(jnp.int32, (128, 1), 0)
    qn = (i & 31) * 16 + (i >> 5) * 4 + cls
    seen = block >= 1
    for lies, size in ((0, keys), (keys, 128)):
        k = lax.broadcasted_iota(jnp.int32, (1, size), 1)
        if lies == 0:
            o = qn - natural(k)
        else:
            o = qn - ((k & 31) * 16 + (k >> 5) * 4 + cls) + keys
        count = (o <= SPAN).astype(F32)
        count = count + (((o & 3) == 0) & (o <= 4 * SPAN)).astype(F32)
        count = count + ((o & 15) == 0).astype(F32)
        if lies == 0:
            count = jnp.where(o >= 0, count, 0.0)
        else:
            count = jnp.where(seen, count, 0.0)
        count_ref[:, lies : lies + size] = count
        bias_ref[:, lies : lies + size] = jnp.where(count > 0, 0.0, LOW).astype(F32)
    k = lax.broadcasted_iota(jnp.int32, (1, 128), 1)
    o = qn - ((24 + (k & 7)) * 16 + ((k >> 3) & 3) * 4 + (k >> 5)) + keys
    ok = (o <= SPAN) & ((k >> 5) != cls) & seen
    bias_ref[:, keys + 128 :] = jnp.where(ok, 0.0, LOW).astype(F32)

    stacked = stack_heads(q_ref[...])
    s_ref[:, :keys] = lax.dot_general(stacked, k0_ref[...], NT, preferred_element_type=F32)
    rest = jnp.concatenate([k1_ref[mine, :], tail_ref[0]], axis=0)
    s_ref[:, keys:] = lax.dot_general(stacked, rest, NT, preferred_element_type=F32)
    step = 32
    for r in range(0, heads * 128, step):
        mask = slice(r % 128, r % 128 + step)
        s = s_ref[r : r + step, :] + bias_ref[mask, :]
        m = jnp.max(s, axis=1, keepdims=True)
        p = jnp.exp(s - m)
        p = jnp.concatenate([p[:, : keys + 128] * count_ref[mask, :], p[:, keys + 128 :]], axis=1)
        stat_ref[0, r : r + step, :] = jnp.broadcast_to(m, (step, width))
        stat_ref[1, r : r + step, :] = jnp.broadcast_to(jnp.sum(p, axis=1, keepdims=True), (step, width))
        p_ref[r : r + step, :] = p.astype(BF16)
    pv = jnp.dot(p_ref[:, :keys], v0_ref[...], preferred_element_type=F32)
    rest = jnp.concatenate([v1_ref[mine, :], tail_ref[1]], axis=0)
    pv = pv + jnp.dot(p_ref[:, keys:], rest, preferred_element_type=F32)
    max_ref[...] = own_heads(stat_ref[0])
    sum_ref[...] = own_heads(stat_ref[1])
    acc_ref[...] = own_heads(pv)


def far_kernel(backs, last, place_ref, q_ref, max_ref, sum_ref, acc_ref, *refs):
    width = q_ref.shape[1]
    heads = width // HEAD_DIM
    count = len(backs)
    sources, outs = refs[: 2 * count], refs[2 * count :]
    p_ref, stat_ref = outs[-2:]
    bias = jnp.concatenate([far_bias(place_ref[0], back) for back in backs], axis=1)
    key = jnp.concatenate([ref[...] for ref in sources[0::2]], axis=0)
    value = jnp.concatenate([ref[...] for ref in sources[1::2]], axis=0)
    scores = lax.dot_general(stack_heads(q_ref[...]), key, NT, preferred_element_type=F32)
    for h in range(heads):
        part = slice(h * 128, (h + 1) * 128)
        s = scores[part] + bias
        m = jnp.maximum(jnp.max(s, axis=1, keepdims=True), max_ref[:, h * HEAD_DIM : h * HEAD_DIM + 1])
        p = jnp.exp(s - m)
        p_ref[part, :] = p.astype(BF16)
        stat_ref[0, part, :] = jnp.broadcast_to(m, (128, width))
        stat_ref[1, part, :] = jnp.broadcast_to(jnp.sum(p, axis=1, keepdims=True), (128, width))
    pv = jnp.dot(p_ref[...], value, preferred_element_type=F32)
    m = own_heads(stat_ref[0])
    alpha = jnp.exp(max_ref[...] - m)
    total = sum_ref[...] * alpha + own_heads(stat_ref[1])
    acc = acc_ref[...] * alpha + own_heads(pv)
    if last:
        cls = pl.program_id(0)
        out_ref, log_ref, att_ref = outs[:3]
        att_ref[pl.ds(pl.multiple_of(cls * 128, 128), 128), :] = (acc / total).astype(BF16)
        log_ref[...] = m + jnp.log(total)

        @pl.when(cls == pl.num_programs(0) - 1)
        def _():
            out_ref[...] = permuted(to_natural(att_ref.shape[0]), att_ref[...])
    else:
        for ref, value in zip(outs[:3], (m, total, acc)):
            ref[...] = value


def log_kernel(lw_ref, log_ref):
    rows, width = lw_ref.shape
    perm = to_natural(rows)
    rest = lw_ref[...]
    ordered = jnp.zeros((rows, width), F32)
    for _ in range(3):
        piece = rest.astype(BF16)
        rest = rest - piece.astype(F32)
        ordered = ordered + jnp.dot(perm, piece, preferred_element_type=F32)
    flipped = ordered.T
    for head in range(width // HEAD_DIM):
        log_ref[head : head + 1, :] = flipped[head * HEAD_DIM : head * HEAD_DIM + 1, :]


def out_kernel(place_ref, att_ref, own_ref, before_ref, after_ref, upper_ref, lower_ref, keep_ref, give_ref, sum_ref):
    x, core = place_ref[2], place_ref[3]
    half = own_ref.shape[0] // 2
    rows = keep_ref.shape[0]
    for n, ref in enumerate((own_ref, before_ref, after_ref, None)):
        att = att_ref[lax.rem(x + HOPS[n], 4)]
        if ref is None:
            part = jnp.dot(att[:, :half], upper_ref[...], preferred_element_type=F32)
            part = part + jnp.dot(att[:, half:], lower_ref[...], preferred_element_type=F32)
        else:
            part = jnp.dot(att, ref[...], preferred_element_type=F32)
        part = part.astype(BF16).astype(F32)
        if n == 0:
            sum_ref[...] = part
        else:
            sum_ref[...] += part
    keep_ref[...] = sum_ref[pl.ds(pl.multiple_of(core * rows, rows), rows), :]
    give_ref[...] = sum_ref[pl.ds(pl.multiple_of((1 - core) * rows, rows), rows), :].astype(BF16)


def end_kernel(keep_ref, taken_ref, gain_ref, out_ref):
    summed = keep_ref[...] + taken_ref[...].astype(F32)
    scale = lax.rsqrt(jnp.mean(summed * summed, axis=1, keepdims=True) + EPS)
    out_ref[...] = (summed * scale * gain_ref[...]).astype(BF16)


SMEM = pl.BlockSpec(memory_space=pltpu.SMEM)
VMEM = pl.BlockSpec(memory_space=pltpu.VMEM)


def kernel_call(body, outs, args, flops, limit, scratch=(), **more):
    if "grid_spec" not in more:
        more["scratch_shapes"] = [pltpu.VMEM(s, t) for s, t in scratch]
    if "in_specs" not in more and "grid_spec" not in more:
        more["in_specs"] = [SMEM if a.dtype == jnp.int32 else VMEM for a in args]
        more["out_specs"] = tuple(VMEM for _ in outs)
    data = sum(a.size * a.dtype.itemsize for a in args)
    return pl.pallas_call(
        body,
        out_shape=tuple(jax.ShapeDtypeStruct(s, t) for s, t in outs),
        compiler_params=pltpu.CompilerParams(vmem_limit_bytes=limit * 1024 * 1024),
        cost_estimate=pl.CostEstimate(flops=flops, bytes_accessed=data, transcendentals=0),
        **more,
    )(*args)


def spread_to(value, axis, count):
    copies = jnp.broadcast_to(value[None], (count,) + value.shape)
    return lax.all_to_all(copies, axis, split_axis=0, concat_axis=0, tiled=True)


def layer(hidden_in, pre_gain, query_proj, key_proj, value_proj, out_proj, post_gain):
    rows, depth = hidden_in.shape
    width = query_proj.shape[1]
    heads = width // HEAD_DIM
    piece = rows // 8
    sp, x, core = lax.axis_index(SP), lax.axis_index("x"), lax.axis_index("c")
    place = jnp.stack([sp, lax.axis_index("zl"), x, core]).astype(jnp.int32)
    member = (x * 2 + core)[None].astype(jnp.int32)
    gain = pre_gain[None]
    row = (rows, width)

    shard = jnp.concatenate([key_proj, value_proj], axis=1)
    mine = spread_to(shard, ("zh", "y"), 32).reshape(4, 256, 2 * width)
    below = lax.ppermute(mine[:2], Z, ring(8, 1))
    above = lax.ppermute(mine[2:], Z, ring(8, -1))

    (eighth,) = kernel_call(
        slice_kernel,
        [((piece, depth), BF16)],
        (member, hidden_in, gain),
        10 * piece * depth,
        12,
        grid_spec=pltpu.PrefetchScalarGridSpec(
            num_scalar_prefetch=1,
            grid=(1,),
            in_specs=[pl.BlockSpec((piece, depth), lambda i, t: (t[0], 0)), pl.BlockSpec((1, depth), lambda i, t: (0, 0))],
            out_specs=[pl.BlockSpec((piece, depth), lambda i, t: (0, 0))],
        ),
    )
    fourth = lax.ppermute(eighth, SP, ring(64, 4))
    far_rows = spread_to(fourth, TP, 8).reshape(rows, depth)

    before = lax.ppermute(out_proj, "x", ring(4, 1))
    after = lax.ppermute(out_proj, "x", ring(4, -1))
    upper = lax.ppermute(before[: width // 2], "x", ring(4, 1))
    lower = lax.ppermute(after[width // 2 :], "x", ring(4, -1))

    quarter = HEAD_DIM // 2
    frequency = ROPE_BASE ** (-(jnp.arange(quarter, dtype=F32) * 2.0 / HEAD_DIM))
    local = jnp.arange(rows, dtype=jnp.int32)
    positions = jnp.concatenate([(sp - 4) * rows + local, sp * rows + local]).astype(F32)
    angles = positions[None, :] * frequency[:, None]
    turns = jnp.stack([jnp.cos(angles), jnp.sin(angles)])

    normed, query = kernel_call(
        query_kernel, [((rows, depth), BF16), (row, BF16)], (hidden_in, gain, query_proj, turns), 2 * rows * depth * width, 16
    )
    key, value, weights = kernel_call(
        key_value_kernel,
        [(row, BF16), (row, BF16), ((depth, 2 * width), BF16)],
        (place, normed, mine, below, above, turns),
        4 * rows * depth * width,
        20,
    )
    forward = [(i, i + 1) for i in range(63)]
    keys, values = [key], [value]
    for _ in range(1, 4):
        keys.append(lax.ppermute(keys[-1], SP, forward))
        values.append(lax.ppermute(values[-1], SP, forward))
    key4, value4 = kernel_call(
        far_key_value_kernel, [(row, BF16)] * 2, (far_rows, weights, turns), 4 * rows * depth * width, 16
    )

    whole = pl.BlockSpec(row, lambda c: (0, 0))
    part = pl.BlockSpec((128, width), lambda c: (c, 0))
    state = kernel_call(
        near_kernel,
        [(row, F32)] * 3,
        (place, query, keys[0], values[0], keys[1], values[1]),
        16 * rows * rows * width,
        20,
        [((512, 768), F32), ((512, 768), BF16), ((128, 768), F32), ((128, 640), F32), ((2, 512, width), F32), ((2, 128, width), BF16)],
        grid=(rows // 128,),
        in_specs=[SMEM, part] + [whole] * 4,
        out_specs=(part,) * 3,
    )
    sources = {2: (keys[2], values[2]), 3: (keys[3], values[3]), 4: (key4, value4)}
    for backs in ((2, 4), (3,)):
        last = backs == (3,)
        state = kernel_call(
            functools.partial(far_kernel, backs, last),
            [(row, BF16), (row, F32)] if last else [(row, F32)] * 3,
            (place, query, *state, *(array for back in backs for array in sources[back])),
            4 * rows * 512 * width * len(backs),
            16,
            ([(row, BF16)] if last else []) + [((512, 128 * len(backs)), BF16), ((2, 512, width), F32)],
            grid=(rows // 128,),
            in_specs=[SMEM] + [part] * (4 + 2 * len(backs)),
            out_specs=(whole, part) if last else (part,) * 3,
        )
    attended, logs = state

    arrived = lax.all_to_all(attended.reshape(4, rows // 4, width), "x", split_axis=0, concat_axis=0, tiled=True)
    (log_weight,) = kernel_call(log_kernel, [((heads, rows), F32)], (logs,), 6 * rows * rows * width, 12)
    keep, give = kernel_call(
        out_kernel,
        [((piece, depth), F32), ((piece, depth), BF16)],
        (place, arrived, out_proj, before, after, upper, lower),
        2 * rows // 8 * depth * depth,
        20,
        [((2 * piece, depth), F32)],
    )
    taken = lax.ppermute(give, "c", ring(2, 1))
    (layer_out,) = kernel_call(end_kernel, [((piece, depth), BF16)], (keep, taken, post_gain[None]), 10 * piece * depth, 8)
    return layer_out, log_weight


def solution(mesh):
    fine = Mesh(np.asarray(mesh.devices).reshape(4, 2, 8, 4, 2), ("zh", "zl", "y", "x", "c"))
    placed = (P(SP, None), P(), P(None, TP), P(SP, TP), P(SP, TP), P(TP, None), P())
    return jax.shard_map(
        layer,
        mesh=fine,
        in_specs=placed,
        out_specs=(P(SP + TP, None), P(TP, SP)),
        check_vma=False,
    )
```

```python
import functools

import jax
import jax.numpy as jnp
import numpy as np
from jax import lax
from jax.experimental import pallas as pl
from jax.experimental.pallas import tpu as pltpu
from jax.sharding import Mesh
from jax.sharding import PartitionSpec as P

HEAD_DIM = 64
SPAN = 128
EPS = 1e-06
ROPE_BASE = 10000.0
LOW = -1e30
SP = ("zh", "zl", "y")
Z = ("zh", "zl")
TP = ("x", "c")
F32 = jnp.float32
BF16 = jnp.bfloat16
NT = (((1,), (1,)), ((), ()))
HOPS = (0, 3, 1, 2)


def ring(count, steps):
    return [(i, (i + steps) % count) for i in range(count)]


def natural(i):
    return (i & 31) * 16 + ((i >> 5) & 3) * 4 + (i >> 7)


def to_residue(rows, columns=None):
    i = lax.broadcasted_iota(jnp.int32, (rows, rows), 0)
    if columns is None:
        columns = lax.broadcasted_iota(jnp.int32, (rows, rows), 1)
    return (natural(i) == columns).astype(BF16)


def to_natural(rows):
    i = lax.broadcasted_iota(jnp.int32, (rows, rows), 1)
    n = lax.broadcasted_iota(jnp.int32, (rows, rows), 0)
    return (natural(i) == n).astype(BF16)


def rotated(x, cos, sin):
    width = x.shape[1]
    lane = lax.broadcasted_iota(jnp.int32, x.shape, 1)
    other = jnp.where((lane & 63) < 32, pltpu.roll(x, width - 32, 1), pltpu.roll(x, 32, 1))
    return x * cos + other * sin


def permuted(perm, x):
    return jnp.dot(perm, x, preferred_element_type=F32).astype(BF16)


def normed_rows(x, gain):
    x = x.astype(F32)
    scale = lax.rsqrt(jnp.mean(x * x, axis=1, keepdims=True) + EPS)
    return (x * scale * gain).astype(BF16)


def spread(turn_ref, part):
    cos, sin = turn_ref[0, :, part], turn_ref[1, :, part]
    cos = jnp.concatenate([cos] * 4, axis=0).T
    sin = jnp.concatenate([-sin, sin] * 2, axis=0).T
    return jnp.concatenate([cos, cos], axis=1), jnp.concatenate([sin, sin], axis=1)


def slice_kernel(place_ref, hidden_ref, gain_ref, out_ref):
    out_ref[...] = normed_rows(hidden_ref[...], gain_ref[...])


def query_kernel(hidden_ref, gain_ref, weight_ref, turn_ref, normed_ref, query_ref):
    rows = hidden_ref.shape[0]
    gain = gain_ref[...]

    def step(i, carry):
        part = pl.ds(pl.multiple_of(i * 64, 64), 64)
        normed_ref[part, :] = normed_rows(hidden_ref[part, :], gain)
        return carry

    lax.fori_loop(0, rows // 64, step, 0)
    query = jnp.dot(normed_ref[...], weight_ref[...], preferred_element_type=F32)
    cos, sin = spread(turn_ref, slice(rows, 2 * rows))
    query = rotated(query, cos, sin).astype(BF16) * 0.125
    query_ref[...] = permuted(to_residue(rows), query)


def project(normed, weight_ref, cos, sin, key_ref, value_ref):
    rows, width = key_ref.shape
    perm = to_residue(rows)
    key = jnp.dot(normed, weight_ref[:, :width], preferred_element_type=F32)
    key_ref[...] = permuted(perm, rotated(key, cos, sin).astype(BF16))
    value = jnp.dot(normed, weight_ref[:, width:], preferred_element_type=F32).astype(BF16)
    value_ref[...] = permuted(perm, value)


def key_value_kernel(place_ref, normed_ref, mine_ref, below_ref, above_ref, turn_ref, key_ref, value_ref, weight_ref):
    rows = normed_ref.shape[0]
    low = place_ref[1]
    slabs = []
    for k in range(4):
        slabs.append((2 * k + low, mine_ref, k))
    for k in range(2):
        slabs.append((2 * k + 1 - low, below_ref, k))
        slabs.append((2 * (k + 2) + 1 - low, above_ref, k))
    for place, ref, k in slabs:
        weight_ref[pl.ds(pl.multiple_of(place * 256, 256), 256), :] = ref[k]
    project(normed_ref[...], weight_ref, *spread(turn_ref, slice(rows, 2 * rows)), key_ref, value_ref)


def far_key_value_kernel(normed_ref, weight_ref, turn_ref, key_ref, value_ref):
    project(normed_ref[...], weight_ref, *spread(turn_ref, slice(0, normed_ref.shape[0])), key_ref, value_ref)


def stack_heads(q):
    lane = lax.broadcasted_iota(jnp.int32, q.shape, 1) >> 6
    return jnp.concatenate([jnp.where(lane == h, q, jnp.zeros_like(q)) for h in range(q.shape[1] // HEAD_DIM)], axis=0)


def own_heads(stacked):
    width = stacked.shape[1]
    heads = width // HEAD_DIM
    rows = stacked.shape[0] // heads
    lane = lax.broadcasted_iota(jnp.int32, (rows, width), 1) >> 6
    out = stacked[:rows]
    for h in range(1, heads):
        out = jnp.where(lane == h, stacked[h * rows : (h + 1) * rows], out)
    return out


def far_bias(block, back):
    qi = lax.broadcasted_iota(jnp.int32, (128, 128), 0)
    ki = lax.broadcasted_iota(jnp.int32, (128, 128), 1)
    ok = ((qi >> 5) == (ki >> 5)) & (block >= back)
    if back == 4:
        ok = ok & ((ki & 31) >= (qi & 31))
    return jnp.where(ok, 0.0, LOW).astype(F32)


def times_seen(o):
    count = (o <= SPAN).astype(F32)
    count = count + (((o & 3) == 0) & (o <= 4 * SPAN)).astype(F32)
    return count + ((o & 15) == 0).astype(F32)


def query_places(cls):
    i = lax.broadcasted_iota(jnp.int32, (128, 1), 0)
    return (i & 31) * 16 + (i >> 5) * 4 + cls


def own_kernel(q_ref, k_ref, v_ref, max_ref, sum_ref, acc_ref, s_ref, p_ref, bias_ref, count_ref, stat_ref):
    keys, width = k_ref.shape
    heads = width // HEAD_DIM
    o = query_places(pl.program_id(0)) - natural(lax.broadcasted_iota(jnp.int32, (1, keys), 1))
    count = jnp.where(o >= 0, times_seen(o), 0.0)
    count_ref[...] = count
    bias_ref[...] = jnp.where(count > 0, 0.0, LOW).astype(F32)
    s_ref[...] = lax.dot_general(stack_heads(q_ref[...]), k_ref[...], NT, preferred_element_type=F32)
    step = 32
    for r in range(0, heads * 128, step):
        mask = slice(r % 128, r % 128 + step)
        s = s_ref[r : r + step, :] + bias_ref[mask, :]
        m = jnp.max(s, axis=1, keepdims=True)
        p = jnp.exp(s - m) * count_ref[mask, :]
        stat_ref[0, r : r + step, :] = jnp.broadcast_to(m, (step, width))
        stat_ref[1, r : r + step, :] = jnp.broadcast_to(jnp.sum(p, axis=1, keepdims=True), (step, width))
        p_ref[r : r + step, :] = p.astype(BF16)
    pv = jnp.dot(p_ref[...], v_ref[...], preferred_element_type=F32)
    max_ref[...] = own_heads(stat_ref[0])
    sum_ref[...] = own_heads(stat_ref[1])
    acc_ref[...] = own_heads(pv)


def merged(scores, bias, count, value, max_ref, sum_ref, acc_ref, p_ref, stat_ref):
    width = max_ref.shape[1]
    for h in range(width // HEAD_DIM):
        part = slice(h * 128, (h + 1) * 128)
        s = scores[part] + bias
        m = jnp.maximum(jnp.max(s, axis=1, keepdims=True), max_ref[:, h * HEAD_DIM : h * HEAD_DIM + 1])
        p = jnp.exp(s - m)
        if count is not None:
            p = p * count
        p_ref[part, :] = p.astype(BF16)
        stat_ref[0, part, :] = jnp.broadcast_to(m, (128, width))
        stat_ref[1, part, :] = jnp.broadcast_to(jnp.sum(p, axis=1, keepdims=True), (128, width))
    pv = jnp.dot(p_ref[...], value, preferred_element_type=F32)
    m = own_heads(stat_ref[0])
    alpha = jnp.exp(max_ref[...] - m)
    total = sum_ref[...] * alpha + own_heads(stat_ref[1])
    return m, total, acc_ref[...] * alpha + own_heads(pv)


def before_kernel(place_ref, q_ref, max_ref, sum_ref, acc_ref, k_ref, v_ref, new_max, new_sum, new_acc, p_ref, stat_ref, tail_ref):
    cls = pl.program_id(0)
    keys = k_ref.shape[0]
    mine = pl.ds(pl.multiple_of(cls * 128, 128), 128)

    @pl.when(cls == 0)
    def _():
        j = lax.broadcasted_iota(jnp.int32, (128, keys), 0)
        i = lax.broadcasted_iota(jnp.int32, (128, keys), 1)
        pick = (i == (j >> 3) * 32 + 24 + (j & 7)).astype(BF16)
        tail_ref[0] = permuted(pick, k_ref[...])
        tail_ref[1] = permuted(pick, v_ref[...])

    seen = place_ref[0] >= 1
    qn = query_places(cls)
    k = lax.broadcasted_iota(jnp.int32, (1, 128), 1)
    same = times_seen(qn - ((k & 31) * 16 + (k >> 5) * 4 + cls) + keys)
    last = qn - ((24 + (k & 7)) * 16 + ((k >> 3) & 3) * 4 + (k >> 5)) + keys
    last = ((last <= SPAN) & ((k >> 5) != cls)).astype(F32)
    count = jnp.where(seen, jnp.concatenate([same, last], axis=1), 0.0)
    bias = jnp.where(count > 0, 0.0, LOW).astype(F32)
    key = jnp.concatenate([k_ref[mine, :], tail_ref[0]], axis=0)
    value = jnp.concatenate([v_ref[mine, :], tail_ref[1]], axis=0)
    scores = lax.dot_general(stack_heads(q_ref[...]), key, NT, preferred_element_type=F32)
    state = merged(scores, bias, count, value, max_ref, sum_ref, acc_ref, p_ref, stat_ref)
    for ref, part in zip((new_max, new_sum, new_acc), state):
        ref[...] = part


def far_kernel(backs, last, place_ref, q_ref, max_ref, sum_ref, acc_ref, *refs):
    count = len(backs)
    sources, outs = refs[: 2 * count], refs[2 * count :]
    p_ref, stat_ref = outs[-2:]
    bias = jnp.concatenate([far_bias(place_ref[0], back) for back in backs], axis=1)
    key = jnp.concatenate([ref[...] for ref in sources[0::2]], axis=0)
    value = jnp.concatenate([ref[...] for ref in sources[1::2]], axis=0)
    scores = lax.dot_general(stack_heads(q_ref[...]), key, NT, preferred_element_type=F32)
    m, total, acc = merged(scores, bias, None, value, max_ref, sum_ref, acc_ref, p_ref, stat_ref)
    if last:
        cls = pl.program_id(0)
        out_ref, log_ref, att_ref = outs[:3]
        att_ref[pl.ds(pl.multiple_of(cls * 128, 128), 128), :] = (acc / total).astype(BF16)
        log_ref[...] = m + jnp.log(total)

        @pl.when(cls == pl.num_programs(0) - 1)
        def _():
            out_ref[...] = permuted(to_natural(att_ref.shape[0]), att_ref[...])
    else:
        for ref, part in zip(outs[:3], (m, total, acc)):
            ref[...] = part


def log_kernel(lw_ref, log_ref):
    rows, width = lw_ref.shape
    perm = to_natural(rows)
    rest = lw_ref[...]
    ordered = jnp.zeros((rows, width), F32)
    for _ in range(3):
        piece = rest.astype(BF16)
        rest = rest - piece.astype(F32)
        ordered = ordered + jnp.dot(perm, piece, preferred_element_type=F32)
    flipped = ordered.T
    for head in range(width // HEAD_DIM):
        log_ref[head : head + 1, :] = flipped[head * HEAD_DIM : head * HEAD_DIM + 1, :]


def out_kernel(place_ref, att_ref, own_ref, before_ref, after_ref, across_ref, keep_ref, give_ref, sum_ref):
    x, core = place_ref[2], place_ref[3]
    rows = keep_ref.shape[0]
    for n, ref in enumerate((own_ref, before_ref, after_ref, across_ref)):
        part = jnp.dot(att_ref[lax.rem(x + HOPS[n], 4)], ref[...], preferred_element_type=F32)
        part = part.astype(BF16).astype(F32)
        if n == 0:
            sum_ref[...] = part
        else:
            sum_ref[...] += part
    keep_ref[...] = sum_ref[pl.ds(pl.multiple_of(core * rows, rows), rows), :]
    give_ref[...] = sum_ref[pl.ds(pl.multiple_of((1 - core) * rows, rows), rows), :].astype(BF16)


def end_kernel(keep_ref, taken_ref, gain_ref, out_ref):
    summed = keep_ref[...] + taken_ref[...].astype(F32)
    scale = lax.rsqrt(jnp.mean(summed * summed, axis=1, keepdims=True) + EPS)
    out_ref[...] = (summed * scale * gain_ref[...]).astype(BF16)


SMEM = pl.BlockSpec(memory_space=pltpu.SMEM)
VMEM = pl.BlockSpec(memory_space=pltpu.VMEM)


def kernel_call(body, outs, args, flops, limit, scratch=(), **more):
    if "grid_spec" not in more:
        more["scratch_shapes"] = [pltpu.VMEM(s, t) for s, t in scratch]
    if "in_specs" not in more and "grid_spec" not in more:
        more["in_specs"] = [SMEM if a.dtype == jnp.int32 else VMEM for a in args]
        more["out_specs"] = tuple(VMEM for _ in outs)
    data = sum(a.size * a.dtype.itemsize for a in args)
    return pl.pallas_call(
        body,
        out_shape=tuple(jax.ShapeDtypeStruct(s, t) for s, t in outs),
        compiler_params=pltpu.CompilerParams(vmem_limit_bytes=limit * 1024 * 1024),
        cost_estimate=pl.CostEstimate(flops=flops, bytes_accessed=data, transcendentals=0),
        **more,
    )(*args)


def spread_to(value, axis, count):
    copies = jnp.broadcast_to(value[None], (count,) + value.shape)
    return lax.all_to_all(copies, axis, split_axis=0, concat_axis=0, tiled=True)


def layer(hidden_in, pre_gain, query_proj, key_proj, value_proj, out_proj, post_gain):
    rows, depth = hidden_in.shape
    width = query_proj.shape[1]
    heads = width // HEAD_DIM
    piece = rows // 8
    sp, x, core = lax.axis_index(SP), lax.axis_index("x"), lax.axis_index("c")
    place = jnp.stack([sp, lax.axis_index("zl"), x, core]).astype(jnp.int32)
    member = (x * 2 + core)[None].astype(jnp.int32)
    gain = pre_gain[None]
    row = (rows, width)

    shard = jnp.concatenate([key_proj, value_proj], axis=1)
    mine = spread_to(shard, ("zh", "y"), 32).reshape(4, 256, 2 * width)
    below = lax.ppermute(mine[:2], Z, ring(8, 1))
    above = lax.ppermute(mine[2:], Z, ring(8, -1))

    (eighth,) = kernel_call(
        slice_kernel,
        [((piece, depth), BF16)],
        (member, hidden_in, gain),
        10 * piece * depth,
        12,
        grid_spec=pltpu.PrefetchScalarGridSpec(
            num_scalar_prefetch=1,
            grid=(1,),
            in_specs=[pl.BlockSpec((piece, depth), lambda i, t: (t[0], 0)), pl.BlockSpec((1, depth), lambda i, t: (0, 0))],
            out_specs=[pl.BlockSpec((piece, depth), lambda i, t: (0, 0))],
        ),
    )
    fourth = lax.ppermute(eighth, SP, ring(64, 4))
    far_rows = spread_to(fourth, TP, 8).reshape(rows, depth)

    before = lax.ppermute(out_proj, "x", ring(4, 1))
    after = lax.ppermute(out_proj, "x", ring(4, -1))
    across = lax.ppermute(out_proj, "x", ring(4, 2))

    quarter = HEAD_DIM // 2
    frequency = ROPE_BASE ** (-(jnp.arange(quarter, dtype=F32) * 2.0 / HEAD_DIM))
    local = jnp.arange(rows, dtype=jnp.int32)
    positions = jnp.concatenate([(sp - 4) * rows + local, sp * rows + local]).astype(F32)
    angles = positions[None, :] * frequency[:, None]
    turns = jnp.stack([jnp.cos(angles), jnp.sin(angles)])

    normed, query = kernel_call(
        query_kernel, [((rows, depth), BF16), (row, BF16)], (hidden_in, gain, query_proj, turns), 2 * rows * depth * width, 12
    )
    key, value, weights = kernel_call(
        key_value_kernel,
        [(row, BF16), (row, BF16), ((depth, 2 * width), BF16)],
        (place, normed, mine, below, above, turns),
        4 * rows * depth * width,
        12,
    )
    forward = [(i, i + 1) for i in range(63)]
    keys, values = [key], [value]
    for _ in range(1, 4):
        keys.append(lax.ppermute(keys[-1], SP, forward))
        values.append(lax.ppermute(values[-1], SP, forward))
    key4, value4 = kernel_call(
        far_key_value_kernel, [(row, BF16)] * 2, (far_rows, weights, turns), 4 * rows * depth * width, 10
    )

    whole = pl.BlockSpec(row, lambda c: (0, 0))
    part = pl.BlockSpec((128, width), lambda c: (c, 0))
    pair = ((512, 256), BF16), ((2, 512, width), F32)
    state = kernel_call(
        own_kernel,
        [(row, F32)] * 3,
        (query, keys[0], values[0]),
        8 * rows * rows * width,
        10,
        [((512, 512), F32), ((512, 512), BF16), ((128, 512), F32), ((128, 512), F32), ((2, 512, width), F32)],
        grid=(rows // 128,),
        in_specs=[part, whole, whole],
        out_specs=(part,) * 3,
    )
    state = kernel_call(
        before_kernel,
        [(row, F32)] * 3,
        (place, query, *state, keys[1], values[1]),
        4 * rows * rows * width,
        10,
        [*pair, ((2, 128, width), BF16)],
        grid=(rows // 128,),
        in_specs=[SMEM] + [part] * 4 + [whole, whole],
        out_specs=(part,) * 3,
    )
    sources = {2: (keys[2], values[2]), 3: (keys[3], values[3]), 4: (key4, value4)}
    for backs in ((2, 4), (3,)):
        last = backs == (3,)
        state = kernel_call(
            functools.partial(far_kernel, backs, last),
            [(row, BF16), (row, F32)] if last else [(row, F32)] * 3,
            (place, query, *state, *(array for back in backs for array in sources[back])),
            4 * rows * 512 * width * len(backs),
            10,
            ([(row, BF16)] if last else []) + [((512, 128 * len(backs)), BF16), ((2, 512, width), F32)],
            grid=(rows // 128,),
            in_specs=[SMEM] + [part] * (4 + 2 * len(backs)),
            out_specs=(whole, part) if last else (part,) * 3,
        )
    attended, logs = state

    arrived = lax.all_to_all(attended.reshape(4, rows // 4, width), "x", split_axis=0, concat_axis=0, tiled=True)
    (log_weight,) = kernel_call(log_kernel, [((heads, rows), F32)], (logs,), 6 * rows * rows * width, 8)
    keep, give = kernel_call(
        out_kernel,
        [((piece, depth), F32), ((piece, depth), BF16)],
        (place, arrived, out_proj, before, after, across),
        2 * rows // 8 * depth * depth,
        12,
        [((2 * piece, depth), F32)],
    )
    taken = lax.ppermute(give, "c", ring(2, 1))
    (layer_out,) = kernel_call(end_kernel, [((piece, depth), BF16)], (keep, taken, post_gain[None]), 10 * piece * depth, 8)
    return layer_out, log_weight


def solution(mesh):
    fine = Mesh(np.asarray(mesh.devices).reshape(4, 2, 8, 4, 2), ("zh", "zl", "y", "x", "c"))
    placed = (P(SP, None), P(), P(None, TP), P(SP, TP), P(SP, TP), P(TP, None), P())
    return jax.shard_map(
        layer,
        mesh=fine,
        in_specs=placed,
        out_specs=(P(SP + TP, None), P(TP, SP)),
        check_vma=False,
    )
```

```python
import functools

import jax
import jax.numpy as jnp
import numpy as np
from jax import lax
from jax.experimental import pallas as pl
from jax.experimental.pallas import tpu as pltpu
from jax.sharding import Mesh
from jax.sharding import PartitionSpec as P

HEAD_DIM = 64
SPAN = 128
EPS = 1e-06
ROPE_BASE = 10000.0
LOW = -1e30
SP = ("zh", "zl", "y")
Z = ("zh", "zl")
TP = ("x", "c")
F32 = jnp.float32
BF16 = jnp.bfloat16
NT = (((1,), (1,)), ((), ()))
HOPS = (0, 3, 1, 2)


def ring(count, steps):
    return [(i, (i + steps) % count) for i in range(count)]


def natural(i):
    return (i & 31) * 16 + ((i >> 5) & 3) * 4 + (i >> 7)


def to_residue(rows, columns=None):
    i = lax.broadcasted_iota(jnp.int32, (rows, rows), 0)
    if columns is None:
        columns = lax.broadcasted_iota(jnp.int32, (rows, rows), 1)
    return (natural(i) == columns).astype(BF16)


def to_natural(rows):
    i = lax.broadcasted_iota(jnp.int32, (rows, rows), 1)
    n = lax.broadcasted_iota(jnp.int32, (rows, rows), 0)
    return (natural(i) == n).astype(BF16)


def rotated(x, cos, sin):
    width = x.shape[1]
    lane = lax.broadcasted_iota(jnp.int32, x.shape, 1)
    other = jnp.where((lane & 63) < 32, pltpu.roll(x, width - 32, 1), pltpu.roll(x, 32, 1))
    return x * cos + other * sin


def permuted(perm, x):
    return jnp.dot(perm, x, preferred_element_type=F32).astype(BF16)


def normed_rows(x, gain):
    x = x.astype(F32)
    scale = lax.rsqrt(jnp.mean(x * x, axis=1, keepdims=True) + EPS)
    return (x * scale * gain).astype(BF16)


def spread(turn_ref, part):
    cos, sin = turn_ref[0, :, part], turn_ref[1, :, part]
    cos = jnp.concatenate([cos] * 4, axis=0).T
    sin = jnp.concatenate([-sin, sin] * 2, axis=0).T
    return jnp.concatenate([cos, cos], axis=1), jnp.concatenate([sin, sin], axis=1)


def slice_kernel(place_ref, hidden_ref, gain_ref, out_ref):
    out_ref[...] = normed_rows(hidden_ref[...], gain_ref[...])


def query_kernel(hidden_ref, gain_ref, weight_ref, turn_ref, normed_ref, query_ref):
    rows = hidden_ref.shape[0]
    gain = gain_ref[...]

    def step(i, carry):
        part = pl.ds(pl.multiple_of(i * 64, 64), 64)
        normed_ref[part, :] = normed_rows(hidden_ref[part, :], gain)
        return carry

    lax.fori_loop(0, rows // 64, step, 0)
    query = jnp.dot(normed_ref[...], weight_ref[...], preferred_element_type=F32)
    cos, sin = spread(turn_ref, slice(rows, 2 * rows))
    query = rotated(query, cos, sin).astype(BF16) * 0.125
    query_ref[...] = permuted(to_residue(rows), query)


def project(normed_ref, turn_ref, weight_ref, key_ref, value_ref, both_ref):
    rows, width = key_ref.shape
    block = normed_ref.shape[0]
    n = pl.program_id(0)
    cos, sin = spread(turn_ref, slice(0, block))
    both = jnp.dot(normed_ref[...], weight_ref[...], preferred_element_type=F32)
    part = pl.ds(pl.multiple_of(n * block, block), block)
    both_ref[part, :width] = rotated(both[:, :width], cos, sin).astype(BF16)
    both_ref[part, width:] = both[:, width:].astype(BF16)

    @pl.when(n == pl.num_programs(0) - 1)
    def _():
        ordered = permuted(to_residue(rows), both_ref[...])
        key_ref[...] = ordered[:, :width]
        value_ref[...] = ordered[:, width:]


def key_value_kernel(place_ref, normed_ref, turn_ref, mine_ref, below_ref, above_ref, key_ref, value_ref, weight_ref, both_ref):
    @pl.when(pl.program_id(0) == 0)
    def _():
        low = place_ref[1]
        slabs = []
        for k in range(4):
            slabs.append((2 * k + low, mine_ref, k))
        for k in range(2):
            slabs.append((2 * k + 1 - low, below_ref, k))
            slabs.append((2 * (k + 2) + 1 - low, above_ref, k))
        for place, ref, k in slabs:
            weight_ref[pl.ds(pl.multiple_of(place * 256, 256), 256), :] = ref[k]

    project(normed_ref, turn_ref, weight_ref, key_ref, value_ref, both_ref)


def far_key_value_kernel(normed_ref, turn_ref, weight_ref, key_ref, value_ref, both_ref):
    project(normed_ref, turn_ref, weight_ref, key_ref, value_ref, both_ref)


def stack_heads(q):
    lane = lax.broadcasted_iota(jnp.int32, q.shape, 1) >> 6
    return jnp.concatenate([jnp.where(lane == h, q, jnp.zeros_like(q)) for h in range(q.shape[1] // HEAD_DIM)], axis=0)


def own_heads(stacked):
    width = stacked.shape[1]
    heads = width // HEAD_DIM
    rows = stacked.shape[0] // heads
    lane = lax.broadcasted_iota(jnp.int32, (rows, width), 1) >> 6
    out = stacked[:rows]
    for h in range(1, heads):
        out = jnp.where(lane == h, stacked[h * rows : (h + 1) * rows], out)
    return out


def far_bias(block, back):
    qi = lax.broadcasted_iota(jnp.int32, (128, 128), 0)
    ki = lax.broadcasted_iota(jnp.int32, (128, 128), 1)
    ok = ((qi >> 5) == (ki >> 5)) & (block >= back)
    if back == 4:
        ok = ok & ((ki & 31) >= (qi & 31))
    return jnp.where(ok, 0.0, LOW).astype(F32)


def times_seen(o):
    count = (o <= SPAN).astype(F32)
    count = count + (((o & 3) == 0) & (o <= 4 * SPAN)).astype(F32)
    return count + ((o & 15) == 0).astype(F32)


def query_places(cls):
    i = lax.broadcasted_iota(jnp.int32, (128, 1), 0)
    return (i & 31) * 16 + (i >> 5) * 4 + cls


def statistics(tops, sums):
    lane = lax.broadcasted_iota(jnp.int32, (tops[0].shape[0], 128), 1)
    out = jnp.zeros(lane.shape, F32)
    for n, column in enumerate(tops + sums):
        out = jnp.where(lane == n, column, out)
    return out


def by_head(columns, width):
    lane = lax.broadcasted_iota(jnp.int32, (columns[0].shape[0], width), 1) >> 6
    out = jnp.broadcast_to(columns[0], lane.shape)
    for h in range(1, len(columns)):
        out = jnp.where(lane == h, columns[h], out)
    return out


def own_kernel(q_ref, k_ref, v_ref, stat_ref, acc_ref, s_ref, p_ref, bias_ref, count_ref, raw_ref):
    keys, width = k_ref.shape
    heads = width // HEAD_DIM
    o = query_places(pl.program_id(0)) - natural(lax.broadcasted_iota(jnp.int32, (1, keys), 1))
    count = jnp.where(o >= 0, times_seen(o), 0.0)
    count_ref[...] = count
    bias_ref[...] = jnp.where(count > 0, 0.0, LOW).astype(F32)
    s_ref[...] = lax.dot_general(stack_heads(q_ref[...]), k_ref[...], NT, preferred_element_type=F32)
    step = 32
    for r in range(0, heads * 128, step):
        mask = slice(r % 128, r % 128 + step)
        s = s_ref[r : r + step, :] + bias_ref[mask, :]
        m = jnp.max(s, axis=1, keepdims=True)
        p = jnp.exp(s - m) * count_ref[mask, :]
        raw_ref[0, r : r + step, :] = jnp.broadcast_to(m, (step, 128))
        raw_ref[1, r : r + step, :] = jnp.broadcast_to(jnp.sum(p, axis=1, keepdims=True), (step, 128))
        p_ref[r : r + step, :] = p.astype(BF16)
    columns = [[raw_ref[n, h * 128 : (h + 1) * 128, :] for h in range(heads)] for n in range(2)]
    stat_ref[...] = statistics(*columns)
    acc_ref[...] = own_heads(jnp.dot(p_ref[...], v_ref[...], preferred_element_type=F32))


def merged(q, key, value, bias, count, stat, acc):
    width = q.shape[1]
    heads = width // HEAD_DIM
    scores = lax.dot_general(stack_heads(q), key, NT, preferred_element_type=F32)
    tops, sums, shares, scales = [], [], [], []
    for h in range(heads):
        s = scores[h * 128 : (h + 1) * 128] + bias
        old = stat[:, h : h + 1]
        m = jnp.maximum(jnp.max(s, axis=1, keepdims=True), old)
        p = jnp.exp(s - m)
        if count is not None:
            p = p * count
        scale = jnp.exp(old - m)
        tops.append(m)
        sums.append(stat[:, heads + h : heads + h + 1] * scale + jnp.sum(p, axis=1, keepdims=True))
        scales.append(scale)
        shares.append(p.astype(BF16))
    pv = own_heads(jnp.dot(jnp.concatenate(shares, axis=0), value, preferred_element_type=F32))
    return tops, sums, acc * by_head(scales, width) + pv


def before_kernel(place_ref, q_ref, stat_ref, acc_ref, k_ref, v_ref, new_stat, new_acc, tail_ref):
    cls = pl.program_id(0)
    keys = k_ref.shape[0]
    mine = pl.ds(pl.multiple_of(cls * 128, 128), 128)

    @pl.when(cls == 0)
    def _():
        j = lax.broadcasted_iota(jnp.int32, (128, keys), 0)
        i = lax.broadcasted_iota(jnp.int32, (128, keys), 1)
        pick = (i == (j >> 3) * 32 + 24 + (j & 7)).astype(BF16)
        tail_ref[0] = permuted(pick, k_ref[...])
        tail_ref[1] = permuted(pick, v_ref[...])

    seen = place_ref[0] >= 1
    qn = query_places(cls)
    k = lax.broadcasted_iota(jnp.int32, (1, 128), 1)
    same = times_seen(qn - ((k & 31) * 16 + (k >> 5) * 4 + cls) + keys)
    last = qn - ((24 + (k & 7)) * 16 + ((k >> 3) & 3) * 4 + (k >> 5)) + keys
    last = ((last <= SPAN) & ((k >> 5) != cls)).astype(F32)
    count = jnp.where(seen, jnp.concatenate([same, last], axis=1), 0.0)
    bias = jnp.where(count > 0, 0.0, LOW).astype(F32)
    key = jnp.concatenate([k_ref[mine, :], tail_ref[0]], axis=0)
    value = jnp.concatenate([v_ref[mine, :], tail_ref[1]], axis=0)
    tops, sums, acc = merged(q_ref[...], key, value, bias, count, stat_ref[...], acc_ref[...])
    new_stat[...] = statistics(tops, sums)
    new_acc[...] = acc


def far_kernel(backs, place_ref, q_ref, stat_ref, acc_ref, *refs):
    sources, (new_stat, new_acc) = refs[:-2], refs[-2:]
    bias = jnp.concatenate([far_bias(place_ref[0], back) for back in backs], axis=1)
    key = jnp.concatenate([ref[...] for ref in sources[0::2]], axis=0)
    value = jnp.concatenate([ref[...] for ref in sources[1::2]], axis=0)
    tops, sums, acc = merged(q_ref[...], key, value, bias, None, stat_ref[...], acc_ref[...])
    new_stat[...] = statistics(tops, sums)
    new_acc[...] = acc


def last_kernel(back, place_ref, q_ref, stat_ref, acc_ref, k_ref, v_ref, out_ref, new_stat):
    rows, width = q_ref.shape
    bias = far_bias(place_ref[0], back)
    done = []
    for cls in range(rows // 128):
        part = slice(cls * 128, (cls + 1) * 128)
        tops, sums, acc = merged(q_ref[part, :], k_ref[part, :], v_ref[part, :], bias, None, stat_ref[part, :], acc_ref[part, :])
        new_stat[part, :] = statistics(tops, sums)
        done.append((acc / by_head(sums, width)).astype(BF16))
    out_ref[...] = permuted(to_natural(rows), jnp.concatenate(done, axis=0))


def log_kernel(stat_ref, log_ref):
    rows = stat_ref.shape[0]
    heads = log_ref.shape[0]
    perm = to_natural(rows)
    rest = stat_ref[...]
    ordered = jnp.zeros(rest.shape, F32)
    for _ in range(3):
        piece = rest.astype(BF16)
        rest = rest - piece.astype(F32)
        ordered = ordered + jnp.dot(perm, piece, preferred_element_type=F32)
    flipped = ordered.T
    log_ref[...] = flipped[:heads] + jnp.log(flipped[heads : 2 * heads])


def out_kernel(place_ref, att_ref, own_ref, before_ref, after_ref, across_ref, keep_ref, give_ref, sum_ref):
    x, core = place_ref[2], place_ref[3]
    rows = keep_ref.shape[0]
    total = None
    for n, ref in enumerate((own_ref, before_ref, after_ref, across_ref)):
        part = jnp.dot(att_ref[lax.rem(x + HOPS[n], 4)], ref[...], preferred_element_type=F32)
        part = part.astype(BF16).astype(F32)
        total = part if total is None else total + part
    sum_ref[...] = total
    keep_ref[...] = sum_ref[pl.ds(pl.multiple_of(core * rows, rows), rows), :]
    give_ref[...] = sum_ref[pl.ds(pl.multiple_of((1 - core) * rows, rows), rows), :].astype(BF16)


def end_kernel(keep_ref, taken_ref, gain_ref, out_ref):
    summed = keep_ref[...] + taken_ref[...].astype(F32)
    scale = lax.rsqrt(jnp.mean(summed * summed, axis=1, keepdims=True) + EPS)
    out_ref[...] = (summed * scale * gain_ref[...]).astype(BF16)


SMEM = pl.BlockSpec(memory_space=pltpu.SMEM)
VMEM = pl.BlockSpec(memory_space=pltpu.VMEM)


def kernel_call(body, outs, args, flops, limit, scratch=(), **more):
    if "grid_spec" not in more:
        more["scratch_shapes"] = [pltpu.VMEM(s, t) for s, t in scratch]
    if "in_specs" not in more and "grid_spec" not in more:
        more["in_specs"] = [SMEM if a.dtype == jnp.int32 else VMEM for a in args]
        more["out_specs"] = tuple(VMEM for _ in outs)
    data = sum(a.size * a.dtype.itemsize for a in args)
    return pl.pallas_call(
        body,
        out_shape=tuple(jax.ShapeDtypeStruct(s, t) for s, t in outs),
        compiler_params=pltpu.CompilerParams(vmem_limit_bytes=limit * 1024 * 1024),
        cost_estimate=pl.CostEstimate(flops=flops, bytes_accessed=data, transcendentals=0),
        **more,
    )(*args)


def spread_to(value, axis, count):
    copies = jnp.broadcast_to(value[None], (count,) + value.shape)
    return lax.all_to_all(copies, axis, split_axis=0, concat_axis=0, tiled=True)


def layer(hidden_in, pre_gain, query_proj, key_proj, value_proj, out_proj, post_gain):
    rows, depth = hidden_in.shape
    width = query_proj.shape[1]
    heads = width // HEAD_DIM
    piece = rows // 8
    sp, x, core = lax.axis_index(SP), lax.axis_index("x"), lax.axis_index("c")
    place = jnp.stack([sp, lax.axis_index("zl"), x, core]).astype(jnp.int32)
    member = (x * 2 + core)[None].astype(jnp.int32)
    gain = pre_gain[None]
    row = (rows, width)

    copies = [jnp.broadcast_to(shard[None], (32,) + shard.shape) for shard in (key_proj, value_proj)]
    mine = lax.all_to_all(jnp.concatenate(copies, axis=2), ("zh", "y"), split_axis=0, concat_axis=0, tiled=True)
    mine = mine.reshape(4, 256, 2 * width)
    below = lax.ppermute(mine[:2], Z, ring(8, 1))
    above = lax.ppermute(mine[2:], Z, ring(8, -1))

    (eighth,) = kernel_call(
        slice_kernel,
        [((piece, depth), BF16)],
        (member, hidden_in, gain),
        10 * piece * depth,
        12,
        grid_spec=pltpu.PrefetchScalarGridSpec(
            num_scalar_prefetch=1,
            grid=(1,),
            in_specs=[pl.BlockSpec((piece, depth), lambda i, t: (t[0], 0)), pl.BlockSpec((1, depth), lambda i, t: (0, 0))],
            out_specs=[pl.BlockSpec((piece, depth), lambda i, t: (0, 0))],
        ),
    )
    fourth = lax.ppermute(eighth, SP, ring(64, 4))
    far_rows = spread_to(fourth, TP, 8).reshape(rows, depth)

    before = lax.ppermute(out_proj, "x", ring(4, 1))
    after = lax.ppermute(out_proj, "x", ring(4, -1))
    across = lax.ppermute(out_proj, "x", ring(4, 2))

    quarter = HEAD_DIM // 2
    frequency = ROPE_BASE ** (-(jnp.arange(quarter, dtype=F32) * 2.0 / HEAD_DIM))
    local = jnp.arange(rows, dtype=jnp.int32)
    positions = jnp.concatenate([(sp - 4) * rows + local, sp * rows + local]).astype(F32)
    angles = positions[None, :] * frequency[:, None]
    turns = jnp.stack([jnp.cos(angles), jnp.sin(angles)])

    normed, query = kernel_call(
        query_kernel, [((rows, depth), BF16), (row, BF16)], (hidden_in, gain, query_proj, turns), 2 * rows * depth * width, 12
    )
    block_rows = rows // 4
    row_part = pl.BlockSpec((block_rows, depth), lambda n: (n, 0))
    whole = pl.BlockSpec(row, lambda c: (0, 0))
    weight_spec = pl.BlockSpec((depth, 2 * width), lambda n: (0, 0))
    key, value, weights = kernel_call(
        key_value_kernel,
        [(row, BF16), (row, BF16), ((depth, 2 * width), BF16)],
        (place, normed, turns, mine, below, above),
        4 * rows * depth * width,
        14,
        [((rows, 2 * width), BF16)],
        grid=(4,),
        in_specs=[
            SMEM,
            row_part,
            pl.BlockSpec((2, HEAD_DIM // 2, block_rows), lambda n: (0, 0, 4 + n)),
            pl.BlockSpec((4, 256, 2 * width), lambda n: (0, 0, 0)),
            pl.BlockSpec((2, 256, 2 * width), lambda n: (0, 0, 0)),
            pl.BlockSpec((2, 256, 2 * width), lambda n: (0, 0, 0)),
        ],
        out_specs=(whole, whole, weight_spec),
    )
    forward = [(i, i + 1) for i in range(63)]
    keys, values = [key], [value]
    for _ in range(1, 4):
        keys.append(lax.ppermute(keys[-1], SP, forward))
        values.append(lax.ppermute(values[-1], SP, forward))
    key4, value4 = kernel_call(
        far_key_value_kernel,
        [(row, BF16)] * 2,
        (far_rows, turns, weights),
        4 * rows * depth * width,
        14,
        [((rows, 2 * width), BF16)],
        grid=(4,),
        in_specs=[row_part, pl.BlockSpec((2, HEAD_DIM // 2, block_rows), lambda n: (0, 0, n)), weight_spec],
        out_specs=(whole, whole),
    )

    part = pl.BlockSpec((128, width), lambda c: (c, 0))
    stat_part = pl.BlockSpec((128, 128), lambda c: (c, 0))
    outs = [((rows, 128), F32), (row, F32)]
    state = kernel_call(
        own_kernel,
        outs,
        (query, keys[0], values[0]),
        8 * rows * rows * width,
        10,
        [((512, 512), F32), ((512, 512), BF16), ((128, 512), F32), ((128, 512), F32), ((2, 512, 128), F32)],
        grid=(rows // 128,),
        in_specs=[part, whole, whole],
        out_specs=(stat_part, part),
    )
    state = kernel_call(
        before_kernel,
        outs,
        (place, query, *state, keys[1], values[1]),
        4 * rows * rows * width,
        10,
        [((2, 128, width), BF16)],
        grid=(rows // 128,),
        in_specs=[SMEM, part, stat_part, part, whole, whole],
        out_specs=(stat_part, part),
    )
    state = kernel_call(
        functools.partial(far_kernel, (2, 4)),
        outs,
        (place, query, *state, keys[2], values[2], key4, value4),
        4 * rows * 1024 * width,
        10,
        grid=(rows // 128,),
        in_specs=[SMEM, part, stat_part] + [part] * 5,
        out_specs=(stat_part, part),
    )
    attended, logs = kernel_call(
        functools.partial(last_kernel, 3),
        [(row, BF16), ((rows, 128), F32)],
        (place, query, *state, keys[3], values[3]),
        4 * rows * 512 * width,
        12,
    )

    arrived = lax.all_to_all(attended.reshape(4, rows // 4, width), "x", split_axis=0, concat_axis=0, tiled=True)
    (log_weight,) = kernel_call(log_kernel, [((heads, rows), F32)], (logs,), 6 * rows * rows * width, 8)
    columns = depth // 4
    piece_spec = pl.BlockSpec((piece, columns), lambda n: (0, n))
    keep, give = kernel_call(
        out_kernel,
        [((piece, depth), F32), ((piece, depth), BF16)],
        (place, arrived, out_proj, before, after, across),
        2 * rows // 8 * depth * depth,
        12,
        [((2 * piece, columns), F32)],
        grid=(4,),
        in_specs=[SMEM, pl.BlockSpec((4, rows // 4, width), lambda n: (0, 0, 0))] + [pl.BlockSpec((width, columns), lambda n: (0, n))] * 4,
        out_specs=(piece_spec, piece_spec),
    )
    taken = lax.ppermute(give, "c", ring(2, 1))
    (layer_out,) = kernel_call(end_kernel, [((piece, depth), BF16)], (keep, taken, post_gain[None]), 10 * piece * depth, 8)
    return layer_out, log_weight


def solution(mesh):
    fine = Mesh(np.asarray(mesh.devices).reshape(4, 2, 8, 4, 2), ("zh", "zl", "y", "x", "c"))
    placed = (P(SP, None), P(), P(None, TP), P(SP, TP), P(SP, TP), P(TP, None), P())
    return jax.shard_map(
        layer,
        mesh=fine,
        in_specs=placed,
        out_specs=(P(SP + TP, None), P(TP, SP)),
        check_vma=False,
    )
```

```python
import functools

import jax
import jax.numpy as jnp
import numpy as np
from jax import lax
from jax.experimental import pallas as pl
from jax.experimental.pallas import tpu as pltpu
from jax.sharding import Mesh
from jax.sharding import PartitionSpec as P

HEAD_DIM = 64
SPAN = 128
EPS = 1e-06
ROPE_BASE = 10000.0
LOW = -1e30
SP = ("zh", "zl", "y")
Z = ("zh", "zl")
TP = ("x", "c")
F32 = jnp.float32
BF16 = jnp.bfloat16
NT = (((1,), (1,)), ((), ()))
HOPS = (0, 3, 1, 2)


def ring(count, steps):
    return [(i, (i + steps) % count) for i in range(count)]


def natural(i):
    return (i & 31) * 16 + ((i >> 5) & 3) * 4 + (i >> 7)


def to_residue(rows, columns=None):
    i = lax.broadcasted_iota(jnp.int32, (rows, rows), 0)
    if columns is None:
        columns = lax.broadcasted_iota(jnp.int32, (rows, rows), 1)
    return (natural(i) == columns).astype(BF16)


def to_natural(rows):
    i = lax.broadcasted_iota(jnp.int32, (rows, rows), 1)
    n = lax.broadcasted_iota(jnp.int32, (rows, rows), 0)
    return (natural(i) == n).astype(BF16)


def rotated(x, cos, sin):
    width = x.shape[1]
    lane = lax.broadcasted_iota(jnp.int32, x.shape, 1)
    other = jnp.where((lane & 63) < 32, pltpu.roll(x, width - 32, 1), pltpu.roll(x, 32, 1))
    return x * cos + other * sin


def permuted(perm, x):
    return jnp.dot(perm, x, preferred_element_type=F32).astype(BF16)


def normed_rows(x, gain):
    x = x.astype(F32)
    scale = lax.rsqrt(jnp.mean(x * x, axis=1, keepdims=True) + EPS)
    return (x * scale * gain).astype(BF16)


def spread(turn_ref, part):
    cos, sin = turn_ref[0, :, part], turn_ref[1, :, part]
    cos = jnp.concatenate([cos] * 4, axis=0).T
    sin = jnp.concatenate([-sin, sin] * 2, axis=0).T
    return jnp.concatenate([cos, cos], axis=1), jnp.concatenate([sin, sin], axis=1)


def slice_kernel(place_ref, hidden_ref, gain_ref, out_ref):
    out_ref[...] = normed_rows(hidden_ref[...], gain_ref[...])


def query_kernel(hidden_ref, gain_ref, weight_ref, turn_ref, normed_ref, query_ref):
    rows = hidden_ref.shape[0]
    gain = gain_ref[...]

    def step(i, carry):
        part = pl.ds(pl.multiple_of(i * 64, 64), 64)
        normed_ref[part, :] = normed_rows(hidden_ref[part, :], gain)
        return carry

    lax.fori_loop(0, rows // 64, step, 0)
    query = jnp.dot(normed_ref[...], weight_ref[...], preferred_element_type=F32)
    cos, sin = spread(turn_ref, slice(rows, 2 * rows))
    query = rotated(query, cos, sin).astype(BF16) * 0.125
    query_ref[...] = permuted(to_residue(rows), query)


def project(normed_ref, turn_ref, weight_ref, key_ref, value_ref, both_ref):
    rows, width = key_ref.shape
    block = normed_ref.shape[0]
    n = pl.program_id(0)
    cos, sin = spread(turn_ref, slice(0, block))
    both = jnp.dot(normed_ref[...], weight_ref[...], preferred_element_type=F32)
    part = pl.ds(pl.multiple_of(n * block, block), block)
    both_ref[part, :width] = rotated(both[:, :width], cos, sin).astype(BF16)
    both_ref[part, width:] = both[:, width:].astype(BF16)

    @pl.when(n == pl.num_programs(0) - 1)
    def _():
        ordered = permuted(to_residue(rows), both_ref[...])
        key_ref[...] = ordered[:, :width]
        value_ref[...] = ordered[:, width:]


def key_value_kernel(place_ref, normed_ref, turn_ref, mine_ref, below_ref, above_ref, key_ref, value_ref, weight_ref, both_ref):
    @pl.when(pl.program_id(0) == 0)
    def _():
        low = place_ref[1]
        slabs = []
        for k in range(4):
            slabs.append((2 * k + low, mine_ref, k))
        for k in range(2):
            slabs.append((2 * k + 1 - low, below_ref, k))
            slabs.append((2 * (k + 2) + 1 - low, above_ref, k))
        for place, ref, k in slabs:
            weight_ref[pl.ds(pl.multiple_of(place * 256, 256), 256), :] = ref[k]

    project(normed_ref, turn_ref, weight_ref, key_ref, value_ref, both_ref)


def far_key_value_kernel(normed_ref, turn_ref, weight_ref, key_ref, value_ref, both_ref):
    project(normed_ref, turn_ref, weight_ref, key_ref, value_ref, both_ref)


def stack_heads(q):
    lane = lax.broadcasted_iota(jnp.int32, q.shape, 1) >> 6
    return jnp.concatenate([jnp.where(lane == h, q, jnp.zeros_like(q)) for h in range(q.shape[1] // HEAD_DIM)], axis=0)


def own_heads(stacked):
    width = stacked.shape[1]
    heads = width // HEAD_DIM
    rows = stacked.shape[0] // heads
    lane = lax.broadcasted_iota(jnp.int32, (rows, width), 1) >> 6
    out = stacked[:rows]
    for h in range(1, heads):
        out = jnp.where(lane == h, stacked[h * rows : (h + 1) * rows], out)
    return out


def far_bias(block, back):
    qi = lax.broadcasted_iota(jnp.int32, (128, 128), 0)
    ki = lax.broadcasted_iota(jnp.int32, (128, 128), 1)
    ok = ((qi >> 5) == (ki >> 5)) & (block >= back)
    if back == 4:
        ok = ok & ((ki & 31) >= (qi & 31))
    return jnp.where(ok, 0.0, LOW).astype(F32)


def times_seen(o):
    count = (o <= SPAN).astype(F32)
    count = count + (((o & 3) == 0) & (o <= 4 * SPAN)).astype(F32)
    return count + ((o & 15) == 0).astype(F32)


def query_places(cls):
    i = lax.broadcasted_iota(jnp.int32, (128, 1), 0)
    return (i & 31) * 16 + (i >> 5) * 4 + cls


def own_kernel(q_ref, k_ref, v_ref, max_ref, sum_ref, acc_ref, s_ref, p_ref, bias_ref, count_ref, stat_ref):
    keys, width = k_ref.shape
    heads = width // HEAD_DIM
    o = query_places(pl.program_id(0)) - natural(lax.broadcasted_iota(jnp.int32, (1, keys), 1))
    count = jnp.where(o >= 0, times_seen(o), 0.0)
    count_ref[...] = count
    bias_ref[...] = jnp.where(count > 0, 0.0, LOW).astype(F32)
    s_ref[...] = lax.dot_general(stack_heads(q_ref[...]), k_ref[...], NT, preferred_element_type=F32)
    step = 32
    for r in range(0, heads * 128, step):
        mask = slice(r % 128, r % 128 + step)
        s = s_ref[r : r + step, :] + bias_ref[mask, :]
        m = jnp.max(s, axis=1, keepdims=True)
        p = jnp.exp(s - m) * count_ref[mask, :]
        stat_ref[0, r : r + step, :] = jnp.broadcast_to(m, (step, width))
        stat_ref[1, r : r + step, :] = jnp.broadcast_to(jnp.sum(p, axis=1, keepdims=True), (step, width))
        p_ref[r : r + step, :] = p.astype(BF16)
    pv = jnp.dot(p_ref[...], v_ref[...], preferred_element_type=F32)
    max_ref[...] = own_heads(stat_ref[0])
    sum_ref[...] = own_heads(stat_ref[1])
    acc_ref[...] = own_heads(pv)


def merged(q, key, value, bias, count, max_ref, sum_ref, acc_ref, s_ref, p_ref, stat_ref):
    width = max_ref.shape[1]
    s_ref[...] = lax.dot_general(stack_heads(q), key, NT, preferred_element_type=F32)
    for h in range(width // HEAD_DIM):
        part = slice(h * 128, (h + 1) * 128)
        s = s_ref[part, :] + bias
        m = jnp.maximum(jnp.max(s, axis=1, keepdims=True), max_ref[:, h * HEAD_DIM : h * HEAD_DIM + 1])
        p = jnp.exp(s - m)
        if count is not None:
            p = p * count
        p_ref[part, :] = p.astype(BF16)
        stat_ref[0, part, :] = jnp.broadcast_to(m, (128, width))
        stat_ref[1, part, :] = jnp.broadcast_to(jnp.sum(p, axis=1, keepdims=True), (128, width))
    pv = jnp.dot(p_ref[...], value, preferred_element_type=F32)
    m = own_heads(stat_ref[0])
    alpha = jnp.exp(max_ref[...] - m)
    total = sum_ref[...] * alpha + own_heads(stat_ref[1])
    return m, total, acc_ref[...] * alpha + own_heads(pv)


def before_kernel(place_ref, q_ref, max_ref, sum_ref, acc_ref, k_ref, v_ref, new_max, new_sum, new_acc, s_ref, p_ref, stat_ref, tail_ref):
    cls = pl.program_id(0)
    keys = k_ref.shape[0]
    mine = pl.ds(pl.multiple_of(cls * 128, 128), 128)

    @pl.when(cls == 0)
    def _():
        j = lax.broadcasted_iota(jnp.int32, (128, keys), 0)
        i = lax.broadcasted_iota(jnp.int32, (128, keys), 1)
        pick = (i == (j >> 3) * 32 + 24 + (j & 7)).astype(BF16)
        tail_ref[0] = permuted(pick, k_ref[...])
        tail_ref[1] = permuted(pick, v_ref[...])

    seen = place_ref[0] >= 1
    qn = query_places(cls)
    k = lax.broadcasted_iota(jnp.int32, (1, 128), 1)
    same = times_seen(qn - ((k & 31) * 16 + (k >> 5) * 4 + cls) + keys)
    last = qn - ((24 + (k & 7)) * 16 + ((k >> 3) & 3) * 4 + (k >> 5)) + keys
    last = ((last <= SPAN) & ((k >> 5) != cls)).astype(F32)
    count = jnp.where(seen, jnp.concatenate([same, last], axis=1), 0.0)
    bias = jnp.where(count > 0, 0.0, LOW).astype(F32)
    key = jnp.concatenate([k_ref[mine, :], tail_ref[0]], axis=0)
    value = jnp.concatenate([v_ref[mine, :], tail_ref[1]], axis=0)
    state = merged(q_ref[...], key, value, bias, count, max_ref, sum_ref, acc_ref, s_ref, p_ref, stat_ref)
    for ref, part in zip((new_max, new_sum, new_acc), state):
        ref[...] = part


def far_kernel(backs, last, place_ref, q_ref, max_ref, sum_ref, acc_ref, *refs):
    count = len(backs)
    sources, outs = refs[: 2 * count], refs[2 * count :]
    s_ref, p_ref, stat_ref = outs[-3:]
    bias = jnp.concatenate([far_bias(place_ref[0], back) for back in backs], axis=1)
    key = jnp.concatenate([ref[...] for ref in sources[0::2]], axis=0)
    value = jnp.concatenate([ref[...] for ref in sources[1::2]], axis=0)
    m, total, acc = merged(q_ref[...], key, value, bias, None, max_ref, sum_ref, acc_ref, s_ref, p_ref, stat_ref)
    if last:
        cls = pl.program_id(0)
        out_ref, log_ref, att_ref = outs[:3]
        att_ref[pl.ds(pl.multiple_of(cls * 128, 128), 128), :] = (acc / total).astype(BF16)
        log_ref[...] = m + jnp.log(total)

        @pl.when(cls == pl.num_programs(0) - 1)
        def _():
            out_ref[...] = permuted(to_natural(att_ref.shape[0]), att_ref[...])
    else:
        for ref, part in zip(outs[:3], (m, total, acc)):
            ref[...] = part


def log_kernel(lw_ref, log_ref):
    rows, width = lw_ref.shape
    perm = to_natural(rows)
    rest = lw_ref[...]
    ordered = jnp.zeros((rows, width), F32)
    for _ in range(3):
        piece = rest.astype(BF16)
        rest = rest - piece.astype(F32)
        ordered = ordered + jnp.dot(perm, piece, preferred_element_type=F32)
    flipped = ordered.T
    for head in range(width // HEAD_DIM):
        log_ref[head : head + 1, :] = flipped[head * HEAD_DIM : head * HEAD_DIM + 1, :]


def out_kernel(place_ref, att_ref, own_ref, before_ref, after_ref, across_ref, keep_ref, give_ref, sum_ref):
    x, core = place_ref[2], place_ref[3]
    rows = keep_ref.shape[0]
    total = None
    for n, ref in enumerate((own_ref, before_ref, after_ref, across_ref)):
        part = jnp.dot(att_ref[lax.rem(x + HOPS[n], 4)], ref[...], preferred_element_type=F32)
        part = part.astype(BF16).astype(F32)
        total = part if total is None else total + part
    sum_ref[...] = total
    keep_ref[...] = sum_ref[pl.ds(pl.multiple_of(core * rows, rows), rows), :]
    give_ref[...] = sum_ref[pl.ds(pl.multiple_of((1 - core) * rows, rows), rows), :].astype(BF16)


def end_kernel(keep_ref, taken_ref, gain_ref, out_ref):
    summed = keep_ref[...] + taken_ref[...].astype(F32)
    scale = lax.rsqrt(jnp.mean(summed * summed, axis=1, keepdims=True) + EPS)
    out_ref[...] = (summed * scale * gain_ref[...]).astype(BF16)


SMEM = pl.BlockSpec(memory_space=pltpu.SMEM)
VMEM = pl.BlockSpec(memory_space=pltpu.VMEM)


def kernel_call(body, outs, args, flops, limit, scratch=(), **more):
    if "grid_spec" not in more:
        more["scratch_shapes"] = [pltpu.VMEM(s, t) for s, t in scratch]
    if "in_specs" not in more and "grid_spec" not in more:
        more["in_specs"] = [SMEM if a.dtype == jnp.int32 else VMEM for a in args]
        more["out_specs"] = tuple(VMEM for _ in outs)
    data = sum(a.size * a.dtype.itemsize for a in args)
    return pl.pallas_call(
        body,
        out_shape=tuple(jax.ShapeDtypeStruct(s, t) for s, t in outs),
        compiler_params=pltpu.CompilerParams(vmem_limit_bytes=limit * 1024 * 1024),
        cost_estimate=pl.CostEstimate(flops=flops, bytes_accessed=data, transcendentals=0),
        **more,
    )(*args)


def spread_to(value, axis, count):
    copies = jnp.broadcast_to(value[None], (count,) + value.shape)
    return lax.all_to_all(copies, axis, split_axis=0, concat_axis=0, tiled=True)


def layer(hidden_in, pre_gain, query_proj, key_proj, value_proj, out_proj, post_gain):
    rows, depth = hidden_in.shape
    width = query_proj.shape[1]
    heads = width // HEAD_DIM
    piece = rows // 8
    sp, x, core = lax.axis_index(SP), lax.axis_index("x"), lax.axis_index("c")
    place = jnp.stack([sp, lax.axis_index("zl"), x, core]).astype(jnp.int32)
    member = (x * 2 + core)[None].astype(jnp.int32)
    gain = pre_gain[None]
    row = (rows, width)

    copies = [jnp.broadcast_to(shard[None], (32,) + shard.shape) for shard in (key_proj, value_proj)]
    mine = lax.all_to_all(jnp.concatenate(copies, axis=2), ("zh", "y"), split_axis=0, concat_axis=0, tiled=True)
    mine = mine.reshape(4, 256, 2 * width)
    below = lax.ppermute(mine[:2], Z, ring(8, 1))
    above = lax.ppermute(mine[2:], Z, ring(8, -1))

    (eighth,) = kernel_call(
        slice_kernel,
        [((piece, depth), BF16)],
        (member, hidden_in, gain),
        10 * piece * depth,
        12,
        grid_spec=pltpu.PrefetchScalarGridSpec(
            num_scalar_prefetch=1,
            grid=(1,),
            in_specs=[pl.BlockSpec((piece, depth), lambda i, t: (t[0], 0)), pl.BlockSpec((1, depth), lambda i, t: (0, 0))],
            out_specs=[pl.BlockSpec((piece, depth), lambda i, t: (0, 0))],
        ),
    )
    fourth = lax.ppermute(eighth, SP, ring(64, 4))
    far_rows = spread_to(fourth, TP, 8).reshape(rows, depth)

    before = lax.ppermute(out_proj, "x", ring(4, 1))
    after = lax.ppermute(out_proj, "x", ring(4, -1))
    across = lax.ppermute(out_proj, "x", ring(4, 2))

    quarter = HEAD_DIM // 2
    frequency = ROPE_BASE ** (-(jnp.arange(quarter, dtype=F32) * 2.0 / HEAD_DIM))
    local = jnp.arange(rows, dtype=jnp.int32)
    positions = jnp.concatenate([(sp - 4) * rows + local, sp * rows + local]).astype(F32)
    angles = positions[None, :] * frequency[:, None]
    turns = jnp.stack([jnp.cos(angles), jnp.sin(angles)])

    normed, query = kernel_call(
        query_kernel, [((rows, depth), BF16), (row, BF16)], (hidden_in, gain, query_proj, turns), 2 * rows * depth * width, 12
    )
    block_rows = rows // 4
    row_part = pl.BlockSpec((block_rows, depth), lambda n: (n, 0))
    whole = pl.BlockSpec(row, lambda c: (0, 0))
    weight_spec = pl.BlockSpec((depth, 2 * width), lambda n: (0, 0))
    key, value, weights = kernel_call(
        key_value_kernel,
        [(row, BF16), (row, BF16), ((depth, 2 * width), BF16)],
        (place, normed, turns, mine, below, above),
        4 * rows * depth * width,
        14,
        [((rows, 2 * width), BF16)],
        grid=(4,),
        in_specs=[
            SMEM,
            row_part,
            pl.BlockSpec((2, HEAD_DIM // 2, block_rows), lambda n: (0, 0, 4 + n)),
            pl.BlockSpec((4, 256, 2 * width), lambda n: (0, 0, 0)),
            pl.BlockSpec((2, 256, 2 * width), lambda n: (0, 0, 0)),
            pl.BlockSpec((2, 256, 2 * width), lambda n: (0, 0, 0)),
        ],
        out_specs=(whole, whole, weight_spec),
    )
    forward = [(i, i + 1) for i in range(63)]
    keys, values = [key], [value]
    for _ in range(1, 4):
        keys.append(lax.ppermute(keys[-1], SP, forward))
        values.append(lax.ppermute(values[-1], SP, forward))
    key4, value4 = kernel_call(
        far_key_value_kernel,
        [(row, BF16)] * 2,
        (far_rows, turns, weights),
        4 * rows * depth * width,
        14,
        [((rows, 2 * width), BF16)],
        grid=(4,),
        in_specs=[row_part, pl.BlockSpec((2, HEAD_DIM // 2, block_rows), lambda n: (0, 0, n)), weight_spec],
        out_specs=(whole, whole),
    )

    part = pl.BlockSpec((128, width), lambda c: (c, 0))
    pair = ((512, 256), F32), ((512, 256), BF16), ((2, 512, width), F32)
    state = kernel_call(
        own_kernel,
        [(row, F32)] * 3,
        (query, keys[0], values[0]),
        8 * rows * rows * width,
        10,
        [((512, 512), F32), ((512, 512), BF16), ((128, 512), F32), ((128, 512), F32), ((2, 512, width), F32)],
        grid=(rows // 128,),
        in_specs=[part, whole, whole],
        out_specs=(part,) * 3,
    )
    state = kernel_call(
        before_kernel,
        [(row, F32)] * 3,
        (place, query, *state, keys[1], values[1]),
        4 * rows * rows * width,
        10,
        [*pair, ((2, 128, width), BF16)],
        grid=(rows // 128,),
        in_specs=[SMEM] + [part] * 4 + [whole, whole],
        out_specs=(part,) * 3,
    )
    sources = {2: (keys[2], values[2]), 3: (keys[3], values[3]), 4: (key4, value4)}
    for backs in ((2, 4), (3,)):
        last = backs == (3,)
        state = kernel_call(
            functools.partial(far_kernel, backs, last),
            [(row, BF16), (row, F32)] if last else [(row, F32)] * 3,
            (place, query, *state, *(array for back in backs for array in sources[back])),
            4 * rows * 512 * width * len(backs),
            10,
            ([(row, BF16)] if last else []) + [((512, 128 * len(backs)), t) for t in (F32, BF16)] + [((2, 512, width), F32)],
            grid=(rows // 128,),
            in_specs=[SMEM] + [part] * (4 + 2 * len(backs)),
            out_specs=(whole, part) if last else (part,) * 3,
        )
    attended, logs = state

    arrived = lax.all_to_all(attended.reshape(4, rows // 4, width), "x", split_axis=0, concat_axis=0, tiled=True)
    (log_weight,) = kernel_call(log_kernel, [((heads, rows), F32)], (logs,), 6 * rows * rows * width, 8)
    columns = depth // 4
    piece_spec = pl.BlockSpec((piece, columns), lambda n: (0, n))
    keep, give = kernel_call(
        out_kernel,
        [((piece, depth), F32), ((piece, depth), BF16)],
        (place, arrived, out_proj, before, after, across),
        2 * rows // 8 * depth * depth,
        12,
        [((2 * piece, columns), F32)],
        grid=(4,),
        in_specs=[SMEM, pl.BlockSpec((4, rows // 4, width), lambda n: (0, 0, 0))] + [pl.BlockSpec((width, columns), lambda n: (0, n))] * 4,
        out_specs=(piece_spec, piece_spec),
    )
    taken = lax.ppermute(give, "c", ring(2, 1))
    (layer_out,) = kernel_call(end_kernel, [((piece, depth), BF16)], (keep, taken, post_gain[None]), 10 * piece * depth, 8)
    return layer_out, log_weight


def solution(mesh):
    fine = Mesh(np.asarray(mesh.devices).reshape(4, 2, 8, 4, 2), ("zh", "zl", "y", "x", "c"))
    placed = (P(SP, None), P(), P(None, TP), P(SP, TP), P(SP, TP), P(TP, None), P())
    return jax.shard_map(
        layer,
        mesh=fine,
        in_specs=placed,
        out_specs=(P(SP + TP, None), P(TP, SP)),
        check_vma=False,
    )
```

```python
import functools

import jax
import jax.numpy as jnp
import numpy as np
from jax import lax
from jax.experimental import pallas as pl
from jax.experimental.pallas import tpu as pltpu
from jax.sharding import Mesh
from jax.sharding import PartitionSpec as P

HEAD_DIM = 64
SPAN = 128
EPS = 1e-06
ROPE_BASE = 10000.0
LOW = -1e30
SP = ("zh", "zl", "y")
Z = ("zh", "zl")
TP = ("x", "c")
F32 = jnp.float32
BF16 = jnp.bfloat16
NT = (((1,), (1,)), ((), ()))
HOPS = (0, 3, 1, 2)


def ring(count, steps):
    return [(i, (i + steps) % count) for i in range(count)]


def natural(i):
    return (i & 31) * 16 + ((i >> 5) & 3) * 4 + (i >> 7)


def to_residue(rows, columns=None):
    i = lax.broadcasted_iota(jnp.int32, (rows, rows), 0)
    if columns is None:
        columns = lax.broadcasted_iota(jnp.int32, (rows, rows), 1)
    return (natural(i) == columns).astype(BF16)


def to_natural(rows):
    i = lax.broadcasted_iota(jnp.int32, (rows, rows), 1)
    n = lax.broadcasted_iota(jnp.int32, (rows, rows), 0)
    return (natural(i) == n).astype(BF16)


def rotated(x, cos, sin):
    width = x.shape[1]
    lane = lax.broadcasted_iota(jnp.int32, x.shape, 1)
    other = jnp.where((lane & 63) < 32, pltpu.roll(x, width - 32, 1), pltpu.roll(x, 32, 1))
    return x * cos + other * sin


def permuted(perm, x):
    return jnp.dot(perm, x, preferred_element_type=F32).astype(BF16)


def normed_rows(x, gain):
    x = x.astype(F32)
    scale = lax.rsqrt(jnp.mean(x * x, axis=1, keepdims=True) + EPS)
    return (x * scale * gain).astype(BF16)


def spread(turn_ref, part):
    cos, sin = turn_ref[0, :, part], turn_ref[1, :, part]
    cos = jnp.concatenate([cos] * 4, axis=0).T
    sin = jnp.concatenate([-sin, sin] * 2, axis=0).T
    return jnp.concatenate([cos, cos], axis=1), jnp.concatenate([sin, sin], axis=1)


def query_kernel(hidden_ref, gain_ref, weight_ref, turn_ref, normed_ref, query_ref):
    rows = hidden_ref.shape[0]
    gain = gain_ref[...]

    def step(i, carry):
        part = pl.ds(pl.multiple_of(i * 64, 64), 64)
        normed_ref[part, :] = normed_rows(hidden_ref[part, :], gain)
        return carry

    lax.fori_loop(0, rows // 64, step, 0)
    query = jnp.dot(normed_ref[...], weight_ref[...], preferred_element_type=F32)
    cos, sin = spread(turn_ref, slice(0, rows))
    query = rotated(query, cos, sin).astype(BF16) * 0.125
    query_ref[...] = permuted(to_residue(rows), query)


def project(normed_ref, turn_ref, weight_ref, key_ref, value_ref, both_ref):
    rows, width = key_ref.shape
    block = normed_ref.shape[0]
    n = pl.program_id(0)
    cos, sin = spread(turn_ref, slice(0, block))
    both = jnp.dot(normed_ref[...], weight_ref[...], preferred_element_type=F32)
    part = pl.ds(pl.multiple_of(n * block, block), block)
    both_ref[part, :width] = rotated(both[:, :width], cos, sin).astype(BF16)
    both_ref[part, width:] = both[:, width:].astype(BF16)

    @pl.when(n == pl.num_programs(0) - 1)
    def _():
        ordered = permuted(to_residue(rows), both_ref[...])
        key_ref[...] = ordered[:, :width]
        value_ref[...] = ordered[:, width:]


def key_value_kernel(place_ref, normed_ref, turn_ref, mine_ref, below_ref, above_ref, key_ref, value_ref, weight_ref, both_ref):
    @pl.when(pl.program_id(0) == 0)
    def _():
        low = place_ref[1]
        slabs = []
        for k in range(4):
            slabs.append((2 * k + low, mine_ref, k))
        for k in range(2):
            slabs.append((2 * k + 1 - low, below_ref, k))
            slabs.append((2 * (k + 2) + 1 - low, above_ref, k))
        for place, ref, k in slabs:
            weight_ref[pl.ds(pl.multiple_of(place * 256, 256), 256), :] = ref[k]

    project(normed_ref, turn_ref, weight_ref, key_ref, value_ref, both_ref)


def stack_heads(q):
    lane = lax.broadcasted_iota(jnp.int32, q.shape, 1) >> 6
    return jnp.concatenate([jnp.where(lane == h, q, jnp.zeros_like(q)) for h in range(q.shape[1] // HEAD_DIM)], axis=0)


def own_heads(stacked):
    width = stacked.shape[1]
    heads = width // HEAD_DIM
    rows = stacked.shape[0] // heads
    lane = lax.broadcasted_iota(jnp.int32, (rows, width), 1) >> 6
    out = stacked[:rows]
    for h in range(1, heads):
        out = jnp.where(lane == h, stacked[h * rows : (h + 1) * rows], out)
    return out


def far_bias(block, back):
    qi = lax.broadcasted_iota(jnp.int32, (128, 128), 0)
    ki = lax.broadcasted_iota(jnp.int32, (128, 128), 1)
    ok = ((qi >> 5) == (ki >> 5)) & (block >= back)
    if back == 4:
        ok = ok & ((ki & 31) >= (qi & 31))
    return jnp.where(ok, 0.0, LOW).astype(F32)


def times_seen(o):
    count = (o <= SPAN).astype(F32)
    count = count + (((o & 3) == 0) & (o <= 4 * SPAN)).astype(F32)
    return count + ((o & 15) == 0).astype(F32)


def query_places(cls):
    i = lax.broadcasted_iota(jnp.int32, (128, 1), 0)
    return (i & 31) * 16 + (i >> 5) * 4 + cls


def own_kernel(q_ref, k_ref, v_ref, max_ref, sum_ref, acc_ref, s_ref, p_ref, bias_ref, count_ref, stat_ref):
    keys, width = k_ref.shape
    heads = width // HEAD_DIM
    o = query_places(pl.program_id(0)) - natural(lax.broadcasted_iota(jnp.int32, (1, keys), 1))
    count = jnp.where(o >= 0, times_seen(o), 0.0)
    count_ref[...] = count
    bias_ref[...] = jnp.where(count > 0, 0.0, LOW).astype(F32)
    s_ref[...] = lax.dot_general(stack_heads(q_ref[...]), k_ref[...], NT, preferred_element_type=F32)
    step = 32
    for r in range(0, heads * 128, step):
        mask = slice(r % 128, r % 128 + step)
        s = s_ref[r : r + step, :] + bias_ref[mask, :]
        m = jnp.max(s, axis=1, keepdims=True)
        p = jnp.exp(s - m) * count_ref[mask, :]
        stat_ref[0, r : r + step, :] = jnp.broadcast_to(m, (step, width))
        stat_ref[1, r : r + step, :] = jnp.broadcast_to(jnp.sum(p, axis=1, keepdims=True), (step, width))
        p_ref[r : r + step, :] = p.astype(BF16)
    pv = jnp.dot(p_ref[...], v_ref[...], preferred_element_type=F32)
    max_ref[...] = own_heads(stat_ref[0])
    sum_ref[...] = own_heads(stat_ref[1])
    acc_ref[...] = own_heads(pv)


def merged(q, key, value, bias, count, max_ref, sum_ref, acc_ref, s_ref, p_ref, stat_ref):
    width = max_ref.shape[1]
    s_ref[...] = lax.dot_general(stack_heads(q), key, NT, preferred_element_type=F32)
    for h in range(width // HEAD_DIM):
        part = slice(h * 128, (h + 1) * 128)
        s = s_ref[part, :] + bias
        m = jnp.maximum(jnp.max(s, axis=1, keepdims=True), max_ref[:, h * HEAD_DIM : h * HEAD_DIM + 1])
        p = jnp.exp(s - m)
        if count is not None:
            p = p * count
        p_ref[part, :] = p.astype(BF16)
        stat_ref[0, part, :] = jnp.broadcast_to(m, (128, width))
        stat_ref[1, part, :] = jnp.broadcast_to(jnp.sum(p, axis=1, keepdims=True), (128, width))
    pv = jnp.dot(p_ref[...], value, preferred_element_type=F32)
    m = own_heads(stat_ref[0])
    alpha = jnp.exp(max_ref[...] - m)
    total = sum_ref[...] * alpha + own_heads(stat_ref[1])
    return m, total, acc_ref[...] * alpha + own_heads(pv)


def before_kernel(place_ref, q_ref, max_ref, sum_ref, acc_ref, k_ref, v_ref, new_max, new_sum, new_acc, s_ref, p_ref, stat_ref, tail_ref):
    cls = pl.program_id(0)
    keys = k_ref.shape[0]
    mine = pl.ds(pl.multiple_of(cls * 128, 128), 128)

    @pl.when(cls == 0)
    def _():
        j = lax.broadcasted_iota(jnp.int32, (128, keys), 0)
        i = lax.broadcasted_iota(jnp.int32, (128, keys), 1)
        pick = (i == (j >> 3) * 32 + 24 + (j & 7)).astype(BF16)
        tail_ref[0] = permuted(pick, k_ref[...])
        tail_ref[1] = permuted(pick, v_ref[...])

    seen = place_ref[0] >= 1
    qn = query_places(cls)
    k = lax.broadcasted_iota(jnp.int32, (1, 128), 1)
    same = times_seen(qn - ((k & 31) * 16 + (k >> 5) * 4 + cls) + keys)
    last = qn - ((24 + (k & 7)) * 16 + ((k >> 3) & 3) * 4 + (k >> 5)) + keys
    last = ((last <= SPAN) & ((k >> 5) != cls)).astype(F32)
    count = jnp.where(seen, jnp.concatenate([same, last], axis=1), 0.0)
    bias = jnp.where(count > 0, 0.0, LOW).astype(F32)
    key = jnp.concatenate([k_ref[mine, :], tail_ref[0]], axis=0)
    value = jnp.concatenate([v_ref[mine, :], tail_ref[1]], axis=0)
    state = merged(q_ref[...], key, value, bias, count, max_ref, sum_ref, acc_ref, s_ref, p_ref, stat_ref)
    for ref, part in zip((new_max, new_sum, new_acc), state):
        ref[...] = part


def far_kernel(backs, last, place_ref, q_ref, max_ref, sum_ref, acc_ref, *refs):
    count = len(backs)
    sources, outs = refs[: 2 * count], refs[2 * count :]
    s_ref, p_ref, stat_ref = outs[-3:]
    bias = jnp.concatenate([far_bias(place_ref[0], back) for back in backs], axis=1)
    key = jnp.concatenate([ref[...] for ref in sources[0::2]], axis=0)
    value = jnp.concatenate([ref[...] for ref in sources[1::2]], axis=0)
    m, total, acc = merged(q_ref[...], key, value, bias, None, max_ref, sum_ref, acc_ref, s_ref, p_ref, stat_ref)
    if last:
        cls = pl.program_id(0)
        out_ref, log_ref, att_ref = outs[:3]
        att_ref[pl.ds(pl.multiple_of(cls * 128, 128), 128), :] = (acc / total).astype(BF16)
        log_ref[...] = m + jnp.log(total)

        @pl.when(cls == pl.num_programs(0) - 1)
        def _():
            out_ref[...] = permuted(to_natural(att_ref.shape[0]), att_ref[...])
    else:
        for ref, part in zip(outs[:3], (m, total, acc)):
            ref[...] = part


def log_kernel(lw_ref, log_ref):
    rows, width = lw_ref.shape
    perm = to_natural(rows)
    rest = lw_ref[...]
    ordered = jnp.zeros((rows, width), F32)
    for _ in range(3):
        piece = rest.astype(BF16)
        rest = rest - piece.astype(F32)
        ordered = ordered + jnp.dot(perm, piece, preferred_element_type=F32)
    flipped = ordered.T
    for head in range(width // HEAD_DIM):
        log_ref[head : head + 1, :] = flipped[head * HEAD_DIM : head * HEAD_DIM + 1, :]


def out_kernel(place_ref, att_ref, *refs):
    weights, (gain_ref, out_ref, sum_ref) = refs[:8], refs[8:]
    x, core = place_ref[2], place_ref[3]
    n = pl.program_id(0)
    columns = weights[0].shape[1]
    total = None
    for half, c in enumerate((core, 1 - core)):
        for k, hop in enumerate(HOPS):
            group = lax.rem(x + hop, 4) * 2 + c
            part = jnp.dot(att_ref[group], weights[half * 4 + k][...], preferred_element_type=F32)
            part = part.astype(BF16).astype(F32)
            total = part if total is None else total + part
    sum_ref[:, pl.ds(pl.multiple_of(n * columns, columns), columns)] = total

    @pl.when(n == pl.num_programs(0) - 1)
    def _():
        summed = sum_ref[...]
        scale = lax.rsqrt(jnp.mean(summed * summed, axis=1, keepdims=True) + EPS)
        out_ref[...] = (summed * scale * gain_ref[...]).astype(BF16)


SMEM = pl.BlockSpec(memory_space=pltpu.SMEM)
VMEM = pl.BlockSpec(memory_space=pltpu.VMEM)


def kernel_call(body, outs, args, flops, limit, scratch=(), **more):
    if "grid_spec" not in more:
        more["scratch_shapes"] = [pltpu.VMEM(s, t) for s, t in scratch]
    if "in_specs" not in more and "grid_spec" not in more:
        more["in_specs"] = [SMEM if a.dtype == jnp.int32 else VMEM for a in args]
        more["out_specs"] = tuple(VMEM for _ in outs)
    data = sum(a.size * a.dtype.itemsize for a in args)
    return pl.pallas_call(
        body,
        out_shape=tuple(jax.ShapeDtypeStruct(s, t) for s, t in outs),
        compiler_params=pltpu.CompilerParams(vmem_limit_bytes=limit * 1024 * 1024),
        cost_estimate=pl.CostEstimate(flops=flops, bytes_accessed=data, transcendentals=0),
        **more,
    )(*args)


def layer(hidden_in, pre_gain, query_proj, key_proj, value_proj, out_proj, post_gain):
    rows, depth = hidden_in.shape
    width = query_proj.shape[1]
    heads = width // HEAD_DIM
    piece = rows // 8
    sp, x, core = lax.axis_index(SP), lax.axis_index("x"), lax.axis_index("c")
    place = jnp.stack([sp, lax.axis_index("zl"), x, core]).astype(jnp.int32)
    gain = pre_gain[None]
    row = (rows, width)

    copies = [jnp.broadcast_to(shard[None], (32,) + shard.shape) for shard in (key_proj, value_proj)]
    mine = lax.all_to_all(jnp.concatenate(copies, axis=2), ("zh", "y"), split_axis=0, concat_axis=0, tiled=True)
    mine = mine.reshape(4, 256, 2 * width)
    below = lax.ppermute(mine[:2], Z, ring(8, 1))
    above = lax.ppermute(mine[2:], Z, ring(8, -1))

    groups = [out_proj]
    for steps in (1, -1, 2):
        groups.append(lax.ppermute(out_proj, "x", ring(4, steps)))
    for n in range(4):
        groups.append(lax.ppermute(groups[n], "c", ring(2, 1)))

    quarter = HEAD_DIM // 2
    frequency = ROPE_BASE ** (-(jnp.arange(quarter, dtype=F32) * 2.0 / HEAD_DIM))
    positions = (sp * rows + jnp.arange(rows, dtype=jnp.int32)).astype(F32)
    angles = positions[None, :] * frequency[:, None]
    turns = jnp.stack([jnp.cos(angles), jnp.sin(angles)])

    normed, query = kernel_call(
        query_kernel, [((rows, depth), BF16), (row, BF16)], (hidden_in, gain, query_proj, turns), 2 * rows * depth * width, 12
    )
    block_rows = rows // 4
    row_part = pl.BlockSpec((block_rows, depth), lambda n: (n, 0))
    whole = pl.BlockSpec(row, lambda c: (0, 0))
    key, value = kernel_call(
        key_value_kernel,
        [(row, BF16)] * 2,
        (place, normed, turns, mine, below, above),
        4 * rows * depth * width,
        14,
        [((depth, 2 * width), BF16), ((rows, 2 * width), BF16)],
        grid=(4,),
        in_specs=[
            SMEM,
            row_part,
            pl.BlockSpec((2, HEAD_DIM // 2, block_rows), lambda n: (0, 0, n)),
            pl.BlockSpec((4, 256, 2 * width), lambda n: (0, 0, 0)),
            pl.BlockSpec((2, 256, 2 * width), lambda n: (0, 0, 0)),
            pl.BlockSpec((2, 256, 2 * width), lambda n: (0, 0, 0)),
        ],
        out_specs=(whole, whole),
    )
    forward = [(i, i + 1) for i in range(63)]
    keys, values = [key], [value]
    for _ in range(1, 5):
        keys.append(lax.ppermute(keys[-1], SP, forward))
        values.append(lax.ppermute(values[-1], SP, forward))
    part = pl.BlockSpec((128, width), lambda c: (c, 0))
    pair = ((512, 256), F32), ((512, 256), BF16), ((2, 512, width), F32)
    state = kernel_call(
        own_kernel,
        [(row, F32)] * 3,
        (query, keys[0], values[0]),
        8 * rows * rows * width,
        10,
        [((512, 512), F32), ((512, 512), BF16), ((128, 512), F32), ((128, 512), F32), ((2, 512, width), F32)],
        grid=(rows // 128,),
        in_specs=[part, whole, whole],
        out_specs=(part,) * 3,
    )
    state = kernel_call(
        before_kernel,
        [(row, F32)] * 3,
        (place, query, *state, keys[1], values[1]),
        4 * rows * rows * width,
        10,
        [*pair, ((2, 128, width), BF16)],
        grid=(rows // 128,),
        in_specs=[SMEM] + [part] * 4 + [whole, whole],
        out_specs=(part,) * 3,
    )
    for back in (2, 3, 4):
        last = back == 4
        state = kernel_call(
            functools.partial(far_kernel, (back,), last),
            [(row, BF16), (row, F32)] if last else [(row, F32)] * 3,
            (place, query, *state, keys[back], values[back]),
            4 * rows * 512 * width,
            10,
            ([(row, BF16)] if last else []) + [((512, 128), t) for t in (F32, BF16)] + [((2, 512, width), F32)],
            grid=(rows // 128,),
            in_specs=[SMEM] + [part] * 6,
            out_specs=(whole, part) if last else (part,) * 3,
        )
    attended, logs = state

    arrived = lax.all_to_all(attended.reshape(8, piece, width), TP, split_axis=0, concat_axis=0, tiled=True)
    (log_weight,) = kernel_call(log_kernel, [((heads, rows), F32)], (logs,), 6 * rows * rows * width, 8)
    columns = depth // 4
    (layer_out,) = kernel_call(
        out_kernel,
        [((piece, depth), BF16)],
        (place, arrived, *groups, post_gain[None]),
        2 * piece * depth * depth,
        12,
        [((piece, depth), F32)],
        grid=(4,),
        in_specs=[SMEM, pl.BlockSpec((8, piece, width), lambda n: (0, 0, 0))]
        + [pl.BlockSpec((width, columns), lambda n: (0, n))] * 8
        + [pl.BlockSpec((1, depth), lambda n: (0, 0))],
        out_specs=(pl.BlockSpec((piece, depth), lambda n: (0, 0)),),
    )
    return layer_out, log_weight


def solution(mesh):
    fine = Mesh(np.asarray(mesh.devices).reshape(4, 2, 8, 4, 2), ("zh", "zl", "y", "x", "c"))
    placed = (P(SP, None), P(), P(None, TP), P(SP, TP), P(SP, TP), P(TP, None), P())
    return jax.shard_map(
        layer,
        mesh=fine,
        in_specs=placed,
        out_specs=(P(SP + TP, None), P(TP, SP)),
        check_vma=False,
    )
```

```python
import functools

import jax
import jax.numpy as jnp
import numpy as np
from jax import lax
from jax.experimental import pallas as pl
from jax.experimental.pallas import tpu as pltpu
from jax.sharding import Mesh
from jax.sharding import PartitionSpec as P

HEAD_DIM = 64
SPAN = 128
EPS = 1e-06
ROPE_BASE = 10000.0
LOW = -1e30
SP = ("zh", "zl", "y")
Z = ("zh", "zl")
TP = ("x", "c")
F32 = jnp.float32
BF16 = jnp.bfloat16
NT = (((1,), (1,)), ((), ()))
HOPS = (0, 3, 1, 2)


def ring(count, steps):
    return [(i, (i + steps) % count) for i in range(count)]


def natural(i):
    return (i & 31) * 16 + ((i >> 5) & 3) * 4 + (i >> 7)


def to_residue(rows, columns=None):
    i = lax.broadcasted_iota(jnp.int32, (rows, rows), 0)
    if columns is None:
        columns = lax.broadcasted_iota(jnp.int32, (rows, rows), 1)
    return (natural(i) == columns).astype(BF16)


def to_natural(rows):
    i = lax.broadcasted_iota(jnp.int32, (rows, rows), 1)
    n = lax.broadcasted_iota(jnp.int32, (rows, rows), 0)
    return (natural(i) == n).astype(BF16)


def rotated(x, cos, sin):
    width = x.shape[1]
    lane = lax.broadcasted_iota(jnp.int32, x.shape, 1)
    other = jnp.where((lane & 63) < 32, pltpu.roll(x, width - 32, 1), pltpu.roll(x, 32, 1))
    return x * cos + other * sin


def permuted(perm, x):
    return jnp.dot(perm, x, preferred_element_type=F32).astype(BF16)


def normed_rows(x, gain):
    x = x.astype(F32)
    scale = lax.rsqrt(jnp.mean(x * x, axis=1, keepdims=True) + EPS)
    return (x * scale * gain).astype(BF16)


def spread(turn_ref, part):
    cos, sin = turn_ref[0, :, part], turn_ref[1, :, part]
    cos = jnp.concatenate([cos] * 4, axis=0).T
    sin = jnp.concatenate([-sin, sin] * 2, axis=0).T
    return jnp.concatenate([cos, cos], axis=1), jnp.concatenate([sin, sin], axis=1)


def query_kernel(hidden_ref, gain_ref, weight_ref, turn_ref, normed_ref, query_ref):
    rows = hidden_ref.shape[0]
    gain = gain_ref[...]

    def step(i, carry):
        part = pl.ds(pl.multiple_of(i * 64, 64), 64)
        normed_ref[part, :] = normed_rows(hidden_ref[part, :], gain)
        return carry

    lax.fori_loop(0, rows // 64, step, 0)
    query = jnp.dot(normed_ref[...], weight_ref[...], preferred_element_type=F32)
    cos, sin = spread(turn_ref, slice(0, rows))
    query = rotated(query, cos, sin).astype(BF16) * 0.125
    query_ref[...] = permuted(to_residue(rows), query)


def copies_kernel(key_ref, value_ref, out_ref):
    both = jnp.concatenate([key_ref[...], value_ref[...]], axis=1)
    for n in range(out_ref.shape[0]):
        out_ref[n] = both


def assembled(place_ref, mine_ref, below_ref, above_ref, weight_ref, columns):
    low = place_ref[1]
    for k in range(4):
        weight_ref[pl.ds(pl.multiple_of((2 * k + low) * 256, 256), 256), :] = mine_ref[k, :, columns]
    for k in range(2):
        weight_ref[pl.ds(pl.multiple_of((2 * k + 1 - low) * 256, 256), 256), :] = below_ref[k]
        weight_ref[pl.ds(pl.multiple_of((2 * k + 5 - low) * 256, 256), 256), :] = above_ref[k]


def key_kernel(place_ref, normed_ref, mine_ref, below_ref, above_ref, turn_ref, key_ref, weight_ref):
    rows, width = key_ref.shape
    assembled(place_ref, mine_ref, below_ref, above_ref, weight_ref, slice(0, width))
    key = jnp.dot(normed_ref[...], weight_ref[...], preferred_element_type=F32)
    key = rotated(key, *spread(turn_ref, slice(0, rows))).astype(BF16)
    key_ref[...] = permuted(to_residue(rows), key)


def value_kernel(place_ref, normed_ref, mine_ref, below_ref, above_ref, value_ref, weight_ref):
    rows, width = value_ref.shape
    assembled(place_ref, mine_ref, below_ref, above_ref, weight_ref, slice(width, 2 * width))
    value = jnp.dot(normed_ref[...], weight_ref[...], preferred_element_type=F32).astype(BF16)
    value_ref[...] = permuted(to_residue(rows), value)


def stack_heads(q):
    lane = lax.broadcasted_iota(jnp.int32, q.shape, 1) >> 6
    return jnp.concatenate([jnp.where(lane == h, q, jnp.zeros_like(q)) for h in range(q.shape[1] // HEAD_DIM)], axis=0)


def own_heads(stacked):
    width = stacked.shape[1]
    heads = width // HEAD_DIM
    rows = stacked.shape[0] // heads
    lane = lax.broadcasted_iota(jnp.int32, (rows, width), 1) >> 6
    out = stacked[:rows]
    for h in range(1, heads):
        out = jnp.where(lane == h, stacked[h * rows : (h + 1) * rows], out)
    return out


def far_bias(block, back):
    qi = lax.broadcasted_iota(jnp.int32, (128, 128), 0)
    ki = lax.broadcasted_iota(jnp.int32, (128, 128), 1)
    ok = ((qi >> 5) == (ki >> 5)) & (block >= back)
    if back == 4:
        ok = ok & ((ki & 31) >= (qi & 31))
    return jnp.where(ok, 0.0, LOW).astype(F32)


def times_seen(o):
    count = (o <= SPAN).astype(F32)
    count = count + (((o & 3) == 0) & (o <= 4 * SPAN)).astype(F32)
    return count + ((o & 15) == 0).astype(F32)


def query_places(cls):
    i = lax.broadcasted_iota(jnp.int32, (128, 1), 0)
    return (i & 31) * 16 + (i >> 5) * 4 + cls


def own_kernel(q_ref, k_ref, v_ref, max_ref, sum_ref, acc_ref, s_ref, p_ref, bias_ref, count_ref, stat_ref):
    keys, width = k_ref.shape
    heads = width // HEAD_DIM
    o = query_places(pl.program_id(0)) - natural(lax.broadcasted_iota(jnp.int32, (1, keys), 1))
    count = jnp.where(o >= 0, times_seen(o), 0.0)
    count_ref[...] = count
    bias_ref[...] = jnp.where(count > 0, 0.0, LOW).astype(F32)
    s_ref[...] = lax.dot_general(stack_heads(q_ref[...]), k_ref[...], NT, preferred_element_type=F32)
    step = 32
    for r in range(0, heads * 128, step):
        mask = slice(r % 128, r % 128 + step)
        s = s_ref[r : r + step, :] + bias_ref[mask, :]
        m = jnp.max(s, axis=1, keepdims=True)
        p = jnp.exp(s - m) * count_ref[mask, :]
        stat_ref[0, r : r + step, :] = jnp.broadcast_to(m, (step, width))
        stat_ref[1, r : r + step, :] = jnp.broadcast_to(jnp.sum(p, axis=1, keepdims=True), (step, width))
        p_ref[r : r + step, :] = p.astype(BF16)
    pv = jnp.dot(p_ref[...], v_ref[...], preferred_element_type=F32)
    max_ref[...] = own_heads(stat_ref[0])
    sum_ref[...] = own_heads(stat_ref[1])
    acc_ref[...] = own_heads(pv)


def merged(q, key, value, bias, count, max_ref, sum_ref, acc_ref, s_ref, p_ref, stat_ref):
    width = max_ref.shape[1]
    s_ref[...] = lax.dot_general(stack_heads(q), key, NT, preferred_element_type=F32)
    for h in range(width // HEAD_DIM):
        part = slice(h * 128, (h + 1) * 128)
        s = s_ref[part, :] + bias
        m = jnp.maximum(jnp.max(s, axis=1, keepdims=True), max_ref[:, h * HEAD_DIM : h * HEAD_DIM + 1])
        p = jnp.exp(s - m)
        if count is not None:
            p = p * count
        p_ref[part, :] = p.astype(BF16)
        stat_ref[0, part, :] = jnp.broadcast_to(m, (128, width))
        stat_ref[1, part, :] = jnp.broadcast_to(jnp.sum(p, axis=1, keepdims=True), (128, width))
    pv = jnp.dot(p_ref[...], value, preferred_element_type=F32)
    m = own_heads(stat_ref[0])
    alpha = jnp.exp(max_ref[...] - m)
    total = sum_ref[...] * alpha + own_heads(stat_ref[1])
    return m, total, acc_ref[...] * alpha + own_heads(pv)


def before_kernel(place_ref, q_ref, max_ref, sum_ref, acc_ref, k_ref, v_ref, new_max, new_sum, new_acc, s_ref, p_ref, stat_ref, tail_ref):
    cls = pl.program_id(0)
    keys = k_ref.shape[0]
    mine = pl.ds(pl.multiple_of(cls * 128, 128), 128)

    @pl.when(cls == 0)
    def _():
        j = lax.broadcasted_iota(jnp.int32, (128, keys), 0)
        i = lax.broadcasted_iota(jnp.int32, (128, keys), 1)
        pick = (i == (j >> 3) * 32 + 24 + (j & 7)).astype(BF16)
        tail_ref[0] = permuted(pick, k_ref[...])
        tail_ref[1] = permuted(pick, v_ref[...])

    seen = place_ref[0] >= 1
    qn = query_places(cls)
    k = lax.broadcasted_iota(jnp.int32, (1, 128), 1)
    same = times_seen(qn - ((k & 31) * 16 + (k >> 5) * 4 + cls) + keys)
    last = qn - ((24 + (k & 7)) * 16 + ((k >> 3) & 3) * 4 + (k >> 5)) + keys
    last = ((last <= SPAN) & ((k >> 5) != cls)).astype(F32)
    count = jnp.where(seen, jnp.concatenate([same, last], axis=1), 0.0)
    bias = jnp.where(count > 0, 0.0, LOW).astype(F32)
    key = jnp.concatenate([k_ref[mine, :], tail_ref[0]], axis=0)
    value = jnp.concatenate([v_ref[mine, :], tail_ref[1]], axis=0)
    state = merged(q_ref[...], key, value, bias, count, max_ref, sum_ref, acc_ref, s_ref, p_ref, stat_ref)
    for ref, part in zip((new_max, new_sum, new_acc), state):
        ref[...] = part


def far_kernel(backs, last, place_ref, q_ref, max_ref, sum_ref, acc_ref, *refs):
    count = len(backs)
    sources, outs = refs[: 2 * count], refs[2 * count :]
    s_ref, p_ref, stat_ref = outs[-3:]
    bias = jnp.concatenate([far_bias(place_ref[0], back) for back in backs], axis=1)
    key = jnp.concatenate([ref[...] for ref in sources[0::2]], axis=0)
    value = jnp.concatenate([ref[...] for ref in sources[1::2]], axis=0)
    m, total, acc = merged(q_ref[...], key, value, bias, None, max_ref, sum_ref, acc_ref, s_ref, p_ref, stat_ref)
    if last:
        cls = pl.program_id(0)
        out_ref, log_ref, att_ref = outs[:3]
        att_ref[pl.ds(pl.multiple_of(cls * 128, 128), 128), :] = (acc / total).astype(BF16)
        log_ref[...] = m + jnp.log(total)

        @pl.when(cls == pl.num_programs(0) - 1)
        def _():
            out_ref[...] = permuted(to_natural(att_ref.shape[0]), att_ref[...])
    else:
        for ref, part in zip(outs[:3], (m, total, acc)):
            ref[...] = part


def log_kernel(lw_ref, log_ref):
    rows, width = lw_ref.shape
    perm = to_natural(rows)
    rest = lw_ref[...]
    ordered = jnp.zeros((rows, width), F32)
    for _ in range(3):
        piece = rest.astype(BF16)
        rest = rest - piece.astype(F32)
        ordered = ordered + jnp.dot(perm, piece, preferred_element_type=F32)
    flipped = ordered.T
    for head in range(width // HEAD_DIM):
        log_ref[head : head + 1, :] = flipped[head * HEAD_DIM : head * HEAD_DIM + 1, :]


def out_kernel(place_ref, att_ref, *refs):
    weights, (gain_ref, out_ref, sum_ref) = refs[:8], refs[8:]
    x, core = place_ref[2], place_ref[3]
    n = pl.program_id(0)
    columns = weights[0].shape[1]
    total = None
    for half, c in enumerate((core, 1 - core)):
        for k, hop in enumerate(HOPS):
            group = lax.rem(x + hop, 4) * 2 + c
            part = jnp.dot(att_ref[group], weights[half * 4 + k][...], preferred_element_type=F32)
            part = part.astype(BF16).astype(F32)
            total = part if total is None else total + part
    sum_ref[:, pl.ds(pl.multiple_of(n * columns, columns), columns)] = total

    @pl.when(n == pl.num_programs(0) - 1)
    def _():
        summed = sum_ref[...]
        scale = lax.rsqrt(jnp.mean(summed * summed, axis=1, keepdims=True) + EPS)
        out_ref[...] = (summed * scale * gain_ref[...]).astype(BF16)


SMEM = pl.BlockSpec(memory_space=pltpu.SMEM)
VMEM = pl.BlockSpec(memory_space=pltpu.VMEM)


def kernel_call(body, outs, args, flops, limit, scratch=(), **more):
    if "grid_spec" not in more:
        more["scratch_shapes"] = [pltpu.VMEM(s, t) for s, t in scratch]
    if "in_specs" not in more and "grid_spec" not in more:
        more["in_specs"] = [SMEM if a.dtype == jnp.int32 else VMEM for a in args]
        more["out_specs"] = tuple(VMEM for _ in outs)
    data = sum(a.size * a.dtype.itemsize for a in args)
    return pl.pallas_call(
        body,
        out_shape=tuple(jax.ShapeDtypeStruct(s, t) for s, t in outs),
        compiler_params=pltpu.CompilerParams(vmem_limit_bytes=limit * 1024 * 1024),
        cost_estimate=pl.CostEstimate(flops=flops, bytes_accessed=data, transcendentals=0),
        **more,
    )(*args)


def layer(hidden_in, pre_gain, query_proj, key_proj, value_proj, out_proj, post_gain):
    rows, depth = hidden_in.shape
    width = query_proj.shape[1]
    heads = width // HEAD_DIM
    piece = rows // 8
    sp, x, core = lax.axis_index(SP), lax.axis_index("x"), lax.axis_index("c")
    place = jnp.stack([sp, lax.axis_index("zl"), x, core]).astype(jnp.int32)
    gain = pre_gain[None]
    row = (rows, width)

    (copies,) = kernel_call(copies_kernel, [((32, key_proj.shape[0], 2 * width), BF16)], (key_proj, value_proj), 1000, 8)
    mine = lax.all_to_all(copies, ("zh", "y"), split_axis=0, concat_axis=0, tiled=True)
    mine = mine.reshape(4, 256, 2 * width)
    slabs = []
    for columns in (slice(0, width), slice(width, 2 * width)):
        below = lax.ppermute(mine[:2, :, columns], Z, ring(8, 1))
        above = lax.ppermute(mine[2:, :, columns], Z, ring(8, -1))
        slabs.append((mine, below, above))

    groups = [out_proj]
    for steps in (1, -1, 2):
        groups.append(lax.ppermute(out_proj, "x", ring(4, steps)))
    for n in range(4):
        groups.append(lax.ppermute(groups[n], "c", ring(2, 1)))

    quarter = HEAD_DIM // 2
    frequency = ROPE_BASE ** (-(jnp.arange(quarter, dtype=F32) * 2.0 / HEAD_DIM))
    positions = (sp * rows + jnp.arange(rows, dtype=jnp.int32)).astype(F32)
    angles = positions[None, :] * frequency[:, None]
    turns = jnp.stack([jnp.cos(angles), jnp.sin(angles)])

    normed, query = kernel_call(
        query_kernel, [((rows, depth), BF16), (row, BF16)], (hidden_in, gain, query_proj, turns), 2 * rows * depth * width, 12
    )
    weight = [((depth, width), BF16)]
    (key,) = kernel_call(key_kernel, [(row, BF16)], (place, normed, *slabs[0], turns), 2 * rows * depth * width, 14, weight)
    (value,) = kernel_call(value_kernel, [(row, BF16)], (place, normed, *slabs[1]), 2 * rows * depth * width, 14, weight)
    forward = [(i, i + 1) for i in range(63)]
    keys, values = [key], [value]
    for _ in range(1, 5):
        keys.append(lax.ppermute(keys[-1], SP, forward))
        values.append(lax.ppermute(values[-1], SP, forward))
    whole = pl.BlockSpec(row, lambda c: (0, 0))
    part = pl.BlockSpec((128, width), lambda c: (c, 0))
    pair = ((512, 256), F32), ((512, 256), BF16), ((2, 512, width), F32)
    state = kernel_call(
        own_kernel,
        [(row, F32)] * 3,
        (query, keys[0], values[0]),
        8 * rows * rows * width,
        10,
        [((512, 512), F32), ((512, 512), BF16), ((128, 512), F32), ((128, 512), F32), ((2, 512, width), F32)],
        grid=(rows // 128,),
        in_specs=[part, whole, whole],
        out_specs=(part,) * 3,
    )
    state = kernel_call(
        before_kernel,
        [(row, F32)] * 3,
        (place, query, *state, keys[1], values[1]),
        4 * rows * rows * width,
        10,
        [*pair, ((2, 128, width), BF16)],
        grid=(rows // 128,),
        in_specs=[SMEM] + [part] * 4 + [whole, whole],
        out_specs=(part,) * 3,
    )
    for back in (2, 3, 4):
        last = back == 4
        state = kernel_call(
            functools.partial(far_kernel, (back,), last),
            [(row, BF16), (row, F32)] if last else [(row, F32)] * 3,
            (place, query, *state, keys[back], values[back]),
            4 * rows * 512 * width,
            16,
            ([(row, BF16)] if last else []) + [((512, 128), t) for t in (F32, BF16)] + [((2, 512, width), F32)],
            grid=(rows // 128,),
            in_specs=[SMEM] + [part] * 6,
            out_specs=(whole, part) if last else (part,) * 3,
        )
    attended, logs = state

    arrived = lax.all_to_all(attended.reshape(8, piece, width), TP, split_axis=0, concat_axis=0, tiled=True)
    (log_weight,) = kernel_call(log_kernel, [((heads, rows), F32)], (logs,), 6 * rows * rows * width, 8)
    columns = depth // 4
    (layer_out,) = kernel_call(
        out_kernel,
        [((piece, depth), BF16)],
        (place, arrived, *groups, post_gain[None]),
        2 * piece * depth * depth,
        12,
        [((piece, depth), F32)],
        grid=(4,),
        in_specs=[SMEM, pl.BlockSpec((8, piece, width), lambda n: (0, 0, 0))]
        + [pl.BlockSpec((width, columns), lambda n: (0, n))] * 8
        + [pl.BlockSpec((1, depth), lambda n: (0, 0))],
        out_specs=(pl.BlockSpec((piece, depth), lambda n: (0, 0)),),
    )
    return layer_out, log_weight


def solution(mesh):
    fine = Mesh(np.asarray(mesh.devices).reshape(4, 2, 8, 4, 2), ("zh", "zl", "y", "x", "c"))
    placed = (P(SP, None), P(), P(None, TP), P(SP, TP), P(SP, TP), P(TP, None), P())
    return jax.shard_map(
        layer,
        mesh=fine,
        in_specs=placed,
        out_specs=(P(SP + TP, None), P(TP, SP)),
        check_vma=False,
    )
```

```python
import functools

import jax
import jax.numpy as jnp
import numpy as np
from jax import lax
from jax.experimental import pallas as pl
from jax.experimental.pallas import tpu as pltpu
from jax.sharding import Mesh
from jax.sharding import PartitionSpec as P

HEAD_DIM = 64
SPAN = 128
EPS = 1e-06
ROPE_BASE = 10000.0
LOW = -1e30
SP = ("zh", "zl", "y")
Z = ("zh", "zl")
TP = ("x", "c")
F32 = jnp.float32
BF16 = jnp.bfloat16
NT = (((1,), (1,)), ((), ()))
HOPS = (0, 3, 1, 2)


def ring(count, steps):
    return [(i, (i + steps) % count) for i in range(count)]


def natural(i):
    return (i & 31) * 16 + ((i >> 5) & 3) * 4 + (i >> 7)


def to_residue(rows, columns=None):
    i = lax.broadcasted_iota(jnp.int32, (rows, rows), 0)
    if columns is None:
        columns = lax.broadcasted_iota(jnp.int32, (rows, rows), 1)
    return (natural(i) == columns).astype(BF16)


def to_natural(rows):
    i = lax.broadcasted_iota(jnp.int32, (rows, rows), 1)
    n = lax.broadcasted_iota(jnp.int32, (rows, rows), 0)
    return (natural(i) == n).astype(BF16)


def rotated(x, cos, sin):
    width = x.shape[1]
    lane = lax.broadcasted_iota(jnp.int32, x.shape, 1)
    other = jnp.where((lane & 63) < 32, pltpu.roll(x, width - 32, 1), pltpu.roll(x, 32, 1))
    return x * cos + other * sin


def permuted(perm, x):
    return jnp.dot(perm, x, preferred_element_type=F32).astype(BF16)


def normed_rows(x, gain):
    x = x.astype(F32)
    scale = lax.rsqrt(jnp.mean(x * x, axis=1, keepdims=True) + EPS)
    return (x * scale * gain).astype(BF16)


def spread(turn_ref, part):
    cos, sin = turn_ref[0, :, part], turn_ref[1, :, part]
    cos = jnp.concatenate([cos] * 4, axis=0).T
    sin = jnp.concatenate([-sin, sin] * 2, axis=0).T
    return jnp.concatenate([cos, cos], axis=1), jnp.concatenate([sin, sin], axis=1)


def query_kernel(hidden_ref, gain_ref, weight_ref, turn_ref, normed_ref, query_ref):
    rows = hidden_ref.shape[0]
    gain = gain_ref[...]

    def step(i, carry):
        part = pl.ds(pl.multiple_of(i * 64, 64), 64)
        normed_ref[part, :] = normed_rows(hidden_ref[part, :], gain)
        return carry

    lax.fori_loop(0, rows // 64, step, 0)
    query = jnp.dot(normed_ref[...], weight_ref[...], preferred_element_type=F32)
    cos, sin = spread(turn_ref, slice(0, rows))
    query = rotated(query, cos, sin).astype(BF16) * 0.125
    query_ref[...] = permuted(to_residue(rows), query)


def copies_kernel(key_ref, value_ref, out_ref):
    both = jnp.concatenate([key_ref[...], value_ref[...]], axis=1)
    for n in range(out_ref.shape[0]):
        out_ref[n] = both


def assembled(place_ref, mine_ref, below_ref, above_ref, weight_ref, columns):
    low = place_ref[1]
    for k in range(4):
        weight_ref[pl.ds(pl.multiple_of((2 * k + low) * 256, 256), 256), :] = mine_ref[k, :, columns]
    for k in range(2):
        weight_ref[pl.ds(pl.multiple_of((2 * k + 1 - low) * 256, 256), 256), :] = below_ref[k]
        weight_ref[pl.ds(pl.multiple_of((2 * k + 5 - low) * 256, 256), 256), :] = above_ref[k]


def key_kernel(place_ref, normed_ref, mine_ref, below_ref, above_ref, turn_ref, key_ref, weight_ref):
    rows, width = key_ref.shape
    assembled(place_ref, mine_ref, below_ref, above_ref, weight_ref, slice(0, width))
    key = jnp.dot(normed_ref[...], weight_ref[...], preferred_element_type=F32)
    key = rotated(key, *spread(turn_ref, slice(0, rows))).astype(BF16)
    key_ref[...] = permuted(to_residue(rows), key)


def value_kernel(place_ref, normed_ref, mine_ref, below_ref, above_ref, value_ref, weight_ref):
    rows, width = value_ref.shape
    assembled(place_ref, mine_ref, below_ref, above_ref, weight_ref, slice(width, 2 * width))
    value = jnp.dot(normed_ref[...], weight_ref[...], preferred_element_type=F32).astype(BF16)
    value_ref[...] = permuted(to_residue(rows), value)


def stack_heads(q):
    lane = lax.broadcasted_iota(jnp.int32, q.shape, 1) >> 6
    return jnp.concatenate([jnp.where(lane == h, q, jnp.zeros_like(q)) for h in range(q.shape[1] // HEAD_DIM)], axis=0)


def own_heads(stacked):
    width = stacked.shape[1]
    heads = width // HEAD_DIM
    rows = stacked.shape[0] // heads
    lane = lax.broadcasted_iota(jnp.int32, (rows, width), 1) >> 6
    out = stacked[:rows]
    for h in range(1, heads):
        out = jnp.where(lane == h, stacked[h * rows : (h + 1) * rows], out)
    return out


def far_bias(block, back):
    qi = lax.broadcasted_iota(jnp.int32, (128, 128), 0)
    ki = lax.broadcasted_iota(jnp.int32, (128, 128), 1)
    ok = ((qi >> 5) == (ki >> 5)) & (block >= back)
    if back == 4:
        ok = ok & ((ki & 31) >= (qi & 31))
    return jnp.where(ok, 0.0, LOW).astype(F32)


def times_seen(o):
    count = (o <= SPAN).astype(F32)
    count = count + (((o & 3) == 0) & (o <= 4 * SPAN)).astype(F32)
    return count + ((o & 15) == 0).astype(F32)


def query_places(cls):
    i = lax.broadcasted_iota(jnp.int32, (128, 1), 0)
    return (i & 31) * 16 + (i >> 5) * 4 + cls


def own_kernel(q_ref, k_ref, v_ref, max_ref, sum_ref, acc_ref, s_ref, p_ref, bias_ref, count_ref, stat_ref):
    keys, width = k_ref.shape
    heads = width // HEAD_DIM
    o = query_places(pl.program_id(0)) - natural(lax.broadcasted_iota(jnp.int32, (1, keys), 1))
    count = jnp.where(o >= 0, times_seen(o), 0.0)
    count_ref[...] = count
    bias_ref[...] = jnp.where(count > 0, 0.0, LOW).astype(F32)
    s_ref[...] = lax.dot_general(stack_heads(q_ref[...]), k_ref[...], NT, preferred_element_type=F32)
    step = 32
    for r in range(0, heads * 128, step):
        mask = slice(r % 128, r % 128 + step)
        s = s_ref[r : r + step, :] + bias_ref[mask, :]
        m = jnp.max(s, axis=1, keepdims=True)
        p = jnp.exp(s - m) * count_ref[mask, :]
        stat_ref[0, r : r + step, :] = jnp.broadcast_to(m, (step, width))
        stat_ref[1, r : r + step, :] = jnp.broadcast_to(jnp.sum(p, axis=1, keepdims=True), (step, width))
        p_ref[r : r + step, :] = p.astype(BF16)
    pv = jnp.dot(p_ref[...], v_ref[...], preferred_element_type=F32)
    max_ref[...] = own_heads(stat_ref[0])
    sum_ref[...] = own_heads(stat_ref[1])
    acc_ref[...] = own_heads(pv)


def merged(q, key, value, bias, count, max_ref, sum_ref, acc_ref, s_ref, p_ref, stat_ref):
    width = max_ref.shape[1]
    s_ref[...] = lax.dot_general(stack_heads(q), key, NT, preferred_element_type=F32)
    for h in range(width // HEAD_DIM):
        part = slice(h * 128, (h + 1) * 128)
        s = s_ref[part, :] + bias
        m = jnp.maximum(jnp.max(s, axis=1, keepdims=True), max_ref[:, h * HEAD_DIM : h * HEAD_DIM + 1])
        p = jnp.exp(s - m)
        if count is not None:
            p = p * count
        p_ref[part, :] = p.astype(BF16)
        stat_ref[0, part, :] = jnp.broadcast_to(m, (128, width))
        stat_ref[1, part, :] = jnp.broadcast_to(jnp.sum(p, axis=1, keepdims=True), (128, width))
    pv = jnp.dot(p_ref[...], value, preferred_element_type=F32)
    m = own_heads(stat_ref[0])
    alpha = jnp.exp(max_ref[...] - m)
    total = sum_ref[...] * alpha + own_heads(stat_ref[1])
    return m, total, acc_ref[...] * alpha + own_heads(pv)


def before_kernel(place_ref, q_ref, max_ref, sum_ref, acc_ref, k_ref, v_ref, new_max, new_sum, new_acc, s_ref, p_ref, stat_ref, tail_ref):
    cls = pl.program_id(0)
    keys = k_ref.shape[0]
    mine = pl.ds(pl.multiple_of(cls * 128, 128), 128)

    @pl.when(cls == 0)
    def _():
        j = lax.broadcasted_iota(jnp.int32, (128, keys), 0)
        i = lax.broadcasted_iota(jnp.int32, (128, keys), 1)
        pick = (i == (j >> 3) * 32 + 24 + (j & 7)).astype(BF16)
        tail_ref[0] = permuted(pick, k_ref[...])
        tail_ref[1] = permuted(pick, v_ref[...])

    seen = place_ref[0] >= 1
    qn = query_places(cls)
    k = lax.broadcasted_iota(jnp.int32, (1, 128), 1)
    same = times_seen(qn - ((k & 31) * 16 + (k >> 5) * 4 + cls) + keys)
    last = qn - ((24 + (k & 7)) * 16 + ((k >> 3) & 3) * 4 + (k >> 5)) + keys
    last = ((last <= SPAN) & ((k >> 5) != cls)).astype(F32)
    count = jnp.where(seen, jnp.concatenate([same, last], axis=1), 0.0)
    bias = jnp.where(count > 0, 0.0, LOW).astype(F32)
    key = jnp.concatenate([k_ref[mine, :], tail_ref[0]], axis=0)
    value = jnp.concatenate([v_ref[mine, :], tail_ref[1]], axis=0)
    state = merged(q_ref[...], key, value, bias, count, max_ref, sum_ref, acc_ref, s_ref, p_ref, stat_ref)
    for ref, part in zip((new_max, new_sum, new_acc), state):
        ref[...] = part


def far_kernel(backs, last, place_ref, q_ref, max_ref, sum_ref, acc_ref, *refs):
    count = len(backs)
    sources, outs = refs[: 2 * count], refs[2 * count :]
    s_ref, p_ref, stat_ref = outs[-3:]
    bias = jnp.concatenate([far_bias(place_ref[0], back) for back in backs], axis=1)
    key = jnp.concatenate([ref[...] for ref in sources[0::2]], axis=0)
    value = jnp.concatenate([ref[...] for ref in sources[1::2]], axis=0)
    m, total, acc = merged(q_ref[...], key, value, bias, None, max_ref, sum_ref, acc_ref, s_ref, p_ref, stat_ref)
    if last:
        cls = pl.program_id(0)
        out_ref, log_ref, att_ref = outs[:3]
        att_ref[pl.ds(pl.multiple_of(cls * 128, 128), 128), :] = (acc / total).astype(BF16)
        lw = m + jnp.log(total)
        lane = lax.broadcasted_iota(jnp.int32, log_ref.shape, 1)
        compact = jnp.zeros(log_ref.shape, F32)
        for h in range(lw.shape[1] // HEAD_DIM):
            compact = jnp.where(lane == h, lw[:, h * HEAD_DIM : h * HEAD_DIM + 1], compact)
        log_ref[...] = compact

        @pl.when(cls == pl.num_programs(0) - 1)
        def _():
            out_ref[...] = permuted(to_natural(att_ref.shape[0]), att_ref[...])
    else:
        for ref, part in zip(outs[:3], (m, total, acc)):
            ref[...] = part


def log_kernel(lw_ref, log_ref):
    rows, lanes = lw_ref.shape
    perm = to_natural(rows)
    rest = lw_ref[...]
    ordered = jnp.zeros((rows, lanes), F32)
    for _ in range(3):
        piece = rest.astype(BF16)
        rest = rest - piece.astype(F32)
        ordered = ordered + jnp.dot(perm, piece, preferred_element_type=F32)
    log_ref[...] = ordered.T[: log_ref.shape[0]]


def out_kernel(place_ref, att_ref, *refs):
    weights, (gain_ref, out_ref, sum_ref) = refs[:8], refs[8:]
    x, core = place_ref[2], place_ref[3]
    n = pl.program_id(0)
    columns = weights[0].shape[1]
    total = None
    for half, c in enumerate((core, 1 - core)):
        for k, hop in enumerate(HOPS):
            group = lax.rem(x + hop, 4) * 2 + c
            part = jnp.dot(att_ref[group], weights[half * 4 + k][...], preferred_element_type=F32)
            part = part.astype(BF16).astype(F32)
            total = part if total is None else total + part
    sum_ref[:, pl.ds(pl.multiple_of(n * columns, columns), columns)] = total

    @pl.when(n == pl.num_programs(0) - 1)
    def _():
        summed = sum_ref[...]
        scale = lax.rsqrt(jnp.mean(summed * summed, axis=1, keepdims=True) + EPS)
        out_ref[...] = (summed * scale * gain_ref[...]).astype(BF16)


SMEM = pl.BlockSpec(memory_space=pltpu.SMEM)
VMEM = pl.BlockSpec(memory_space=pltpu.VMEM)


def kernel_call(body, outs, args, flops, limit, scratch=(), **more):
    if "grid_spec" not in more:
        more["scratch_shapes"] = [pltpu.VMEM(s, t) for s, t in scratch]
    if "in_specs" not in more and "grid_spec" not in more:
        more["in_specs"] = [SMEM if a.dtype == jnp.int32 else VMEM for a in args]
        more["out_specs"] = tuple(VMEM for _ in outs)
    data = sum(a.size * a.dtype.itemsize for a in args)
    return pl.pallas_call(
        body,
        out_shape=tuple(jax.ShapeDtypeStruct(s, t) for s, t in outs),
        compiler_params=pltpu.CompilerParams(vmem_limit_bytes=limit * 1024 * 1024),
        cost_estimate=pl.CostEstimate(flops=flops, bytes_accessed=data, transcendentals=0),
        **more,
    )(*args)


def layer(hidden_in, pre_gain, query_proj, key_proj, value_proj, out_proj, post_gain):
    rows, depth = hidden_in.shape
    width = query_proj.shape[1]
    heads = width // HEAD_DIM
    piece = rows // 8
    sp, x, core = lax.axis_index(SP), lax.axis_index("x"), lax.axis_index("c")
    place = jnp.stack([sp, lax.axis_index("zl"), x, core]).astype(jnp.int32)
    gain = pre_gain[None]
    row = (rows, width)

    shard_spec = pl.BlockSpec(key_proj.shape, lambda n: (0, 0))
    (copies,) = kernel_call(
        copies_kernel,
        [((32, key_proj.shape[0], 2 * width), BF16)],
        (key_proj, value_proj),
        1000,
        56,
        grid=(4,),
        in_specs=[shard_spec] * 2,
        out_specs=(pl.BlockSpec((8, key_proj.shape[0], 2 * width), lambda n: (n, 0, 0)),),
    )
    mine = lax.all_to_all(copies, ("zh", "y"), split_axis=0, concat_axis=0, tiled=True)
    mine = mine.reshape(4, 256, 2 * width)
    slabs = []
    for columns in (slice(0, width), slice(width, 2 * width)):
        below = lax.ppermute(mine[:2, :, columns], Z, ring(8, 1))
        above = lax.ppermute(mine[2:, :, columns], Z, ring(8, -1))
        slabs.append((mine, below, above))

    groups = [out_proj]
    for steps in (1, -1, 2):
        groups.append(lax.ppermute(out_proj, "x", ring(4, steps)))
    for n in range(4):
        groups.append(lax.ppermute(groups[n], "c", ring(2, 1)))

    quarter = HEAD_DIM // 2
    frequency = ROPE_BASE ** (-(jnp.arange(quarter, dtype=F32) * 2.0 / HEAD_DIM))
    positions = (sp * rows + jnp.arange(rows, dtype=jnp.int32)).astype(F32)
    angles = positions[None, :] * frequency[:, None]
    turns = jnp.stack([jnp.cos(angles), jnp.sin(angles)])

    normed, query = kernel_call(
        query_kernel, [((rows, depth), BF16), (row, BF16)], (hidden_in, gain, query_proj, turns), 2 * rows * depth * width, 12
    )
    weight = [((depth, width), BF16)]
    (key,) = kernel_call(key_kernel, [(row, BF16)], (place, normed, *slabs[0], turns), 2 * rows * depth * width, 14, weight)
    (value,) = kernel_call(value_kernel, [(row, BF16)], (place, normed, *slabs[1]), 2 * rows * depth * width, 14, weight)
    forward = [(i, i + 1) for i in range(63)]
    keys, values = [key], [value]
    for _ in range(1, 5):
        keys.append(lax.ppermute(keys[-1], SP, forward))
        values.append(lax.ppermute(values[-1], SP, forward))
    whole = pl.BlockSpec(row, lambda c: (0, 0))
    part = pl.BlockSpec((128, width), lambda c: (c, 0))
    pair = ((512, 256), F32), ((512, 256), BF16), ((2, 512, width), F32)
    state = kernel_call(
        own_kernel,
        [(row, F32)] * 3,
        (query, keys[0], values[0]),
        8 * rows * rows * width,
        10,
        [((512, 512), F32), ((512, 512), BF16), ((128, 512), F32), ((128, 512), F32), ((2, 512, width), F32)],
        grid=(rows // 128,),
        in_specs=[part, whole, whole],
        out_specs=(part,) * 3,
    )
    state = kernel_call(
        before_kernel,
        [(row, F32)] * 3,
        (place, query, *state, keys[1], values[1]),
        4 * rows * rows * width,
        10,
        [*pair, ((2, 128, width), BF16)],
        grid=(rows // 128,),
        in_specs=[SMEM] + [part] * 4 + [whole, whole],
        out_specs=(part,) * 3,
    )
    for back in (2, 3, 4):
        last = back == 4
        state = kernel_call(
            functools.partial(far_kernel, (back,), last),
            [(row, BF16), ((rows, 128), F32)] if last else [(row, F32)] * 3,
            (place, query, *state, keys[back], values[back]),
            4 * rows * 512 * width,
            16,
            ([(row, BF16)] if last else []) + [((512, 128), t) for t in (F32, BF16)] + [((2, 512, width), F32)],
            grid=(rows // 128,),
            in_specs=[SMEM] + [part] * 6,
            out_specs=(whole, pl.BlockSpec((128, 128), lambda c: (c, 0))) if last else (part,) * 3,
        )
    attended, logs = state

    arrived = lax.all_to_all(attended.reshape(8, piece, width), TP, split_axis=0, concat_axis=0, tiled=True)
    (log_weight,) = kernel_call(log_kernel, [((heads, rows), F32)], (logs,), 6 * rows * rows * width, 8)
    columns = depth // 4
    (layer_out,) = kernel_call(
        out_kernel,
        [((piece, depth), BF16)],
        (place, arrived, *groups, post_gain[None]),
        2 * piece * depth * depth,
        12,
        [((piece, depth), F32)],
        grid=(4,),
        in_specs=[SMEM, pl.BlockSpec((8, piece, width), lambda n: (0, 0, 0))]
        + [pl.BlockSpec((width, columns), lambda n: (0, n))] * 8
        + [pl.BlockSpec((1, depth), lambda n: (0, 0))],
        out_specs=(pl.BlockSpec((piece, depth), lambda n: (0, 0)),),
    )
    return layer_out, log_weight


def solution(mesh):
    fine = Mesh(np.asarray(mesh.devices).reshape(4, 2, 8, 4, 2), ("zh", "zl", "y", "x", "c"))
    placed = (P(SP, None), P(), P(None, TP), P(SP, TP), P(SP, TP), P(TP, None), P())
    return jax.shard_map(
        layer,
        mesh=fine,
        in_specs=placed,
        out_specs=(P(SP + TP, None), P(TP, SP)),
        check_vma=False,
    )
```

```python
import functools

import jax
import jax.numpy as jnp
import numpy as np
from jax import lax
from jax.experimental import pallas as pl
from jax.experimental.pallas import tpu as pltpu
from jax.sharding import Mesh
from jax.sharding import PartitionSpec as P

HEAD_DIM = 64
SPAN = 128
EPS = 1e-06
ROPE_BASE = 10000.0
LOW = -1e30
SP = ("zh", "zl", "y")
Z = ("zh", "zl")
TP = ("x", "c")
F32 = jnp.float32
BF16 = jnp.bfloat16
NT = (((1,), (1,)), ((), ()))
HOPS = (0, 3, 1, 2)


def ring(count, steps):
    return [(i, (i + steps) % count) for i in range(count)]


def natural(i):
    return (i & 31) * 16 + ((i >> 5) & 3) * 4 + (i >> 7)


def to_residue(rows, columns=None):
    i = lax.broadcasted_iota(jnp.int32, (rows, rows), 0)
    if columns is None:
        columns = lax.broadcasted_iota(jnp.int32, (rows, rows), 1)
    return (natural(i) == columns).astype(BF16)


def to_natural(rows):
    i = lax.broadcasted_iota(jnp.int32, (rows, rows), 1)
    n = lax.broadcasted_iota(jnp.int32, (rows, rows), 0)
    return (natural(i) == n).astype(BF16)


def rotated(x, cos, sin):
    width = x.shape[1]
    lane = lax.broadcasted_iota(jnp.int32, x.shape, 1)
    other = jnp.where((lane & 63) < 32, pltpu.roll(x, width - 32, 1), pltpu.roll(x, 32, 1))
    return x * cos + other * sin


def permuted(perm, x):
    return jnp.dot(perm, x, preferred_element_type=F32).astype(BF16)


def normed_rows(x, gain):
    x = x.astype(F32)
    scale = lax.rsqrt(jnp.mean(x * x, axis=1, keepdims=True) + EPS)
    return (x * scale * gain).astype(BF16)


def spread(turn_ref, part):
    cos, sin = turn_ref[0, :, part], turn_ref[1, :, part]
    cos = jnp.concatenate([cos] * 4, axis=0).T
    sin = jnp.concatenate([-sin, sin] * 2, axis=0).T
    return jnp.concatenate([cos, cos], axis=1), jnp.concatenate([sin, sin], axis=1)


def query_kernel(hidden_ref, gain_ref, weight_ref, turn_ref, normed_ref, query_ref):
    rows = hidden_ref.shape[0]
    gain = gain_ref[...]

    def step(i, carry):
        part = pl.ds(pl.multiple_of(i * 64, 64), 64)
        normed_ref[part, :] = normed_rows(hidden_ref[part, :], gain)
        return carry

    lax.fori_loop(0, rows // 64, step, 0)
    query = jnp.dot(normed_ref[...], weight_ref[...], preferred_element_type=F32)
    cos, sin = spread(turn_ref, slice(0, rows))
    query = rotated(query, cos, sin).astype(BF16) * 0.125
    query_ref[...] = permuted(to_residue(rows), query)


def copies_kernel(key_ref, value_ref, out_ref):
    both = jnp.concatenate([key_ref[...], value_ref[...]], axis=1)
    for n in range(out_ref.shape[0]):
        out_ref[n] = both


def assembled(place_ref, mine_ref, below_ref, above_ref, weight_ref, columns):
    low = place_ref[1]
    for k in range(4):
        weight_ref[pl.ds(pl.multiple_of((2 * k + low) * 256, 256), 256), :] = mine_ref[k, :, columns]
    for k in range(2):
        weight_ref[pl.ds(pl.multiple_of((2 * k + 1 - low) * 256, 256), 256), :] = below_ref[k]
        weight_ref[pl.ds(pl.multiple_of((2 * k + 5 - low) * 256, 256), 256), :] = above_ref[k]


def key_kernel(place_ref, normed_ref, mine_ref, below_ref, above_ref, turn_ref, key_ref, weight_ref):
    rows, width = key_ref.shape
    assembled(place_ref, mine_ref, below_ref, above_ref, weight_ref, slice(0, width))
    key = jnp.dot(normed_ref[...], weight_ref[...], preferred_element_type=F32)
    key = rotated(key, *spread(turn_ref, slice(0, rows))).astype(BF16)
    key_ref[...] = permuted(to_residue(rows), key)


def value_kernel(place_ref, normed_ref, mine_ref, below_ref, above_ref, value_ref, weight_ref):
    rows, width = value_ref.shape
    assembled(place_ref, mine_ref, below_ref, above_ref, weight_ref, slice(width, 2 * width))
    value = jnp.dot(normed_ref[...], weight_ref[...], preferred_element_type=F32).astype(BF16)
    value_ref[...] = permuted(to_residue(rows), value)


def stack_heads(q):
    lane = lax.broadcasted_iota(jnp.int32, q.shape, 1) >> 6
    return jnp.concatenate([jnp.where(lane == h, q, jnp.zeros_like(q)) for h in range(q.shape[1] // HEAD_DIM)], axis=0)


def own_heads(stacked):
    width = stacked.shape[1]
    heads = width // HEAD_DIM
    rows = stacked.shape[0] // heads
    lane = lax.broadcasted_iota(jnp.int32, (rows, width), 1) >> 6
    out = stacked[:rows]
    for h in range(1, heads):
        out = jnp.where(lane == h, stacked[h * rows : (h + 1) * rows], out)
    return out


def far_bias(block, back):
    qi = lax.broadcasted_iota(jnp.int32, (128, 128), 0)
    ki = lax.broadcasted_iota(jnp.int32, (128, 128), 1)
    ok = ((qi >> 5) == (ki >> 5)) & (block >= back)
    if back == 4:
        ok = ok & ((ki & 31) >= (qi & 31))
    return jnp.where(ok, 0.0, LOW).astype(F32)


def times_seen(o):
    count = (o <= SPAN).astype(F32)
    count = count + (((o & 3) == 0) & (o <= 4 * SPAN)).astype(F32)
    return count + ((o & 15) == 0).astype(F32)


def query_places(cls):
    i = lax.broadcasted_iota(jnp.int32, (128, 1), 0)
    return (i & 31) * 16 + (i >> 5) * 4 + cls


def own_kernel(q_ref, k_ref, v_ref, max_ref, sum_ref, acc_ref, s_ref, p_ref, bias_ref, count_ref):
    keys, width = k_ref.shape
    heads = width // HEAD_DIM
    o = query_places(pl.program_id(0)) - natural(lax.broadcasted_iota(jnp.int32, (1, keys), 1))
    count = jnp.where(o >= 0, times_seen(o), 0.0)
    count_ref[...] = count
    bias_ref[...] = jnp.where(count > 0, 0.0, LOW).astype(F32)
    s_ref[...] = lax.dot_general(stack_heads(q_ref[...]), k_ref[...], NT, preferred_element_type=F32)
    step = 32
    for r in range(0, heads * 128, step):
        mask = slice(r % 128, r % 128 + step)
        s = s_ref[r : r + step, :] + bias_ref[mask, :]
        m = jnp.max(s, axis=1, keepdims=True)
        p = jnp.exp(s - m) * count_ref[mask, :]
        max_ref[r : r + step, :] = jnp.broadcast_to(m, (step, 128))
        sum_ref[r : r + step, :] = jnp.broadcast_to(jnp.sum(p, axis=1, keepdims=True), (step, 128))
        p_ref[r : r + step, :] = p.astype(BF16)
    acc_ref[...] = own_heads(jnp.dot(p_ref[...], v_ref[...], preferred_element_type=F32))


def tiles(parts):
    low = lax.broadcasted_iota(jnp.int32, parts[0].shape, 1) < HEAD_DIM
    return jnp.concatenate([jnp.where(low, a, b) for a, b in zip(parts[0::2], parts[1::2])], axis=1)


def merged(q, key, value, bias, count, max_ref, sum_ref, acc_ref, s_ref, p_ref):
    heads = q.shape[1] // HEAD_DIM
    wide = key.shape[0] // 128
    s_ref[...] = lax.dot_general(stack_heads(q), key, NT, preferred_element_type=F32)
    tops, sums, scales = [], [], []
    for h in range(heads):
        part = slice(h * 128, (h + 1) * 128)
        s = s_ref[part, :] + bias
        old = max_ref[part, :]
        m = jnp.maximum(jnp.max(s, axis=1, keepdims=True), old)
        p = jnp.exp(s - jnp.concatenate([m] * wide, axis=1))
        if count is not None:
            p = p * count
        p_ref[part, :] = p.astype(BF16)
        scale = jnp.exp(old - m)
        tops.append(m)
        sums.append(sum_ref[part, :] * scale + jnp.sum(p, axis=1, keepdims=True))
        scales.append(scale)
    pv = own_heads(jnp.dot(p_ref[...], value, preferred_element_type=F32))
    return tops, sums, acc_ref[...] * tiles(scales) + pv


def store_state(state, max_ref, sum_ref, acc_ref):
    tops, sums, acc_ref[...] = state
    for h in range(len(tops)):
        max_ref[h * 128 : (h + 1) * 128, :] = tops[h]
        sum_ref[h * 128 : (h + 1) * 128, :] = sums[h]


def before_kernel(place_ref, q_ref, max_ref, sum_ref, acc_ref, k_ref, v_ref, new_max, new_sum, new_acc, s_ref, p_ref, tail_ref):
    cls = pl.program_id(0)
    keys = k_ref.shape[0]
    mine = pl.ds(pl.multiple_of(cls * 128, 128), 128)

    @pl.when(cls == 0)
    def _():
        j = lax.broadcasted_iota(jnp.int32, (128, keys), 0)
        i = lax.broadcasted_iota(jnp.int32, (128, keys), 1)
        pick = (i == (j >> 3) * 32 + 24 + (j & 7)).astype(BF16)
        tail_ref[0] = permuted(pick, k_ref[...])
        tail_ref[1] = permuted(pick, v_ref[...])

    seen = place_ref[0] >= 1
    qn = query_places(cls)
    k = lax.broadcasted_iota(jnp.int32, (1, 128), 1)
    same = times_seen(qn - ((k & 31) * 16 + (k >> 5) * 4 + cls) + keys)
    last = qn - ((24 + (k & 7)) * 16 + ((k >> 3) & 3) * 4 + (k >> 5)) + keys
    last = ((last <= SPAN) & ((k >> 5) != cls)).astype(F32)
    count = jnp.where(seen, jnp.concatenate([same, last], axis=1), 0.0)
    bias = jnp.where(count > 0, 0.0, LOW).astype(F32)
    key = jnp.concatenate([k_ref[mine, :], tail_ref[0]], axis=0)
    value = jnp.concatenate([v_ref[mine, :], tail_ref[1]], axis=0)
    store_state(merged(q_ref[...], key, value, bias, count, max_ref, sum_ref, acc_ref, s_ref, p_ref), new_max, new_sum, new_acc)


def far_kernel(backs, last, place_ref, q_ref, max_ref, sum_ref, acc_ref, *refs):
    count = len(backs)
    sources, outs = refs[: 2 * count], refs[2 * count :]
    s_ref, p_ref = outs[-2:]
    bias = jnp.concatenate([far_bias(place_ref[0], back) for back in backs], axis=1)
    key = jnp.concatenate([ref[...] for ref in sources[0::2]], axis=0)
    value = jnp.concatenate([ref[...] for ref in sources[1::2]], axis=0)
    state = merged(q_ref[...], key, value, bias, None, max_ref, sum_ref, acc_ref, s_ref, p_ref)
    if not last:
        store_state(state, *outs[:3])
        return
    tops, sums, acc = state
    cls = pl.program_id(0)
    out_ref, log_ref, att_ref = outs[:3]
    att_ref[pl.ds(pl.multiple_of(cls * 128, 128), 128), :] = (acc / tiles(sums)).astype(BF16)
    lane = lax.broadcasted_iota(jnp.int32, log_ref.shape, 1)
    logs = jnp.zeros(log_ref.shape, F32)
    for h in range(len(tops)):
        logs = jnp.where(lane == h, tops[h] + jnp.log(sums[h]), logs)
    log_ref[...] = logs

    @pl.when(cls == pl.num_programs(0) - 1)
    def _():
        out_ref[...] = permuted(to_natural(att_ref.shape[0]), att_ref[...])


def log_kernel(lw_ref, log_ref):
    rows, lanes = lw_ref.shape
    perm = to_natural(rows)
    rest = lw_ref[...]
    ordered = jnp.zeros((rows, lanes), F32)
    for _ in range(3):
        piece = rest.astype(BF16)
        rest = rest - piece.astype(F32)
        ordered = ordered + jnp.dot(perm, piece, preferred_element_type=F32)
    log_ref[...] = ordered.T[: log_ref.shape[0]]


def out_kernel(place_ref, att_ref, *refs):
    weights, (gain_ref, out_ref, sum_ref) = refs[:8], refs[8:]
    x, core = place_ref[2], place_ref[3]
    n = pl.program_id(0)
    columns = weights[0].shape[1]
    total = None
    for half, c in enumerate((core, 1 - core)):
        for k, hop in enumerate(HOPS):
            group = lax.rem(x + hop, 4) * 2 + c
            part = jnp.dot(att_ref[group], weights[half * 4 + k][...], preferred_element_type=F32)
            part = part.astype(BF16).astype(F32)
            total = part if total is None else total + part
    sum_ref[:, pl.ds(pl.multiple_of(n * columns, columns), columns)] = total

    @pl.when(n == pl.num_programs(0) - 1)
    def _():
        summed = sum_ref[...]
        scale = lax.rsqrt(jnp.mean(summed * summed, axis=1, keepdims=True) + EPS)
        out_ref[...] = (summed * scale * gain_ref[...]).astype(BF16)


SMEM = pl.BlockSpec(memory_space=pltpu.SMEM)
VMEM = pl.BlockSpec(memory_space=pltpu.VMEM)


def kernel_call(body, outs, args, flops, limit, scratch=(), **more):
    if "grid_spec" not in more:
        more["scratch_shapes"] = [pltpu.VMEM(s, t) for s, t in scratch]
    if "in_specs" not in more and "grid_spec" not in more:
        more["in_specs"] = [SMEM if a.dtype == jnp.int32 else VMEM for a in args]
        more["out_specs"] = tuple(VMEM for _ in outs)
    data = sum(a.size * a.dtype.itemsize for a in args)
    return pl.pallas_call(
        body,
        out_shape=tuple(jax.ShapeDtypeStruct(s, t) for s, t in outs),
        compiler_params=pltpu.CompilerParams(vmem_limit_bytes=limit * 1024 * 1024),
        cost_estimate=pl.CostEstimate(flops=flops, bytes_accessed=data, transcendentals=0),
        **more,
    )(*args)


def layer(hidden_in, pre_gain, query_proj, key_proj, value_proj, out_proj, post_gain):
    rows, depth = hidden_in.shape
    width = query_proj.shape[1]
    heads = width // HEAD_DIM
    piece = rows // 8
    sp, x, core = lax.axis_index(SP), lax.axis_index("x"), lax.axis_index("c")
    place = jnp.stack([sp, lax.axis_index("zl"), x, core]).astype(jnp.int32)
    gain = pre_gain[None]
    row = (rows, width)

    shard_spec = pl.BlockSpec(key_proj.shape, lambda n: (0, 0))
    (copies,) = kernel_call(
        copies_kernel,
        [((32, key_proj.shape[0], 2 * width), BF16)],
        (key_proj, value_proj),
        1000,
        56,
        grid=(4,),
        in_specs=[shard_spec] * 2,
        out_specs=(pl.BlockSpec((8, key_proj.shape[0], 2 * width), lambda n: (n, 0, 0)),),
    )
    mine = lax.all_to_all(copies, ("zh", "y"), split_axis=0, concat_axis=0, tiled=True)
    mine = mine.reshape(4, 256, 2 * width)
    slabs = []
    for columns in (slice(0, width), slice(width, 2 * width)):
        below = lax.ppermute(mine[:2, :, columns], Z, ring(8, 1))
        above = lax.ppermute(mine[2:, :, columns], Z, ring(8, -1))
        slabs.append((mine, below, above))

    groups = [out_proj]
    for steps in (1, -1, 2):
        groups.append(lax.ppermute(out_proj, "x", ring(4, steps)))
    for n in range(4):
        groups.append(lax.ppermute(groups[n], "c", ring(2, 1)))

    quarter = HEAD_DIM // 2
    frequency = ROPE_BASE ** (-(jnp.arange(quarter, dtype=F32) * 2.0 / HEAD_DIM))
    positions = (sp * rows + jnp.arange(rows, dtype=jnp.int32)).astype(F32)
    angles = positions[None, :] * frequency[:, None]
    turns = jnp.stack([jnp.cos(angles), jnp.sin(angles)])

    normed, query = kernel_call(
        query_kernel, [((rows, depth), BF16), (row, BF16)], (hidden_in, gain, query_proj, turns), 2 * rows * depth * width, 12
    )
    weight = [((depth, width), BF16)]
    (key,) = kernel_call(key_kernel, [(row, BF16)], (place, normed, *slabs[0], turns), 2 * rows * depth * width, 14, weight)
    (value,) = kernel_call(value_kernel, [(row, BF16)], (place, normed, *slabs[1]), 2 * rows * depth * width, 14, weight)
    forward = [(i, i + 1) for i in range(63)]
    keys, values = [key], [value]
    for _ in range(1, 5):
        keys.append(lax.ppermute(keys[-1], SP, forward))
        values.append(lax.ppermute(values[-1], SP, forward))
    whole = pl.BlockSpec(row, lambda c: (0, 0))
    part = pl.BlockSpec((128, width), lambda c: (c, 0))
    stat = pl.BlockSpec((512, 128), lambda c: (c, 0))
    stats = (4 * rows, 128)
    outs = [(stats, F32), (stats, F32), (row, F32)]
    pair = ((512, 256), F32), ((512, 256), BF16)
    state = kernel_call(
        own_kernel,
        outs,
        (query, keys[0], values[0]),
        8 * rows * rows * width,
        12,
        [((512, 512), F32), ((512, 512), BF16), ((128, 512), F32), ((128, 512), F32)],
        grid=(rows // 128,),
        in_specs=[part, whole, whole],
        out_specs=(stat, stat, part),
    )
    state = kernel_call(
        before_kernel,
        outs,
        (place, query, *state, keys[1], values[1]),
        4 * rows * rows * width,
        12,
        [*pair, ((2, 128, width), BF16)],
        grid=(rows // 128,),
        in_specs=[SMEM, part, stat, stat, part, whole, whole],
        out_specs=(stat, stat, part),
    )
    for back in (2, 3, 4):
        last = back == 4
        state = kernel_call(
            functools.partial(far_kernel, (back,), last),
            [(row, BF16), ((rows, 128), F32)] if last else outs,
            (place, query, *state, keys[back], values[back]),
            4 * rows * 512 * width,
            16,
            ([(row, BF16)] if last else []) + [((512, 128), t) for t in (F32, BF16)],
            grid=(rows // 128,),
            in_specs=[SMEM, part, stat, stat, part, part, part],
            out_specs=(whole, pl.BlockSpec((128, 128), lambda c: (c, 0))) if last else (stat, stat, part),
        )
    attended, logs = state

    arrived = lax.all_to_all(attended.reshape(8, piece, width), TP, split_axis=0, concat_axis=0, tiled=True)
    (log_weight,) = kernel_call(log_kernel, [((heads, rows), F32)], (logs,), 6 * rows * rows * width, 8)
    columns = depth // 4
    (layer_out,) = kernel_call(
        out_kernel,
        [((piece, depth), BF16)],
        (place, arrived, *groups, post_gain[None]),
        2 * piece * depth * depth,
        12,
        [((piece, depth), F32)],
        grid=(4,),
        in_specs=[SMEM, pl.BlockSpec((8, piece, width), lambda n: (0, 0, 0))]
        + [pl.BlockSpec((width, columns), lambda n: (0, n))] * 8
        + [pl.BlockSpec((1, depth), lambda n: (0, 0))],
        out_specs=(pl.BlockSpec((piece, depth), lambda n: (0, 0)),),
    )
    return layer_out, log_weight


def solution(mesh):
    fine = Mesh(np.asarray(mesh.devices).reshape(4, 2, 8, 4, 2), ("zh", "zl", "y", "x", "c"))
    placed = (P(SP, None), P(), P(None, TP), P(SP, TP), P(SP, TP), P(TP, None), P())
    return jax.shard_map(
        layer,
        mesh=fine,
        in_specs=placed,
        out_specs=(P(SP + TP, None), P(TP, SP)),
        check_vma=False,
    )
```

```python
import functools

import jax
import jax.numpy as jnp
import numpy as np
from jax import lax
from jax.experimental import pallas as pl
from jax.experimental.pallas import tpu as pltpu
from jax.sharding import Mesh
from jax.sharding import PartitionSpec as P

HEAD_DIM = 64
SPAN = 128
EPS = 1e-06
ROPE_BASE = 10000.0
LOW = -1e30
SP = ("zh", "zl", "y")
Z = ("zh", "zl")
TP = ("x", "c")
F32 = jnp.float32
BF16 = jnp.bfloat16
NT = (((1,), (1,)), ((), ()))
HOPS = (0, 3, 1, 2)


def ring(count, steps):
    return [(i, (i + steps) % count) for i in range(count)]


def natural(i):
    return (i & 31) * 16 + ((i >> 5) & 3) * 4 + (i >> 7)


def to_residue(rows, columns=None):
    i = lax.broadcasted_iota(jnp.int32, (rows, rows), 0)
    if columns is None:
        columns = lax.broadcasted_iota(jnp.int32, (rows, rows), 1)
    return (natural(i) == columns).astype(BF16)


def to_natural(rows):
    i = lax.broadcasted_iota(jnp.int32, (rows, rows), 1)
    n = lax.broadcasted_iota(jnp.int32, (rows, rows), 0)
    return (natural(i) == n).astype(BF16)


def rotated(x, cos, sin):
    width = x.shape[1]
    lane = lax.broadcasted_iota(jnp.int32, x.shape, 1)
    other = jnp.where((lane & 63) < 32, pltpu.roll(x, width - 32, 1), pltpu.roll(x, 32, 1))
    return x * cos + other * sin


def permuted(perm, x):
    return jnp.dot(perm, x, preferred_element_type=F32).astype(BF16)


def normed_rows(x, gain):
    x = x.astype(F32)
    scale = lax.rsqrt(jnp.mean(x * x, axis=1, keepdims=True) + EPS)
    return (x * scale * gain).astype(BF16)


def spread(turn_ref, part):
    cos, sin = turn_ref[0, :, part], turn_ref[1, :, part]
    cos = jnp.concatenate([cos] * 4, axis=0).T
    sin = jnp.concatenate([-sin, sin] * 2, axis=0).T
    return jnp.concatenate([cos, cos], axis=1), jnp.concatenate([sin, sin], axis=1)


def query_kernel(hidden_ref, gain_ref, weight_ref, turn_ref, normed_ref, query_ref):
    rows = hidden_ref.shape[0]
    gain = gain_ref[...]

    def step(i, carry):
        part = pl.ds(pl.multiple_of(i * 64, 64), 64)
        normed_ref[part, :] = normed_rows(hidden_ref[part, :], gain)
        return carry

    lax.fori_loop(0, rows // 64, step, 0)
    query = jnp.dot(normed_ref[...], weight_ref[...], preferred_element_type=F32)
    cos, sin = spread(turn_ref, slice(0, rows))
    query = rotated(query, cos, sin).astype(BF16) * 0.125
    query_ref[...] = permuted(to_residue(rows), query)


def copies_kernel(key_ref, value_ref, out_ref):
    both = jnp.concatenate([key_ref[...], value_ref[...]], axis=1)
    for n in range(out_ref.shape[0]):
        out_ref[n] = both


def assembled(place_ref, mine_ref, below_ref, above_ref, weight_ref, columns):
    low = place_ref[1]
    for k in range(4):
        weight_ref[pl.ds(pl.multiple_of((2 * k + low) * 256, 256), 256), :] = mine_ref[k, :, columns]
    for k in range(2):
        weight_ref[pl.ds(pl.multiple_of((2 * k + 1 - low) * 256, 256), 256), :] = below_ref[k]
        weight_ref[pl.ds(pl.multiple_of((2 * k + 5 - low) * 256, 256), 256), :] = above_ref[k]


def key_kernel(place_ref, normed_ref, mine_ref, below_ref, above_ref, turn_ref, key_ref, weight_ref):
    rows, width = key_ref.shape
    assembled(place_ref, mine_ref, below_ref, above_ref, weight_ref, slice(0, width))
    key = jnp.dot(normed_ref[...], weight_ref[...], preferred_element_type=F32)
    key = rotated(key, *spread(turn_ref, slice(0, rows))).astype(BF16)
    key_ref[...] = permuted(to_residue(rows), key)


def value_kernel(place_ref, normed_ref, mine_ref, below_ref, above_ref, value_ref, weight_ref):
    rows, width = value_ref.shape
    assembled(place_ref, mine_ref, below_ref, above_ref, weight_ref, slice(width, 2 * width))
    value = jnp.dot(normed_ref[...], weight_ref[...], preferred_element_type=F32).astype(BF16)
    value_ref[...] = permuted(to_residue(rows), value)


def stack_heads(q):
    lane = lax.broadcasted_iota(jnp.int32, q.shape, 1) >> 6
    return jnp.concatenate([jnp.where(lane == h, q, jnp.zeros_like(q)) for h in range(q.shape[1] // HEAD_DIM)], axis=0)


def own_heads(stacked):
    width = stacked.shape[1]
    heads = width // HEAD_DIM
    rows = stacked.shape[0] // heads
    lane = lax.broadcasted_iota(jnp.int32, (rows, width), 1) >> 6
    out = stacked[:rows]
    for h in range(1, heads):
        out = jnp.where(lane == h, stacked[h * rows : (h + 1) * rows], out)
    return out


def far_bias(block, back):
    qi = lax.broadcasted_iota(jnp.int32, (128, 128), 0)
    ki = lax.broadcasted_iota(jnp.int32, (128, 128), 1)
    ok = ((qi >> 5) == (ki >> 5)) & (block >= back)
    if back == 4:
        ok = ok & ((ki & 31) >= (qi & 31))
    return jnp.where(ok, 0.0, LOW).astype(F32)


def times_seen(o):
    count = (o <= SPAN).astype(F32)
    count = count + (((o & 3) == 0) & (o <= 4 * SPAN)).astype(F32)
    return count + ((o & 15) == 0).astype(F32)


def query_places(cls):
    i = lax.broadcasted_iota(jnp.int32, (128, 1), 0)
    return (i & 31) * 16 + (i >> 5) * 4 + cls


def own_kernel(q_ref, k_ref, v_ref, max_ref, sum_ref, acc_ref, s_ref, p_ref, bias_ref, count_ref):
    keys, width = k_ref.shape
    heads = width // HEAD_DIM
    o = query_places(pl.program_id(0)) - natural(lax.broadcasted_iota(jnp.int32, (1, keys), 1))
    count = jnp.where(o >= 0, times_seen(o), 0.0)
    count_ref[...] = count
    bias_ref[...] = jnp.where(count > 0, 0.0, LOW).astype(F32)
    s_ref[...] = lax.dot_general(stack_heads(q_ref[...]), k_ref[...], NT, preferred_element_type=F32)
    step = 32
    for r in range(0, heads * 128, step):
        mask = slice(r % 128, r % 128 + step)
        s = s_ref[r : r + step, :] + bias_ref[mask, :]
        m = jnp.max(s, axis=1, keepdims=True)
        p = jnp.exp(s - m) * count_ref[mask, :]
        max_ref[r : r + step, :] = jnp.broadcast_to(m, (step, 128))
        sum_ref[r : r + step, :] = jnp.broadcast_to(jnp.sum(p, axis=1, keepdims=True), (step, 128))
        p_ref[r : r + step, :] = p.astype(BF16)
    acc_ref[...] = own_heads(jnp.dot(p_ref[...], v_ref[...], preferred_element_type=F32))


def tiles(parts):
    low = lax.broadcasted_iota(jnp.int32, parts[0].shape, 1) < HEAD_DIM
    return jnp.concatenate([jnp.where(low, a, b) for a, b in zip(parts[0::2], parts[1::2])], axis=1)


def merged(q, key, value, bias, count, max_ref, sum_ref, acc_ref, s_ref, p_ref):
    heads = q.shape[1] // HEAD_DIM
    wide = key.shape[0] // 128
    s_ref[...] = lax.dot_general(stack_heads(q), key, NT, preferred_element_type=F32)
    tops, sums, scales = [], [], []
    for h in range(heads):
        part = slice(h * 128, (h + 1) * 128)
        s = s_ref[part, :] + bias
        old = max_ref[part, :]
        m = jnp.maximum(jnp.max(s, axis=1, keepdims=True), old)
        p = jnp.exp(s - jnp.concatenate([m] * wide, axis=1))
        if count is not None:
            p = p * count
        p_ref[part, :] = p.astype(BF16)
        scale = jnp.exp(old - m)
        tops.append(m)
        sums.append(sum_ref[part, :] * scale + jnp.sum(p, axis=1, keepdims=True))
        scales.append(scale)
    pv = own_heads(jnp.dot(p_ref[...], value, preferred_element_type=F32))
    return tops, sums, acc_ref[...] * tiles(scales) + pv


def store_state(state, max_ref, sum_ref, acc_ref):
    tops, sums, acc_ref[...] = state
    for h in range(len(tops)):
        max_ref[h * 128 : (h + 1) * 128, :] = tops[h]
        sum_ref[h * 128 : (h + 1) * 128, :] = sums[h]


def before_kernel(place_ref, q_ref, max_ref, sum_ref, acc_ref, k_ref, v_ref, new_max, new_sum, new_acc, s_ref, p_ref, tail_ref):
    cls = pl.program_id(0)
    keys = k_ref.shape[0]
    mine = pl.ds(pl.multiple_of(cls * 128, 128), 128)

    @pl.when(cls == 0)
    def _():
        j = lax.broadcasted_iota(jnp.int32, (128, keys), 0)
        i = lax.broadcasted_iota(jnp.int32, (128, keys), 1)
        pick = (i == (j >> 3) * 32 + 24 + (j & 7)).astype(BF16)
        tail_ref[0] = permuted(pick, k_ref[...])
        tail_ref[1] = permuted(pick, v_ref[...])

    seen = place_ref[0] >= 1
    qn = query_places(cls)
    k = lax.broadcasted_iota(jnp.int32, (1, 128), 1)
    same = times_seen(qn - ((k & 31) * 16 + (k >> 5) * 4 + cls) + keys)
    last = qn - ((24 + (k & 7)) * 16 + ((k >> 3) & 3) * 4 + (k >> 5)) + keys
    last = ((last <= SPAN) & ((k >> 5) != cls)).astype(F32)
    count = jnp.where(seen, jnp.concatenate([same, last], axis=1), 0.0)
    bias = jnp.where(count > 0, 0.0, LOW).astype(F32)
    key = jnp.concatenate([k_ref[mine, :], tail_ref[0]], axis=0)
    value = jnp.concatenate([v_ref[mine, :], tail_ref[1]], axis=0)
    store_state(merged(q_ref[...], key, value, bias, count, max_ref, sum_ref, acc_ref, s_ref, p_ref), new_max, new_sum, new_acc)


def far_kernel(back, place_ref, q_ref, max_ref, sum_ref, acc_ref, k_ref, v_ref, new_max, new_sum, new_acc, s_ref, p_ref):
    bias = far_bias(place_ref[0], back)
    state = merged(q_ref[...], k_ref[...], v_ref[...], bias, None, max_ref, sum_ref, acc_ref, s_ref, p_ref)
    store_state(state, new_max, new_sum, new_acc)


def score_kernel(back, place_ref, q_ref, max_ref, sum_ref, acc_ref, k_ref, p_ref, scaled_ref, total_ref, log_ref, s_ref):
    bias = far_bias(place_ref[0], back)
    s_ref[...] = lax.dot_general(stack_heads(q_ref[...]), k_ref[...], NT, preferred_element_type=F32)
    lane = lax.broadcasted_iota(jnp.int32, log_ref.shape, 1)
    logs = jnp.zeros(log_ref.shape, F32)
    sums, scales = [], []
    for h in range(q_ref.shape[1] // HEAD_DIM):
        part = slice(h * 128, (h + 1) * 128)
        s = s_ref[part, :] + bias
        old = max_ref[part, :]
        m = jnp.maximum(jnp.max(s, axis=1, keepdims=True), old)
        p = jnp.exp(s - m)
        p_ref[part, :] = p.astype(BF16)
        scale = jnp.exp(old - m)
        total = sum_ref[part, :] * scale + jnp.sum(p, axis=1, keepdims=True)
        scales.append(scale)
        sums.append(total)
        logs = jnp.where(lane == h, m + jnp.log(total), logs)
    scaled_ref[...] = acc_ref[...] * tiles(scales)
    total_ref[...] = tiles(sums)
    log_ref[...] = logs


def finish_kernel(p_ref, v_ref, scaled_ref, total_ref, out_ref, att_ref):
    cls = pl.program_id(0)
    pv = own_heads(jnp.dot(p_ref[...], v_ref[...], preferred_element_type=F32))
    att = (scaled_ref[...] + pv) / total_ref[...]
    att_ref[pl.ds(pl.multiple_of(cls * 128, 128), 128), :] = att.astype(BF16)

    @pl.when(cls == pl.num_programs(0) - 1)
    def _():
        out_ref[...] = permuted(to_natural(att_ref.shape[0]), att_ref[...])


def log_kernel(lw_ref, log_ref):
    rows, lanes = lw_ref.shape
    perm = to_natural(rows)
    rest = lw_ref[...]
    ordered = jnp.zeros((rows, lanes), F32)
    for _ in range(3):
        piece = rest.astype(BF16)
        rest = rest - piece.astype(F32)
        ordered = ordered + jnp.dot(perm, piece, preferred_element_type=F32)
    log_ref[...] = ordered.T[: log_ref.shape[0]]


def out_kernel(place_ref, att_ref, *refs):
    weights, (gain_ref, out_ref, sum_ref) = refs[:8], refs[8:]
    x, core = place_ref[2], place_ref[3]
    n = pl.program_id(0)
    columns = weights[0].shape[1]
    total = None
    for half, c in enumerate((core, 1 - core)):
        for k, hop in enumerate(HOPS):
            group = lax.rem(x + hop, 4) * 2 + c
            part = jnp.dot(att_ref[group], weights[half * 4 + k][...], preferred_element_type=F32)
            part = part.astype(BF16).astype(F32)
            total = part if total is None else total + part
    sum_ref[:, pl.ds(pl.multiple_of(n * columns, columns), columns)] = total

    @pl.when(n == pl.num_programs(0) - 1)
    def _():
        summed = sum_ref[...]
        scale = lax.rsqrt(jnp.mean(summed * summed, axis=1, keepdims=True) + EPS)
        out_ref[...] = (summed * scale * gain_ref[...]).astype(BF16)


SMEM = pl.BlockSpec(memory_space=pltpu.SMEM)
VMEM = pl.BlockSpec(memory_space=pltpu.VMEM)


def kernel_call(body, outs, args, flops, limit, scratch=(), **more):
    if "grid_spec" not in more:
        more["scratch_shapes"] = [pltpu.VMEM(s, t) for s, t in scratch]
    if "in_specs" not in more and "grid_spec" not in more:
        more["in_specs"] = [SMEM if a.dtype == jnp.int32 else VMEM for a in args]
        more["out_specs"] = tuple(VMEM for _ in outs)
    data = sum(a.size * a.dtype.itemsize for a in args)
    return pl.pallas_call(
        body,
        out_shape=tuple(jax.ShapeDtypeStruct(s, t) for s, t in outs),
        compiler_params=pltpu.CompilerParams(vmem_limit_bytes=limit * 1024 * 1024),
        cost_estimate=pl.CostEstimate(flops=flops, bytes_accessed=data, transcendentals=0),
        **more,
    )(*args)


def layer(hidden_in, pre_gain, query_proj, key_proj, value_proj, out_proj, post_gain):
    rows, depth = hidden_in.shape
    width = query_proj.shape[1]
    heads = width // HEAD_DIM
    piece = rows // 8
    sp, x, core = lax.axis_index(SP), lax.axis_index("x"), lax.axis_index("c")
    place = jnp.stack([sp, lax.axis_index("zl"), x, core]).astype(jnp.int32)
    gain = pre_gain[None]
    row = (rows, width)

    shard_spec = pl.BlockSpec(key_proj.shape, lambda n: (0, 0))
    (copies,) = kernel_call(
        copies_kernel,
        [((32, key_proj.shape[0], 2 * width), BF16)],
        (key_proj, value_proj),
        1000,
        56,
        grid=(2,),
        in_specs=[shard_spec] * 2,
        out_specs=(pl.BlockSpec((16, key_proj.shape[0], 2 * width), lambda n: (n, 0, 0)),),
    )
    mine = lax.all_to_all(copies, ("zh", "y"), split_axis=0, concat_axis=0, tiled=True)
    mine = mine.reshape(4, 256, 2 * width)
    slabs = []
    for columns in (slice(0, width), slice(width, 2 * width)):
        below = lax.ppermute(mine[:2, :, columns], Z, ring(8, 1))
        above = lax.ppermute(mine[2:, :, columns], Z, ring(8, -1))
        slabs.append((mine, below, above))

    groups = [out_proj]
    for steps in (1, -1, 2):
        groups.append(lax.ppermute(out_proj, "x", ring(4, steps)))
    for n in range(4):
        groups.append(lax.ppermute(groups[n], "c", ring(2, 1)))

    quarter = HEAD_DIM // 2
    frequency = ROPE_BASE ** (-(jnp.arange(quarter, dtype=F32) * 2.0 / HEAD_DIM))
    positions = (sp * rows + jnp.arange(rows, dtype=jnp.int32)).astype(F32)
    angles = positions[None, :] * frequency[:, None]
    turns = jnp.stack([jnp.cos(angles), jnp.sin(angles)])

    normed, query = kernel_call(
        query_kernel, [((rows, depth), BF16), (row, BF16)], (hidden_in, gain, query_proj, turns), 2 * rows * depth * width, 12
    )
    weight = [((depth, width), BF16)]
    (key,) = kernel_call(key_kernel, [(row, BF16)], (place, normed, *slabs[0], turns), 2 * rows * depth * width, 14, weight)
    (value,) = kernel_call(value_kernel, [(row, BF16)], (place, normed, *slabs[1]), 2 * rows * depth * width, 14, weight)
    forward = [(i, i + 1) for i in range(63)]
    keys, values = [key], [value]
    for _ in range(1, 5):
        keys.append(lax.ppermute(keys[-1], SP, forward))
        values.append(lax.ppermute(values[-1], SP, forward))
    whole = pl.BlockSpec(row, lambda c: (0, 0))
    part = pl.BlockSpec((128, width), lambda c: (c, 0))
    stat = pl.BlockSpec((512, 128), lambda c: (c, 0))
    stats = (4 * rows, 128)
    outs = [(stats, F32), (stats, F32), (row, F32)]
    pair = ((512, 256), F32), ((512, 256), BF16)
    state = kernel_call(
        own_kernel,
        outs,
        (query, keys[0], values[0]),
        8 * rows * rows * width,
        12,
        [((512, 512), F32), ((512, 512), BF16), ((128, 512), F32), ((128, 512), F32)],
        grid=(rows // 128,),
        in_specs=[part, whole, whole],
        out_specs=(stat, stat, part),
    )
    state = kernel_call(
        before_kernel,
        outs,
        (place, query, *state, keys[1], values[1]),
        4 * rows * rows * width,
        12,
        [*pair, ((2, 128, width), BF16)],
        grid=(rows // 128,),
        in_specs=[SMEM, part, stat, stat, part, whole, whole],
        out_specs=(stat, stat, part),
    )
    scores = ((512, 128), F32)
    for back in (2, 3):
        state = kernel_call(
            functools.partial(far_kernel, back),
            outs,
            (place, query, *state, keys[back], values[back]),
            4 * rows * 512 * width,
            16,
            [scores, ((512, 128), BF16)],
            grid=(rows // 128,),
            in_specs=[SMEM, part, stat, stat, part, part, part],
            out_specs=(stat, stat, part),
        )
    shares, scaled, total, logs = kernel_call(
        functools.partial(score_kernel, 4),
        [(stats, BF16), (row, F32), (row, F32), ((rows, 128), F32)],
        (place, query, *state, keys[4]),
        2 * rows * 512 * width,
        16,
        [scores],
        grid=(rows // 128,),
        in_specs=[SMEM, part, stat, stat, part, part],
        out_specs=(stat, part, part, pl.BlockSpec((128, 128), lambda c: (c, 0))),
    )
    (attended,) = kernel_call(
        finish_kernel,
        [(row, BF16)],
        (shares, values[4], scaled, total),
        2 * rows * 512 * width,
        16,
        [(row, BF16)],
        grid=(rows // 128,),
        in_specs=[stat, part, part, part],
        out_specs=(whole,),
    )

    arrived = lax.all_to_all(attended.reshape(8, piece, width), TP, split_axis=0, concat_axis=0, tiled=True)
    (log_weight,) = kernel_call(log_kernel, [((heads, rows), F32)], (logs,), 6 * rows * rows * width, 8)
    columns = depth // 4
    (layer_out,) = kernel_call(
        out_kernel,
        [((piece, depth), BF16)],
        (place, arrived, *groups, post_gain[None]),
        2 * piece * depth * depth,
        12,
        [((piece, depth), F32)],
        grid=(4,),
        in_specs=[SMEM, pl.BlockSpec((8, piece, width), lambda n: (0, 0, 0))]
        + [pl.BlockSpec((width, columns), lambda n: (0, n))] * 8
        + [pl.BlockSpec((1, depth), lambda n: (0, 0))],
        out_specs=(pl.BlockSpec((piece, depth), lambda n: (0, 0)),),
    )
    return layer_out, log_weight


def solution(mesh):
    fine = Mesh(np.asarray(mesh.devices).reshape(4, 2, 8, 4, 2), ("zh", "zl", "y", "x", "c"))
    placed = (P(SP, None), P(), P(None, TP), P(SP, TP), P(SP, TP), P(TP, None), P())
    return jax.shard_map(
        layer,
        mesh=fine,
        in_specs=placed,
        out_specs=(P(SP + TP, None), P(TP, SP)),
        check_vma=False,
    )
```

```python
import functools

import jax
import jax.numpy as jnp
import numpy as np
from jax import lax
from jax.experimental import pallas as pl
from jax.experimental.pallas import tpu as pltpu
from jax.sharding import Mesh
from jax.sharding import PartitionSpec as P

HEAD_DIM = 64
SPAN = 128
EPS = 1e-06
ROPE_BASE = 10000.0
LOW = -1e30
SP = ("zh", "zl", "y")
Z = ("zh", "zl")
TP = ("x", "c")
F32 = jnp.float32
BF16 = jnp.bfloat16
NT = (((1,), (1,)), ((), ()))
HOPS = (0, 3, 1, 2)


def ring(count, steps):
    return [(i, (i + steps) % count) for i in range(count)]


def natural(i):
    return (i & 31) * 16 + ((i >> 5) & 3) * 4 + (i >> 7)


def to_residue(rows, columns=None):
    i = lax.broadcasted_iota(jnp.int32, (rows, rows), 0)
    if columns is None:
        columns = lax.broadcasted_iota(jnp.int32, (rows, rows), 1)
    return (natural(i) == columns).astype(BF16)


def to_natural(rows):
    i = lax.broadcasted_iota(jnp.int32, (rows, rows), 1)
    n = lax.broadcasted_iota(jnp.int32, (rows, rows), 0)
    return (natural(i) == n).astype(BF16)


def rotated(x, cos, sin):
    width = x.shape[1]
    lane = lax.broadcasted_iota(jnp.int32, x.shape, 1)
    other = jnp.where((lane & 63) < 32, pltpu.roll(x, width - 32, 1), pltpu.roll(x, 32, 1))
    return x * cos + other * sin


def permuted(perm, x):
    return jnp.dot(perm, x, preferred_element_type=F32).astype(BF16)


def normed_rows(x, gain):
    x = x.astype(F32)
    scale = lax.rsqrt(jnp.mean(x * x, axis=1, keepdims=True) + EPS)
    return (x * scale * gain).astype(BF16)


def spread(turn_ref, part):
    cos, sin = turn_ref[0, :, part], turn_ref[1, :, part]
    cos = jnp.concatenate([cos] * 4, axis=0).T
    sin = jnp.concatenate([-sin, sin] * 2, axis=0).T
    return jnp.concatenate([cos, cos], axis=1), jnp.concatenate([sin, sin], axis=1)


def query_kernel(hidden_ref, gain_ref, weight_ref, turn_ref, normed_ref, query_ref):
    rows = hidden_ref.shape[0]
    gain = gain_ref[...]

    def step(i, carry):
        part = pl.ds(pl.multiple_of(i * 64, 64), 64)
        normed_ref[part, :] = normed_rows(hidden_ref[part, :], gain)
        return carry

    lax.fori_loop(0, rows // 64, step, 0)
    query = jnp.dot(normed_ref[...], weight_ref[...], preferred_element_type=F32)
    cos, sin = spread(turn_ref, slice(0, rows))
    query = rotated(query, cos, sin).astype(BF16) * 0.125
    query_ref[...] = permuted(to_residue(rows), query)


def copies_kernel(key_ref, value_ref, out_ref):
    both = jnp.concatenate([key_ref[...], value_ref[...]], axis=1)
    for n in range(out_ref.shape[0]):
        out_ref[n] = both


def assembled(place_ref, mine_ref, below_ref, above_ref, weight_ref, columns):
    low = place_ref[1]
    for k in range(4):
        weight_ref[pl.ds(pl.multiple_of((2 * k + low) * 256, 256), 256), :] = mine_ref[k, :, columns]
    for k in range(2):
        weight_ref[pl.ds(pl.multiple_of((2 * k + 1 - low) * 256, 256), 256), :] = below_ref[k]
        weight_ref[pl.ds(pl.multiple_of((2 * k + 5 - low) * 256, 256), 256), :] = above_ref[k]


def key_kernel(place_ref, normed_ref, mine_ref, below_ref, above_ref, turn_ref, key_ref, weight_ref):
    rows, width = key_ref.shape
    assembled(place_ref, mine_ref, below_ref, above_ref, weight_ref, slice(0, width))
    key = jnp.dot(normed_ref[...], weight_ref[...], preferred_element_type=F32)
    key = rotated(key, *spread(turn_ref, slice(0, rows))).astype(BF16)
    key_ref[...] = permuted(to_residue(rows), key)


def value_kernel(place_ref, normed_ref, mine_ref, below_ref, above_ref, value_ref, weight_ref):
    rows, width = value_ref.shape
    assembled(place_ref, mine_ref, below_ref, above_ref, weight_ref, slice(width, 2 * width))
    value = jnp.dot(normed_ref[...], weight_ref[...], preferred_element_type=F32).astype(BF16)
    value_ref[...] = permuted(to_residue(rows), value)


def stack_heads(q):
    lane = lax.broadcasted_iota(jnp.int32, q.shape, 1) >> 6
    return jnp.concatenate([jnp.where(lane == h, q, jnp.zeros_like(q)) for h in range(q.shape[1] // HEAD_DIM)], axis=0)


def own_heads(stacked):
    width = stacked.shape[1]
    heads = width // HEAD_DIM
    rows = stacked.shape[0] // heads
    lane = lax.broadcasted_iota(jnp.int32, (rows, width), 1) >> 6
    out = stacked[:rows]
    for h in range(1, heads):
        out = jnp.where(lane == h, stacked[h * rows : (h + 1) * rows], out)
    return out


def far_bias(block, back):
    qi = lax.broadcasted_iota(jnp.int32, (128, 128), 0)
    ki = lax.broadcasted_iota(jnp.int32, (128, 128), 1)
    ok = ((qi >> 5) == (ki >> 5)) & (block >= back)
    if back == 4:
        ok = ok & ((ki & 31) >= (qi & 31))
    return jnp.where(ok, 0.0, LOW).astype(F32)


def times_seen(o):
    count = (o <= SPAN).astype(F32)
    count = count + (((o & 3) == 0) & (o <= 4 * SPAN)).astype(F32)
    return count + ((o & 15) == 0).astype(F32)


def query_places(cls):
    i = lax.broadcasted_iota(jnp.int32, (128, 1), 0)
    return (i & 31) * 16 + (i >> 5) * 4 + cls


def own_kernel(q_ref, k_ref, v_ref, max_ref, sum_ref, acc_ref, s_ref, p_ref, bias_ref, count_ref):
    keys, width = k_ref.shape
    heads = width // HEAD_DIM
    o = query_places(pl.program_id(0)) - natural(lax.broadcasted_iota(jnp.int32, (1, keys), 1))
    count = jnp.where(o >= 0, times_seen(o), 0.0)
    count_ref[...] = count
    bias_ref[...] = jnp.where(count > 0, 0.0, LOW).astype(F32)
    s_ref[...] = lax.dot_general(stack_heads(q_ref[...]), k_ref[...], NT, preferred_element_type=F32)
    step = 32
    for r in range(0, heads * 128, step):
        mask = slice(r % 128, r % 128 + step)
        s = s_ref[r : r + step, :] + bias_ref[mask, :]
        m = jnp.max(s, axis=1, keepdims=True)
        p = jnp.exp(s - m) * count_ref[mask, :]
        max_ref[r : r + step, :] = jnp.broadcast_to(m, (step, 128))
        sum_ref[r : r + step, :] = jnp.broadcast_to(jnp.sum(p, axis=1, keepdims=True), (step, 128))
        p_ref[r : r + step, :] = p.astype(BF16)
    acc_ref[...] = own_heads(jnp.dot(p_ref[...], v_ref[...], preferred_element_type=F32))


def tiles(parts):
    low = lax.broadcasted_iota(jnp.int32, parts[0].shape, 1) < HEAD_DIM
    return jnp.concatenate([jnp.where(low, a, b) for a, b in zip(parts[0::2], parts[1::2])], axis=1)


def merged(q, key, value, bias, count, max_ref, sum_ref, acc_ref, s_ref, p_ref):
    heads = q.shape[1] // HEAD_DIM
    wide = key.shape[0] // 128
    s_ref[...] = lax.dot_general(stack_heads(q), key, NT, preferred_element_type=F32)
    tops, sums, scales = [], [], []
    for h in range(heads):
        part = slice(h * 128, (h + 1) * 128)
        s = s_ref[part, :] + bias
        old = max_ref[part, :]
        m = jnp.maximum(jnp.max(s, axis=1, keepdims=True), old)
        p = jnp.exp(s - jnp.concatenate([m] * wide, axis=1))
        if count is not None:
            p = p * count
        p_ref[part, :] = p.astype(BF16)
        scale = jnp.exp(old - m)
        tops.append(m)
        sums.append(sum_ref[part, :] * scale + jnp.sum(p, axis=1, keepdims=True))
        scales.append(scale)
    pv = own_heads(jnp.dot(p_ref[...], value, preferred_element_type=F32))
    return tops, sums, acc_ref[...] * tiles(scales) + pv


def store_state(state, max_ref, sum_ref, acc_ref):
    tops, sums, acc_ref[...] = state
    for h in range(len(tops)):
        max_ref[h * 128 : (h + 1) * 128, :] = tops[h]
        sum_ref[h * 128 : (h + 1) * 128, :] = sums[h]


def before_kernel(place_ref, q_ref, max_ref, sum_ref, acc_ref, k_ref, v_ref, new_max, new_sum, new_acc, s_ref, p_ref, tail_ref):
    cls = pl.program_id(0)
    keys = k_ref.shape[0]
    mine = pl.ds(pl.multiple_of(cls * 128, 128), 128)

    @pl.when(cls == 0)
    def _():
        j = lax.broadcasted_iota(jnp.int32, (128, keys), 0)
        i = lax.broadcasted_iota(jnp.int32, (128, keys), 1)
        pick = (i == (j >> 3) * 32 + 24 + (j & 7)).astype(BF16)
        tail_ref[0] = permuted(pick, k_ref[...])
        tail_ref[1] = permuted(pick, v_ref[...])

    seen = place_ref[0] >= 1
    qn = query_places(cls)
    k = lax.broadcasted_iota(jnp.int32, (1, 128), 1)
    same = times_seen(qn - ((k & 31) * 16 + (k >> 5) * 4 + cls) + keys)
    last = qn - ((24 + (k & 7)) * 16 + ((k >> 3) & 3) * 4 + (k >> 5)) + keys
    last = ((last <= SPAN) & ((k >> 5) != cls)).astype(F32)
    count = jnp.where(seen, jnp.concatenate([same, last], axis=1), 0.0)
    bias = jnp.where(count > 0, 0.0, LOW).astype(F32)
    key = jnp.concatenate([k_ref[mine, :], tail_ref[0]], axis=0)
    value = jnp.concatenate([v_ref[mine, :], tail_ref[1]], axis=0)
    store_state(merged(q_ref[...], key, value, bias, count, max_ref, sum_ref, acc_ref, s_ref, p_ref), new_max, new_sum, new_acc)


def far_kernel(back, place_ref, q_ref, max_ref, sum_ref, acc_ref, k_ref, v_ref, new_max, new_sum, new_acc, s_ref, p_ref):
    bias = far_bias(place_ref[0], back)
    state = merged(q_ref[...], k_ref[...], v_ref[...], bias, None, max_ref, sum_ref, acc_ref, s_ref, p_ref)
    store_state(state, new_max, new_sum, new_acc)


def score_kernel(back, place_ref, q_ref, max_ref, sum_ref, acc_ref, k_ref, p_ref, scaled_ref, total_ref, log_ref, s_ref):
    bias = far_bias(place_ref[0], back)
    s_ref[...] = lax.dot_general(stack_heads(q_ref[...]), k_ref[...], NT, preferred_element_type=F32)
    lane = lax.broadcasted_iota(jnp.int32, log_ref.shape, 1)
    logs = jnp.zeros(log_ref.shape, F32)
    sums, scales = [], []
    for h in range(q_ref.shape[1] // HEAD_DIM):
        part = slice(h * 128, (h + 1) * 128)
        s = s_ref[part, :] + bias
        old = max_ref[part, :]
        m = jnp.maximum(jnp.max(s, axis=1, keepdims=True), old)
        p = jnp.exp(s - m)
        p_ref[part, :] = p.astype(BF16)
        scale = jnp.exp(old - m)
        total = sum_ref[part, :] * scale + jnp.sum(p, axis=1, keepdims=True)
        scales.append(scale)
        sums.append(total)
        logs = jnp.where(lane == h, m + jnp.log(total), logs)
    inverse = 1.0 / tiles(sums)
    scaled_ref[...] = acc_ref[...] * tiles(scales) * inverse
    total_ref[...] = inverse
    log_ref[...] = logs


def finish_kernel(p_ref, v_ref, scaled_ref, total_ref, out_ref, att_ref):
    cls = pl.program_id(0)
    pv = own_heads(jnp.dot(p_ref[...], v_ref[...], preferred_element_type=F32))
    att = scaled_ref[...] + pv * total_ref[...]
    att_ref[pl.ds(pl.multiple_of(cls * 128, 128), 128), :] = att.astype(BF16)

    @pl.when(cls == pl.num_programs(0) - 1)
    def _():
        out_ref[...] = permuted(to_natural(att_ref.shape[0]), att_ref[...])


def log_kernel(lw_ref, log_ref):
    rows, lanes = lw_ref.shape
    perm = to_natural(rows)
    rest = lw_ref[...]
    ordered = jnp.zeros((rows, lanes), F32)
    for _ in range(3):
        piece = rest.astype(BF16)
        rest = rest - piece.astype(F32)
        ordered = ordered + jnp.dot(perm, piece, preferred_element_type=F32)
    log_ref[...] = ordered.T[: log_ref.shape[0]]


def out_kernel(place_ref, att_ref, *refs):
    weights, (gain_ref, out_ref, sum_ref) = refs[:8], refs[8:]
    x, core = place_ref[2], place_ref[3]
    n = pl.program_id(0)
    columns = weights[0].shape[1]
    total = None
    for half, c in enumerate((core, 1 - core)):
        for k, hop in enumerate(HOPS):
            group = lax.rem(x + hop, 4) * 2 + c
            part = jnp.dot(att_ref[group], weights[half * 4 + k][...], preferred_element_type=F32)
            part = part.astype(BF16).astype(F32)
            total = part if total is None else total + part
    sum_ref[:, pl.ds(pl.multiple_of(n * columns, columns), columns)] = total

    @pl.when(n == pl.num_programs(0) - 1)
    def _():
        summed = sum_ref[...]
        scale = lax.rsqrt(jnp.mean(summed * summed, axis=1, keepdims=True) + EPS)
        out_ref[...] = (summed * scale * gain_ref[...]).astype(BF16)


SMEM = pl.BlockSpec(memory_space=pltpu.SMEM)
VMEM = pl.BlockSpec(memory_space=pltpu.VMEM)


def kernel_call(body, outs, args, flops, limit, scratch=(), **more):
    if "grid_spec" not in more:
        more["scratch_shapes"] = [pltpu.VMEM(s, t) for s, t in scratch]
    if "in_specs" not in more and "grid_spec" not in more:
        more["in_specs"] = [SMEM if a.dtype == jnp.int32 else VMEM for a in args]
        more["out_specs"] = tuple(VMEM for _ in outs)
    data = sum(a.size * a.dtype.itemsize for a in args)
    return pl.pallas_call(
        body,
        out_shape=tuple(jax.ShapeDtypeStruct(s, t) for s, t in outs),
        compiler_params=pltpu.CompilerParams(vmem_limit_bytes=limit * 1024 * 1024),
        cost_estimate=pl.CostEstimate(flops=flops, bytes_accessed=data, transcendentals=0),
        **more,
    )(*args)


def layer(hidden_in, pre_gain, query_proj, key_proj, value_proj, out_proj, post_gain):
    rows, depth = hidden_in.shape
    width = query_proj.shape[1]
    heads = width // HEAD_DIM
    piece = rows // 8
    sp, x, core = lax.axis_index(SP), lax.axis_index("x"), lax.axis_index("c")
    place = jnp.stack([sp, lax.axis_index("zl"), x, core]).astype(jnp.int32)
    gain = pre_gain[None]
    row = (rows, width)

    shard_spec = pl.BlockSpec(key_proj.shape, lambda n: (0, 0))
    (copies,) = kernel_call(
        copies_kernel,
        [((32, key_proj.shape[0], 2 * width), BF16)],
        (key_proj, value_proj),
        1000,
        56,
        grid=(1,),
        in_specs=[shard_spec] * 2,
        out_specs=(pl.BlockSpec((32, key_proj.shape[0], 2 * width), lambda n: (n, 0, 0)),),
    )
    mine = lax.all_to_all(copies, ("zh", "y"), split_axis=0, concat_axis=0, tiled=True)
    mine = mine.reshape(4, 256, 2 * width)
    slabs = []
    for columns in (slice(0, width), slice(width, 2 * width)):
        below = lax.ppermute(mine[:2, :, columns], Z, ring(8, 1))
        above = lax.ppermute(mine[2:, :, columns], Z, ring(8, -1))
        slabs.append((mine, below, above))

    groups = [out_proj]
    for steps in (1, -1, 2):
        groups.append(lax.ppermute(out_proj, "x", ring(4, steps)))
    for n in range(4):
        groups.append(lax.ppermute(groups[n], "c", ring(2, 1)))

    quarter = HEAD_DIM // 2
    frequency = ROPE_BASE ** (-(jnp.arange(quarter, dtype=F32) * 2.0 / HEAD_DIM))
    positions = (sp * rows + jnp.arange(rows, dtype=jnp.int32)).astype(F32)
    angles = positions[None, :] * frequency[:, None]
    turns = jnp.stack([jnp.cos(angles), jnp.sin(angles)])

    normed, query = kernel_call(
        query_kernel, [((rows, depth), BF16), (row, BF16)], (hidden_in, gain, query_proj, turns), 2 * rows * depth * width, 12
    )
    weight = [((depth, width), BF16)]
    (key,) = kernel_call(key_kernel, [(row, BF16)], (place, normed, *slabs[0], turns), 2 * rows * depth * width, 14, weight)
    (value,) = kernel_call(value_kernel, [(row, BF16)], (place, normed, *slabs[1]), 2 * rows * depth * width, 14, weight)
    forward = [(i, i + 1) for i in range(63)]
    keys, values = [key], [value]
    for _ in range(1, 5):
        keys.append(lax.ppermute(keys[-1], SP, forward))
        values.append(lax.ppermute(values[-1], SP, forward))
    whole = pl.BlockSpec(row, lambda c: (0, 0))
    part = pl.BlockSpec((128, width), lambda c: (c, 0))
    stat = pl.BlockSpec((512, 128), lambda c: (c, 0))
    stats = (4 * rows, 128)
    outs = [(stats, F32), (stats, F32), (row, F32)]
    pair = ((512, 256), F32), ((512, 256), BF16)
    state = kernel_call(
        own_kernel,
        outs,
        (query, keys[0], values[0]),
        8 * rows * rows * width,
        12,
        [((512, 512), F32), ((512, 512), BF16), ((128, 512), F32), ((128, 512), F32)],
        grid=(rows // 128,),
        in_specs=[part, whole, whole],
        out_specs=(stat, stat, part),
    )
    state = kernel_call(
        before_kernel,
        outs,
        (place, query, *state, keys[1], values[1]),
        4 * rows * rows * width,
        12,
        [*pair, ((2, 128, width), BF16)],
        grid=(rows // 128,),
        in_specs=[SMEM, part, stat, stat, part, whole, whole],
        out_specs=(stat, stat, part),
    )
    scores = ((512, 128), F32)
    for back in (2, 3):
        state = kernel_call(
            functools.partial(far_kernel, back),
            outs,
            (place, query, *state, keys[back], values[back]),
            4 * rows * 512 * width,
            16,
            [scores, ((512, 128), BF16)],
            grid=(rows // 128,),
            in_specs=[SMEM, part, stat, stat, part, part, part],
            out_specs=(stat, stat, part),
        )
    shares, scaled, total, logs = kernel_call(
        functools.partial(score_kernel, 4),
        [(stats, BF16), (row, F32), (row, F32), ((rows, 128), F32)],
        (place, query, *state, keys[4]),
        2 * rows * 512 * width,
        16,
        [scores],
        grid=(rows // 128,),
        in_specs=[SMEM, part, stat, stat, part, part],
        out_specs=(stat, part, part, pl.BlockSpec((128, 128), lambda c: (c, 0))),
    )
    (attended,) = kernel_call(
        finish_kernel,
        [(row, BF16)],
        (shares, values[4], scaled, total),
        2 * rows * 512 * width,
        16,
        [(row, BF16)],
        grid=(rows // 128,),
        in_specs=[stat, part, part, part],
        out_specs=(whole,),
    )

    arrived = lax.all_to_all(attended.reshape(8, piece, width), TP, split_axis=0, concat_axis=0, tiled=True)
    (log_weight,) = kernel_call(log_kernel, [((heads, rows), F32)], (logs,), 6 * rows * rows * width, 8)
    columns = depth // 4
    (layer_out,) = kernel_call(
        out_kernel,
        [((piece, depth), BF16)],
        (place, arrived, *groups, post_gain[None]),
        2 * piece * depth * depth,
        12,
        [((piece, depth), F32)],
        grid=(4,),
        in_specs=[SMEM, pl.BlockSpec((8, piece, width), lambda n: (0, 0, 0))]
        + [pl.BlockSpec((width, columns), lambda n: (0, n))] * 8
        + [pl.BlockSpec((1, depth), lambda n: (0, 0))],
        out_specs=(pl.BlockSpec((piece, depth), lambda n: (0, 0)),),
    )
    return layer_out, log_weight


def solution(mesh):
    fine = Mesh(np.asarray(mesh.devices).reshape(4, 2, 8, 4, 2), ("zh", "zl", "y", "x", "c"))
    placed = (P(SP, None), P(), P(None, TP), P(SP, TP), P(SP, TP), P(TP, None), P())
    return jax.shard_map(
        layer,
        mesh=fine,
        in_specs=placed,
        out_specs=(P(SP + TP, None), P(TP, SP)),
        check_vma=False,
    )
```
